32 devices in a mesh: ep: 8 (over z, x), tp: 4 (over y, core).
Axes of the slice: x: 2, y: 2, z: 4, core: 2. Of those that a mesh axis runs over, the one named last changes fastest.
Arguments:
- tokens: bfloat16 [2048, 2048], P('ep'), may hold values from -6 to 6
- routes: int32 [2048, 4], P('ep'), may hold values from 0 to 7, all different within a row; in each aligned block of 256 rows (0 to 255, 256 to 511, ...) at most 160 rows name the same one
- gate_weights: float32 [2048, 4], P('ep'), may hold values from 0.05 to 1
- out_grad: bfloat16 [2048, 2048], P('ep'), may hold values from -0.59765625 to 0.59765625
- w_gate: bfloat16 [8, 2048, 1024], P('ep', None, 'tp'), may hold values from -0.1875 to 0.1875
- w_up: bfloat16 [8, 2048, 1024], P('ep', None, 'tp'), may hold values from -0.1875 to 0.1875
- w_down: bfloat16 [8, 1024, 2048], P('ep', 'tp'), may hold values from -0.1875 to 0.1875
Outputs:
- token_grad: bfloat16 [2048, 2048], P('ep', 'tp')
- gate_grad: float32 [2048, 4], P('ep')
- gate_weight_grad: float32 [8, 2048, 1024], P('ep', None, 'tp')
- up_weight_grad: float32 [8, 2048, 1024], P('ep', None, 'tp')
- down_weight_grad: float32 [8, 1024, 2048], P('ep', 'tp')
The draws below stay inside these ranges and needn't reach their ends.
Inputs may be any that keep to these rules, and one draw needn't show every extreme that they name: `routes`: each row names 4 different experts. In each aligned block of 256 rows (the rows of one device) no expert is named by more than 160 rows, and in some block an expert is named by exactly 160 rows.
All inputs are finite; a program needn't handle non-finite values.
Results may differ from the reference program's by a relative error of at most 0.012.
Values may be sent and summed in bfloat16 or wider, within the bound.
A program may use at most 128 MiB of HBM per device.

```python
import math
import jax
import jax.numpy as jnp
import numpy as np
from jax import lax

D = 2048
FF = 1024
TOPK = 4
TOK_DEV = 256
EXPERTS = 8
TOKENS = 2048
CAP = 160
N_EP = 8
N_TP = 4


def steps_of(rng, extent, split, smallest, high):
    def one(axis_at, parts):
        heights = jax.random.uniform(jax.random.fold_in(jax.random.fold_in(rng, 6), axis_at), (parts,), jnp.float32, smallest / len(split), high / len(split))
        return jnp.repeat(jnp.exp(heights), extent[axis_at] // parts).reshape((-1,) + (1,) * (len(extent) - axis_at - 1))

    gain = one(*split[0])
    for cut in split[1:]:
        gain = gain * one(*cut)
    return gain


def assign_block(key, own, number, rows, amount, top, reach, lean):
    ranking = jax.random.permutation(key, amount)
    crowded, usual = portions_of(amount, rows * top, reach, lean, True), portions_of(amount, rows * top, reach, lean, False)
    places = jnp.arange(amount)

    def named(sizes, rotation):
        used = int((sizes > 0).sum())
        fixed = max(1, used // 4)
        moved = fixed + (places - fixed + rotation * (used - fixed)) % max(1, amount - fixed)
        return jnp.zeros((amount,), jnp.int32).at[ranking[jnp.where(places < fixed, places, moved)]].set(jnp.asarray(sizes, jnp.int32))

    sizes = jnp.where(number % 4 == 0, named(crowded, number // 4), named(usual, number - number // 4 - 1))
    mixed = jax.random.permutation(jax.random.fold_in(own, 3), amount)
    source_of, receiver = mixed[0:amount // 2 * 2:2], mixed[1:amount // 2 * 2:2]
    margin = jnp.minimum(sizes[source_of] - 1, reach - sizes[receiver]) // 2
    margin = jnp.where((source_of == ranking[0]) | (receiver == ranking[0]) | (sizes[receiver] == 0), 0, jnp.maximum(margin, 0))
    moved = jax.random.randint(jax.random.fold_in(own, 4), (amount // 2,), 0, 1 << 20) % (margin + 1)
    sizes = sizes.at[source_of].add(-moved).at[receiver].add(moved)
    labels = jnp.searchsorted(jnp.cumsum(sizes), jnp.arange(rows * top), side="right").astype(jnp.int32)
    grid = labels.reshape(top, rows).T
    grid = grid[jax.random.permutation(jax.random.fold_in(own, 1), rows)]
    rotation = jax.random.randint(jax.random.fold_in(own, 2), (rows, 1), 0, top)
    return jnp.take_along_axis(grid, (jnp.arange(top)[None, :] + rotation) % top, axis=1)


def portions_of(count, total, reach, lean, full):
    weights = [(1 << 20) // math.isqrt(rank ** lean) + 1 for rank in range(1, count + 1)]
    largest = reach if full else min(reach, max(-(-total // count), total * weights[0] // sum(weights)))
    least = 1 if total - largest >= count - 1 else 0
    given, surplus = [largest] + [least] * (count - 1), total - largest - least * (count - 1)
    while surplus > 0:
        movable = [i for i in range(1, count) if given[i] < largest] or [i for i in range(1, count) if given[i] < reach]
        mass, remaining = sum([weights[i] for i in movable]), surplus
        for i in movable:
            more = min(reach - given[i], max(1, remaining * weights[i] // mass), surplus)
            given[i] = given[i] + more
            surplus = surplus - more
    return np.array(given)


def bell_draw(key, extent, scale, bound, shards=(), kind=jnp.bfloat16):
    values = jax.random.normal(key, extent, jnp.float32) * scale
    if len(shards) > 0:
        values = steps_of(key, extent, shards, -0.22, 0.18) * values
    return jnp.clip(values, min=-bound, max=bound).astype(kind)


def setup_inputs(seed: int = 0) -> dict:
    key_of = jax.random.split(jax.random.key(seed), 8)
    tokens = bell_draw(key_of[0], (TOKENS, D), 1.0, 6.0, ((0, 8),))
    routes_keys = jax.random.split(jax.random.fold_in(key_of[1], 1), TOKENS // TOK_DEV)
    routes_turns = jax.random.permutation(jax.random.fold_in(key_of[1], 3), TOKENS // TOK_DEV)
    routes = jax.vmap(lambda own, number: assign_block(jax.random.fold_in(key_of[1], 2), own, number, TOK_DEV, EXPERTS, TOPK, CAP, 1))(routes_keys, routes_turns).reshape((TOKENS, TOPK))
    gate_weights = jnp.clip(jnp.exp(math.log(1.0) - 2.9957323 * jax.random.uniform(key_of[2], (TOKENS, TOPK), jnp.float32) ** steps_of(key_of[2], (TOKENS, TOPK), ((0, 8),), -0.2, 0.2)), 0.05, 1.0)
    out_grad = bell_draw(key_of[3], (TOKENS, D), 0.1, 0.59765625, ((0, 8),))
    w_gate = bell_draw(key_of[4], (EXPERTS, D, FF), (D // 2) ** -0.5, 0.1875, ((0, 8), (2, 4)))
    w_up = bell_draw(key_of[5], (EXPERTS, D, FF), (D // 2) ** -0.5, 0.1875, ((0, 8), (2, 4)))
    w_down = bell_draw(key_of[6], (EXPERTS, FF, D), FF ** -0.5, 0.1875, ((0, 8), (1, 4)))
    return dict(tokens=tokens, routes=routes, gate_weights=gate_weights, out_grad=out_grad, w_gate=w_gate, w_up=w_up, w_down=w_down)


clamp_limit = 7.0
sigmoid_slope = 1.702


def unit_backward(gate_pre, up_pre, hidden_grad):
    glu = jnp.minimum(gate_pre, clamp_limit)
    linear = jnp.clip(up_pre, -clamp_limit, clamp_limit)
    sigma = jax.nn.sigmoid(sigmoid_slope * glu)
    active = glu * sigma
    hidden = (active * (linear + 1.0)).astype(jnp.bfloat16)
    slope_term = sigma + sigmoid_slope * active * (1.0 - sigma)
    gate_pre_grad = jnp.where(gate_pre < clamp_limit, hidden_grad * (linear + 1.0) * slope_term, 0.0).astype(jnp.bfloat16)
    up_pre_grad = jnp.where(jnp.abs(up_pre) < clamp_limit, hidden_grad * active, 0.0).astype(jnp.bfloat16)
    return hidden, gate_pre_grad, up_pre_grad


def block_round_total(partial_value):
    rounded = lax.optimization_barrier(partial_value.astype(jnp.bfloat16))
    return jnp.sum(rounded.astype(jnp.float32), axis=0)


def reference(tokens, routes, gate_weights, out_grad, w_gate, w_up, w_down):
    blocks = routes.reshape(N_EP, TOK_DEV * TOPK)
    onehot = (blocks[:, :, None] == jnp.arange(EXPERTS, dtype=jnp.int32)[None, None, :]).astype(jnp.int32)
    slot_rank = jnp.sum((jnp.cumsum(onehot, axis=1) - onehot) * onehot, axis=2)
    source = jnp.arange(N_EP, dtype=jnp.int32)[:, None]
    target = (blocks * (N_EP * CAP) + source * CAP + slot_rank).reshape(-1)
    pair_index = jnp.arange(TOKENS * TOPK, dtype=jnp.int32)
    pair_table = jnp.zeros((EXPERTS * N_EP * CAP,), jnp.int32).at[target].set(pair_index)
    filled = jnp.zeros((EXPERTS * N_EP * CAP,), jnp.int32).at[target].set(1)
    flat_weights = gate_weights.reshape(-1)
    row_count = N_EP * CAP

    def per_expert(running, expert):
        token_acc, gate_acc = running
        slot_pairs = lax.dynamic_slice_in_dim(pair_table, expert * row_count, row_count)
        is_live = lax.dynamic_slice_in_dim(filled, expert * row_count, row_count)[:, None] > 0
        token_index = slot_pairs // TOPK
        x_rows = jnp.where(is_live, tokens[token_index], jnp.zeros((), jnp.bfloat16))
        dy_rows = out_grad[token_index]
        scaled = jnp.where(is_live, flat_weights[slot_pairs][:, None] * dy_rows.astype(jnp.float32), 0.0).astype(jnp.bfloat16)
        gate_mat = w_gate[expert]
        up_mat = w_up[expert]
        down_mat = w_down[expert]
        gate_pre = jnp.dot(x_rows, gate_mat, preferred_element_type=jnp.float32)
        up_pre = jnp.dot(x_rows, up_mat, preferred_element_type=jnp.float32)
        hidden_grad = jnp.dot(scaled, down_mat.T, preferred_element_type=jnp.float32)
        hidden, gate_pre_grad, up_pre_grad = unit_backward(gate_pre, up_pre, hidden_grad)
        unit_block = FF // N_TP
        gate_blocks = gate_pre_grad.astype(jnp.float32).reshape(row_count, N_TP, unit_block)
        up_blocks = up_pre_grad.astype(jnp.float32).reshape(row_count, N_TP, unit_block)
        hidden_blocks = hidden.astype(jnp.float32).reshape(row_count, N_TP, unit_block)
        gate_mat_blocks = gate_mat.astype(jnp.float32).reshape(D, N_TP, unit_block)
        up_mat_blocks = up_mat.astype(jnp.float32).reshape(D, N_TP, unit_block)
        down_blocks = down_mat.astype(jnp.float32).reshape(N_TP, unit_block, D)
        row_partial = jnp.einsum('rnf,dnf->nrd', gate_blocks, gate_mat_blocks) + jnp.einsum('rnf,dnf->nrd', up_blocks, up_mat_blocks)
        row_grad = block_round_total(row_partial).astype(jnp.bfloat16)
        expert_out = block_round_total(jnp.einsum('rnf,nfd->nrd', hidden_blocks, down_blocks))
        token_acc = token_acc.at[token_index].add(jnp.where(is_live, row_grad.astype(jnp.float32), 0.0))
        products = jnp.sum(dy_rows.astype(jnp.float32) * expert_out, axis=1)
        gate_acc = gate_acc.at[slot_pairs].add(jnp.where(is_live[:, 0], products, 0.0))
        gate_weight_grad = jnp.dot(x_rows.T, gate_pre_grad, preferred_element_type=jnp.float32)
        up_weight_grad = jnp.dot(x_rows.T, up_pre_grad, preferred_element_type=jnp.float32)
        down_weight_grad = jnp.dot(hidden.T, scaled, preferred_element_type=jnp.float32)
        return (token_acc, gate_acc), (gate_weight_grad, up_weight_grad, down_weight_grad)

    start = (jnp.zeros((TOKENS, D), jnp.float32), jnp.zeros((TOKENS * TOPK,), jnp.float32))
    (token_acc, gate_acc), grads = lax.scan(per_expert, start, jnp.arange(EXPERTS, dtype=jnp.int32))
    return (token_acc.astype(jnp.bfloat16), gate_acc.reshape(TOKENS, TOPK), grads[0], grads[1], grads[2])
```

```python
import jax
import jax.numpy as jnp
from jax import lax
from jax.experimental import pallas as pl
from jax.experimental.pallas import tpu as pltpu
from jax.sharding import PartitionSpec as P

clamp_limit = 7.0
sigmoid_slope = 1.702
MESH = pl.DeviceIdType.MESH


def partners():
    ep_count = lax.axis_size("ep")
    tp_count = lax.axis_size("tp")
    here = lax.axis_index("ep")
    part = lax.axis_index("tp")
    beside = part + 1 - 2 * (part % 2)
    across = (part + tp_count // 2) % tp_count
    return ep_count, here, part, beside, across


def greet(ep_count, here, part, beside, across):
    barrier = pltpu.get_barrier_semaphore()
    pl.semaphore_signal(barrier, inc=1, device_id=(here, beside), device_id_type=MESH)
    pl.semaphore_signal(barrier, inc=1, device_id=(here, across), device_id_type=MESH)

    def call(j, carry):
        peer = (here + j) % ep_count
        pl.semaphore_signal(barrier, inc=1, device_id=(peer, part), device_id_type=MESH)
        return carry

    lax.fori_loop(1, ep_count, call, 0)
    pl.semaphore_wait(barrier, ep_count + 1)


def remote(src, dst, sent, got, device):
    return pltpu.make_async_remote_copy(
        src_ref=src, dst_ref=dst, send_sem=sent, recv_sem=got, device_id=device, device_id_type=MESH
    )


def dispatch_kernel(
    token_ref, grad_ref, weight_ref, token_rows, grad_rows, weights_out,
    s1, r1, s2, r2, s3, r3, s4, r4, sw, rw, own_sem,
):
    ep_count, here, part, beside, across = partners()
    width = token_ref.shape[2]
    pairs = ((0, token_ref, token_rows), (1, grad_ref, grad_rows))

    def block(rows_ref, source, owner):
        columns = pl.ds(pl.multiple_of(owner * width, width), width)
        return rows_ref.at[source, :, columns]

    greet(ep_count, here, part, beside, across)

    def first(j):
        peer = (here + j) % ep_count
        return [
            remote(send.at[peer], block(rows, here, part), s1.at[i, j], r1.at[i, j], (peer, part))
            for i, send, rows in pairs
        ]

    def first_weight(j):
        peer = (here + j) % ep_count
        return remote(
            weight_ref.at[peer], weights_out.at[here], sw.at[j], rw.at[j], (peer, part)
        )

    def forward(j, owner, sent, got, to):
        source = (here + ep_count - j) % ep_count
        return [
            remote(
                block(rows, source, owner), block(rows, source, owner),
                sent.at[i, j], got.at[i, j], (here, to),
            )
            for i, _, rows in pairs
        ]

    def near(j):
        return forward(j, part, s2, r2, beside)

    def far(j):
        return forward(j, part, s3, r3, across)

    def onward(j):
        return forward(j, across, s4, r4, beside)

    owns = [
        pltpu.make_async_copy(send.at[here], block(rows, here, part), own_sem.at[i])
        for i, send, rows in pairs
    ]
    owns.append(pltpu.make_async_copy(weight_ref.at[here], weights_out.at[here], own_sem.at[2]))
    for copy in owns:
        copy.start()

    def launch(j, carry):
        first_weight(j).start()
        for copy in first(j):
            copy.start()
        return carry

    lax.fori_loop(1, ep_count, launch, 0)
    for copy in owns:
        copy.wait()
    for copy in far(0) + near(0):
        copy.start()

    def pass_on(j, carry):
        @pl.when(j < ep_count)
        def _():
            for i in range(2):
                first(j)[i].wait_recv()
                far(j)[i].start()
                near(j)[i].start()

        @pl.when(j >= 2)
        def _():
            for i in range(2):
                far(j - 2)[i].wait_recv()
                onward(j - 2)[i].start()

        return carry

    lax.fori_loop(1, ep_count + 2, pass_on, 0)

    def finish(j, carry):
        for i in range(2):
            near(j)[i].wait()
            onward(j)[i].wait()
            far(j)[i].wait_send()

        @pl.when(j >= 1)
        def _():
            for copy in first(j):
                copy.wait_send()
            first_weight(j).wait()

        return carry

    lax.fori_loop(0, ep_count, finish, 0)


def dispatch(send_tokens, send_grads, weights, model_width):
    ep_count, capacity, width = send_tokens.shape
    sems = [pltpu.SemaphoreType.DMA((2, ep_count)) for _ in range(8)]
    sems += [pltpu.SemaphoreType.DMA((ep_count,)) for _ in range(2)]
    whole = jax.ShapeDtypeStruct((ep_count, capacity, model_width), jnp.bfloat16)
    return pl.pallas_call(
        dispatch_kernel,
        out_shape=(whole, whole, jax.ShapeDtypeStruct(weights.shape, jnp.float32)),
        in_specs=[pl.BlockSpec(memory_space=pltpu.VMEM)] * 3,
        out_specs=(
            pl.BlockSpec(memory_space=pl.ANY),
            pl.BlockSpec(memory_space=pl.ANY),
            pl.BlockSpec(memory_space=pltpu.VMEM),
        ),
        scratch_shapes=sems + [pltpu.SemaphoreType.DMA((3,))],
        compiler_params=pltpu.CompilerParams(collective_id=0, has_side_effects=True),
    )(send_tokens, send_grads, weights)


def combine_kernel(
    rows_ref, product_ref, back_ref, back_product, near_buf, far_send, far_buf, last_send,
    product_near, product_sum, product_far, product_send,
    s1, r1, s2, r2, s3, r3, sw, rw, small_send, small_recv,
):
    ep_count, here, part, beside, across = partners()
    width = back_ref.shape[2]
    beside_far = (beside + lax.axis_size("tp") // 2) % lax.axis_size("tp")

    def columns(owner):
        return pl.ds(pl.multiple_of(owner * width, width), width)

    greet(ep_count, here, part, beside, across)

    def near(which, j):
        target = (here + j) % ep_count
        owner = beside_far if which == 0 else beside
        return remote(
            rows_ref.at[target, :, columns(owner)], near_buf.at[which, j],
            s1.at[which, j], r1.at[which, j], (here, beside),
        )

    def far(j):
        return remote(far_send.at[j], far_buf.at[j], s2.at[j], r2.at[j], (here, across))

    def last(j):
        peer = (here + j) % ep_count
        return remote(last_send.at[j], back_ref.at[here], s3.at[j], r3.at[j], (peer, part))

    def last_product(j):
        peer = (here + j) % ep_count
        return remote(
            product_send.at[peer], back_product.at[here], sw.at[j], rw.at[j], (peer, part)
        )

    small_near = remote(product_ref, product_near, small_send.at[0], small_recv.at[0], (here, beside))
    small_far = remote(product_sum, product_far, small_send.at[1], small_recv.at[1], (here, across))
    small_near.start()

    def launch(step, carry):
        j = (step + 1) % ep_count
        near(0, j).start()
        near(1, j).start()
        return carry

    lax.fori_loop(0, ep_count, launch, 0)
    small_near.wait_recv()
    product_sum[...] = product_ref[...] + product_near[...]
    small_far.start()

    def middle(step, carry):
        j = (step + 1) % ep_count
        near(0, j).wait_recv()
        target = (here + j) % ep_count
        mine = rows_ref[target, :, columns(across)].astype(jnp.float32)
        far_send[j] = (mine + near_buf[0, j].astype(jnp.float32)).astype(jnp.bfloat16)
        far(j).start()
        return carry

    lax.fori_loop(0, ep_count, middle, 0)
    small_far.wait_recv()
    product_send[...] = product_sum[...] + product_far[...]

    def total(j):
        near(1, j).wait_recv()
        far(j).wait_recv()
        target = (here + j) % ep_count
        mine = rows_ref[target, :, columns(part)].astype(jnp.float32)
        added = mine + near_buf[1, j].astype(jnp.float32) + far_buf[j].astype(jnp.float32)
        return added.astype(jnp.bfloat16)

    def end(j, carry):
        last_send[j] = total(j)
        last(j).start()
        last_product(j).start()
        return carry

    lax.fori_loop(1, ep_count, end, 0)
    back_ref[here] = total(0)
    back_product[here] = product_send[here]

    small_near.wait_send()
    small_far.wait_send()

    def finish(j, carry):
        near(0, j).wait_send()
        near(1, j).wait_send()
        far(j).wait_send()

        @pl.when(j >= 1)
        def _():
            last(j).wait()
            last_product(j).wait()

        return carry

    lax.fori_loop(0, ep_count, finish, 0)


def combine(rows, products, width):
    ep_count, capacity, _ = rows.shape
    one = (ep_count, capacity, width)
    small = pltpu.VMEM(products.shape, jnp.float32)
    dma = pltpu.SemaphoreType.DMA
    return pl.pallas_call(
        combine_kernel,
        out_shape=(
            jax.ShapeDtypeStruct(one, jnp.bfloat16),
            jax.ShapeDtypeStruct(products.shape, jnp.float32),
        ),
        in_specs=[pl.BlockSpec(memory_space=pltpu.VMEM)] * 2,
        out_specs=(pl.BlockSpec(memory_space=pltpu.VMEM),) * 2,
        scratch_shapes=[
            pltpu.VMEM((2,) + one, jnp.bfloat16),
            pltpu.VMEM(one, jnp.bfloat16),
            pltpu.VMEM(one, jnp.bfloat16),
            pltpu.VMEM(one, jnp.bfloat16),
            small, small, small, small,
            dma((2, ep_count)), dma((2, ep_count)),
            dma((ep_count,)), dma((ep_count,)), dma((ep_count,)), dma((ep_count,)),
            dma((ep_count,)), dma((ep_count,)), dma((2,)), dma((2,)),
        ],
        compiler_params=pltpu.CompilerParams(
            collective_id=1, has_side_effects=True, vmem_limit_bytes=48 * 1024 * 1024
        ),
    )(rows, products)


def local(tokens, routes, gate_weights, out_grad, w_gate, w_up, w_down):
    f32, bf16 = jnp.float32, jnp.bfloat16
    ep_count = lax.axis_size("ep")
    tp_count = lax.axis_size("tp")
    part = lax.axis_index("tp")
    token_count, model_width = tokens.shape
    top_count = routes.shape[1]
    experts = ep_count * w_gate.shape[0]
    capacity = token_count * top_count * 5 // (4 * experts)
    width = model_width // tp_count

    match = routes[:, :, None] == jnp.arange(experts, dtype=jnp.int32)[None, None, :]
    named = jnp.any(match, axis=1)
    before = jnp.arange(token_count)[:, None] > jnp.arange(token_count)[None, :]
    rank = jnp.dot(before.astype(bf16), named.astype(bf16), preferred_element_type=f32)
    rank = jnp.where(named, rank.astype(jnp.int32), -1)
    pick = rank.T[:, None, :] == jnp.arange(capacity, dtype=jnp.int32)[None, :, None]
    pick_flat = pick.reshape(experts * capacity, token_count).astype(bf16)
    weight_of = jnp.sum(jnp.where(match, gate_weights[:, :, None], 0.0), axis=1)
    send_weights = jnp.sum(jnp.where(pick, weight_of.T[:, None, :], 0.0), axis=2)
    sends = []
    for array in (tokens, out_grad):
        own = lax.dynamic_slice_in_dim(array, part * width, width, 1)
        picked = jnp.dot(pick_flat, own, preferred_element_type=f32).astype(bf16)
        sends.append(picked.reshape(experts, capacity, width))

    rows, grads, weights = dispatch(*sends, send_weights[:, None, :], model_width)
    row_count = ep_count * capacity
    x_rows = rows.reshape(row_count, model_width)
    dy_rows = grads.reshape(row_count, model_width)
    slot_weights = weights.reshape(row_count, 1)

    gate_pre = jnp.dot(x_rows, w_gate[0], preferred_element_type=f32)
    up_pre = jnp.dot(x_rows, w_up[0], preferred_element_type=f32)
    plain_grad = jnp.einsum("rd,fd->rf", dy_rows, w_down[0], preferred_element_type=f32)
    glu = jnp.minimum(gate_pre, clamp_limit)
    linear = jnp.clip(up_pre, -clamp_limit, clamp_limit)
    sigma = jax.nn.sigmoid(sigmoid_slope * glu)
    active = glu * sigma
    hidden = active * (linear + 1.0)
    product = jnp.sum(hidden * plain_grad, axis=1)
    hidden_grad = plain_grad * slot_weights
    slope_term = sigma + sigmoid_slope * active * (1.0 - sigma)
    gate_pre_grad = jnp.where(
        gate_pre < clamp_limit, hidden_grad * (linear + 1.0) * slope_term, 0.0
    ).astype(bf16)
    up_pre_grad = jnp.where(jnp.abs(up_pre) < clamp_limit, hidden_grad * active, 0.0).astype(bf16)
    hidden = (hidden * slot_weights).astype(bf16)

    row_term = jnp.einsum("rf,df->rd", gate_pre_grad, w_gate[0], preferred_element_type=f32)
    row_term = row_term + jnp.einsum(
        "rf,df->rd", up_pre_grad, w_up[0], preferred_element_type=f32
    )
    row_term = row_term.astype(bf16).reshape(ep_count, capacity, model_width)
    back_rows, back_products = combine(
        row_term, product.reshape(ep_count, 1, capacity), width
    )
    gate_grads = jnp.einsum("rd,rf->df", x_rows, gate_pre_grad, preferred_element_type=f32)
    up_grads = jnp.einsum("rd,rf->df", x_rows, up_pre_grad, preferred_element_type=f32)
    down_grads = jnp.einsum("rf,rd->fd", hidden, dy_rows, preferred_element_type=f32)
    token_grad = jnp.einsum(
        "rt,rw->tw", pick_flat, back_rows.reshape(row_count, width), preferred_element_type=f32
    ).astype(bf16)
    found = jnp.sum(jnp.where(pick, back_products.reshape(experts, capacity, 1), 0.0), axis=1)
    gate_grad = jnp.sum(jnp.where(match, found.T[:, None, :], 0.0), axis=2)
    return (token_grad, gate_grad, gate_grads[None], up_grads[None], down_grads[None])


def fused_kernel(
    tok_ref, grd_ref, meta_ref, gate_ref, up_ref, down_ref,
    token_out, found_out, gate_out, up_out, down_out,
    line, metas, pick_send, rows, gate_g, up_g, hid,
    near_send, near_buf, mine, own_sum, back_send, back_buf,
    z_send, z_buf, total, y_send, y_buf,
    found_loc, found_near, found_sum, found_far, found_send,
    chain_s, chain_r, xm_s, xm_r, x_s, x_r, n_s, n_r, f_s, f_r, o_s, o_r,
    c_s, c_r, b_s, b_r, z_s, z_r, y_s, y_r, sm_s, sm_r, l_s, l_r,
):
    f32, bf16 = jnp.float32, jnp.bfloat16
    ep_count, here, part, beside, across = partners()
    count = ep_count // 2
    z, x = here // 2, here % 2
    other = here + 1 - 2 * x
    plane, core = part // 2, part % 2
    capacity = rows.shape[2]
    model_width = tok_ref.shape[1]
    width = token_out.shape[1]
    token_count = tok_ref.shape[0]

    def columns(owner):
        return pl.ds(pl.multiple_of(owner * width, width), width)

    def order(i):
        high = (2 * z) // count
        paired = z * (1 - high) + (count - 1 - z) * high
        inside = (2 * paired + 4 * count - i) // (4 * count)
        step = z + ((i + 1) // 2) * (1 - 2 * (i % 2))
        rest = i * (1 - high) + (count - 1 - i) * high
        return inside * step + (1 - inside) * rest

    def chain(kind, zi, way):
        ref = metas.at[2 * zi + x] if kind == 2 else line.at[kind, zi]
        to = here + 2 - 4 * way
        return remote(ref, ref, chain_s.at[way, kind, zi], chain_r.at[kind, zi], (to, part))

    def cross_meta(zi):
        ref = metas.at[2 * zi + x]
        return remote(ref, ref, xm_s.at[zi], xm_r.at[zi], (other, part))

    def cross(kind, zi):
        return remote(
            pick_send.at[kind, zi], rows.at[kind, 2 * zi + x, :, columns(part)],
            x_s.at[kind, zi], x_r.at[kind, zi], (other, part),
        )

    def forward(kind, source, owner, sent, got, to):
        ref = rows.at[kind, source, :, columns(owner)]
        return remote(ref, ref, sent.at[kind, source], got.at[kind, source], (here, to))

    def near(kind, source):
        return forward(kind, source, part, n_s, n_r, beside)

    def far(kind, source):
        return forward(kind, source, part, f_s, f_r, across)

    def onward(kind, source):
        return forward(kind, source, across, o_s, o_r, beside)

    def pair(source):
        return remote(
            near_send.at[source], near_buf.at[source], c_s.at[source], c_r.at[source],
            (here, beside),
        )

    def cross_back(zi):
        return remote(back_send.at[zi], back_buf.at[zi], b_s.at[zi], b_r.at[zi], (other, part))

    def line_back(zi):
        return remote(z_send.at[zi], z_buf.at[z], z_s.at[zi], z_r.at[z], (2 * zi + x, part))

    def line_got(zi):
        return remote(z_send.at[zi], z_buf.at[zi], z_s.at[zi], z_r.at[zi], (2 * zi + x, part))

    last_y = remote(y_send, y_buf, y_s.at[0], y_r.at[0], (here, across))
    small_near = remote(found_loc, found_near, sm_s.at[0], sm_r.at[0], (here, beside))
    small_far = remote(found_sum, found_far, sm_s.at[1], sm_r.at[1], (here, across))

    def last_found(j):
        peer = (here + j) % ep_count
        return remote(found_send.at[peer], found_out.at[here], l_s.at[j], l_r.at[j], (peer, part))

    slots = lax.broadcasted_iota(jnp.int32, (capacity, token_count), 0).astype(f32)

    def matches(source, expert):
        return slots == metas[source, pl.ds(expert, 1), :]

    def pick(source, expert):
        return jnp.where(matches(source, expert), 1.0, 0.0).astype(bf16)

    line[0, z] = tok_ref[:, columns(part)]
    line[1, z] = grd_ref[:, columns(part)]
    metas[here] = meta_ref[...]
    greet(ep_count, here, part, beside, across)

    @pl.when(z < count - 1)
    def _():
        for kind in (2, 0, 1):
            chain(kind, z, 0).start()

    @pl.when(z > 0)
    def _():
        for kind in (2, 0, 1):
            chain(kind, z, 1).start()

    def take(kind, zi):
        chain(kind, zi, 0).wait_recv()

        @pl.when((zi < z) & (z < count - 1))
        def _():
            chain(kind, zi, 0).start()

        @pl.when((zi > z) & (z > 0))
        def _():
            chain(kind, zi, 1).start()

    def gather(i):
        zi = order(i)
        source = 2 * zi + x

        @pl.when(i >= 1)
        def _():
            take(2, zi)

        cross_meta(zi).start()
        for kind in range(2):
            @pl.when(i >= 1)
            def _():
                take(kind, zi)

            picked = jnp.dot(
                pick(source, other), line[kind, zi], preferred_element_type=f32
            )
            pick_send[kind, zi] = picked.astype(bf16)
            cross(kind, zi).start()

            @pl.when(i >= 1)
            def _():
                own = jnp.dot(pick(source, here), line[kind, zi], preferred_element_type=f32)
                rows[kind, source, :, columns(part)] = own.astype(bf16)
                far(kind, source).start()
                near(kind, source).start()

            @pl.when(i == 0)
            def _():
                whole = grd_ref if kind else tok_ref
                for q in range(model_width // width):
                    at = pl.ds(q * width, width)
                    own = jnp.dot(
                        pick(source, here), whole[:, at], preferred_element_type=f32
                    )
                    rows[kind, source, :, at] = own.astype(bf16)

    def arrive(i):
        zi = order(i)
        for kind in range(2):
            cross(kind, zi).wait_recv()
            far(kind, 2 * zi + 1 - x).start()
            near(kind, 2 * zi + 1 - x).start()
        cross_meta(zi).wait_recv()

    def hand_on(source):
        for kind in range(2):
            far(kind, source).wait_recv()
            onward(kind, source).start()

    def compute(source, local_rows):
        @pl.when(local_rows == 0)
        def _():
            for kind in range(2):
                near(kind, source).wait_recv()
                onward(kind, source).wait_recv()

        nt = (((1,), (1,)), ((), ()))
        x_rows = rows[0, source]
        gate_pre = jnp.dot(x_rows, gate_ref[...], preferred_element_type=f32)
        up_pre = jnp.dot(x_rows, up_ref[...], preferred_element_type=f32)
        plain = lax.dot_general(rows[1, source], down_ref[...], nt, preferred_element_type=f32)
        hit = matches(source, here)
        weight_row = metas[source, pl.ds(here + ep_count, 1), :]
        weight = jnp.sum(jnp.where(hit, weight_row, 0.0), axis=1, keepdims=True)
        glu = jnp.minimum(gate_pre, clamp_limit)
        linear = jnp.clip(up_pre, -clamp_limit, clamp_limit)
        sigma = jax.nn.sigmoid(sigmoid_slope * glu)
        active = glu * sigma
        hidden = active * (linear + 1.0)
        product = jnp.sum(hidden * plain, axis=1, keepdims=True)
        found_loc[source] = jnp.sum(jnp.where(hit, product, 0.0), axis=0, keepdims=True)
        hidden_grad = plain * weight
        slope_term = sigma + sigmoid_slope * active * (1.0 - sigma)
        gate_grad = jnp.where(
            gate_pre < clamp_limit, hidden_grad * (linear + 1.0) * slope_term, 0.0
        ).astype(bf16)
        up_grad = jnp.where(jnp.abs(up_pre) < clamp_limit, hidden_grad * active, 0.0).astype(bf16)
        gate_g[source] = gate_grad
        up_g[source] = up_grad
        hid[source] = (hidden * weight).astype(bf16)
        for own in range(2):
            for half in range(2):
                owner = 2 * half + (core if own else 1 - core)
                term = lax.dot_general(
                    gate_g[source], gate_ref[columns(owner), :], nt, preferred_element_type=f32
                ) + lax.dot_general(
                    up_g[source], up_ref[columns(owner), :], nt, preferred_element_type=f32
                )
                at = pl.ds(half * width, width)
                if own:
                    mine[source, :, at] = term.astype(bf16)
                else:
                    near_send[source, :, at] = term.astype(bf16)
            if not own:
                pair(source).start()

    def pair_sum(source):
        pair(source).wait_recv()
        added = mine[source].astype(f32) + near_buf[source].astype(f32)
        return added.astype(bf16)

    def merge(i):
        zi = order(i)
        source = 2 * zi + x
        cross_back(zi).wait_recv()
        tn = (((0,), (0,)), ((), ()))
        own_pick, other_pick = pick(source, here), pick(source, other)
        for half in range(2):
            at = pl.ds(half * width, width)
            added = lax.dot_general(
                own_pick, own_sum[zi, :, at], tn, preferred_element_type=f32
            ) + lax.dot_general(
                other_pick, back_buf[zi, :, at], tn, preferred_element_type=f32
            )

            @pl.when(i == 0)
            def _():
                total[:, at] = added

            @pl.when(i >= 1)
            def _():
                z_send[zi, :, at] = added.astype(bf16)

        @pl.when(i >= 1)
        def _():
            line_back(zi).start()

    def body(i, carry):
        @pl.when(i < count)
        def _():
            gather(i)

        @pl.when((i >= 2) & (i <= count))
        def _():
            hand_on(2 * order(i - 1) + x)

        @pl.when(i >= 2)
        def _():
            compute(2 * order(i - 2) + 1 - x, 0)
            own_sum[order(i - 2)] = pair_sum(2 * order(i - 2) + x)

        @pl.when(i < count)
        def _():
            arrive(i)

        @pl.when((i >= 1) & (i <= count))
        def _():
            hand_on(2 * order(i - 1) + 1 - x)
            compute(2 * order(i - 1) + x, (count - i + 1) // count)

        @pl.when(i >= 2)
        def _():
            zi = order(i - 2)
            back_send[zi] = pair_sum(2 * zi + 1 - x)
            cross_back(zi).start()

        @pl.when(i >= 3)
        def _():
            merge(i - 3)

        return carry

    lax.fori_loop(0, count + 2, body, 0)
    small_near.start()

    def weights(n, carry):
        chunk = 256
        tn = (((0,), (0,)), ((), ()))
        at = pl.ds(pl.multiple_of(n * chunk, chunk), chunk)
        flat = ep_count * capacity
        x_part = rows[0, :, :, at].reshape(flat, chunk)
        g_part = rows[1, :, :, at].reshape(flat, chunk)
        units = gate_g.shape[2]
        gate_out[at, :] = lax.dot_general(
            x_part, gate_g[...].reshape(flat, units), tn, preferred_element_type=f32
        )
        up_out[at, :] = lax.dot_general(
            x_part, up_g[...].reshape(flat, units), tn, preferred_element_type=f32
        )
        down_out[:, at] = lax.dot_general(
            hid[...].reshape(flat, units), g_part, tn, preferred_element_type=f32
        )
        return carry

    chunks = model_width // 256
    small_near.wait_recv()
    found_sum[...] = found_loc[...] + found_near[...]
    small_far.start()
    lax.fori_loop(0, chunks // 2, weights, 0)
    small_far.wait_recv()
    found_send[...] = found_sum[...] + found_far[...]
    found_out[here] = found_send[here]

    def share(j, carry):
        last_found(j).start()
        return carry

    lax.fori_loop(1, ep_count, share, 0)
    merge(count - 1)
    lax.fori_loop(chunks // 2, chunks, weights, 0)

    def add(i, carry):
        zi = order(i)
        line_got(zi).wait_recv()
        total[...] = total[...] + z_buf[zi].astype(f32)
        return carry

    lax.fori_loop(1, count, add, 0)
    y_send[...] = total[:, columns(1 - plane)].astype(bf16)
    last_y.start()
    last_y.wait_recv()
    token_out[...] = (total[:, columns(plane)] + y_buf[...].astype(f32)).astype(bf16)

    def finish(zi, carry):
        for kind in range(3):
            @pl.when((zi <= z) & (z < count - 1))
            def _():
                chain(kind, zi, 0).wait_send()

            @pl.when((zi >= z) & (z > 0))
            def _():
                chain(kind, zi, 1).wait_send()

        cross_meta(zi).wait_send()
        cross_back(zi).wait_send()
        for kind in range(2):
            cross(kind, zi).wait_send()

        @pl.when((zi < z) | (zi > z))
        def _():
            line_back(zi).wait_send()

        return carry

    lax.fori_loop(0, count, finish, 0)

    def finish_source(source, carry):
        pair(source).wait_send()

        @pl.when((source < here) | (source > here))
        def _():
            for kind in range(2):
                near(kind, source).wait_send()
                far(kind, source).wait_send()
                onward(kind, source).wait_send()

        return carry

    lax.fori_loop(0, ep_count, finish_source, 0)

    def finish_found(j, carry):
        last_found(j).wait()
        return carry

    lax.fori_loop(1, ep_count, finish_found, 0)
    last_y.wait_send()
    small_near.wait_send()
    small_far.wait_send()


def fused(tokens, grads, meta, w_gate, w_up, w_down, capacity, width):
    f32, bf16 = jnp.float32, jnp.bfloat16
    ep_count = lax.axis_size("ep")
    count = ep_count // 2
    token_count, model_width = tokens.shape
    units = w_gate.shape[1]
    vm = pltpu.VMEM
    dma = pltpu.SemaphoreType.DMA
    small = vm((ep_count, 1, token_count), f32)
    half = (capacity, 2 * width)
    scratch = [
        vm((2, count, token_count, width), bf16),
        vm((ep_count,) + meta.shape, f32),
        vm((2, count, capacity, width), bf16),
        vm((2, ep_count, capacity, model_width), bf16),
        vm((ep_count, capacity, units), bf16),
        vm((ep_count, capacity, units), bf16),
        vm((ep_count, capacity, units), bf16),
        vm((ep_count,) + half, bf16),
        vm((ep_count,) + half, bf16),
        vm((ep_count,) + half, bf16),
        vm((count,) + half, bf16),
        vm((count,) + half, bf16),
        vm((count,) + half, bf16),
        vm((count, token_count, 2 * width), bf16),
        vm((count, token_count, 2 * width), bf16),
        vm((token_count, 2 * width), f32),
        vm((token_count, width), bf16),
        vm((token_count, width), bf16),
        small, small, small, small, small,
        dma((2, 3, count)), dma((3, count)),
        dma((count,)), dma((count,)),
        dma((2, count)), dma((2, count)),
        dma((2, ep_count)), dma((2, ep_count)),
        dma((2, ep_count)), dma((2, ep_count)),
        dma((2, ep_count)), dma((2, ep_count)),
        dma((ep_count,)), dma((ep_count,)),
        dma((count,)), dma((count,)),
        dma((count,)), dma((count,)),
        dma((1,)), dma((1,)), dma((2,)), dma((2,)),
        dma((ep_count,)), dma((ep_count,)),
    ]
    return pl.pallas_call(
        fused_kernel,
        out_shape=(
            jax.ShapeDtypeStruct((token_count, width), bf16),
            jax.ShapeDtypeStruct((ep_count, 1, token_count), f32),
            jax.ShapeDtypeStruct((model_width, units), f32),
            jax.ShapeDtypeStruct((model_width, units), f32),
            jax.ShapeDtypeStruct((units, model_width), f32),
        ),
        in_specs=[pl.BlockSpec(memory_space=pltpu.VMEM)] * 6,
        out_specs=(pl.BlockSpec(memory_space=pltpu.VMEM),) * 5,
        scratch_shapes=scratch,
        compiler_params=pltpu.CompilerParams(
            collective_id=2, has_side_effects=True, vmem_limit_bytes=60 * 1024 * 1024
        ),
    )(tokens, grads, meta, w_gate, w_up, w_down)


def gathered(tokens, routes, gate_weights, out_grad, w_gate, w_up, w_down):
    f32, bf16 = jnp.float32, jnp.bfloat16
    ep_count = lax.axis_size("ep")
    token_count, model_width = tokens.shape
    capacity = token_count * routes.shape[1] * 5 // (4 * ep_count)
    width = model_width // lax.axis_size("tp")
    by_expert = routes.T
    match = by_expert[None, :, :] == jnp.arange(ep_count, dtype=jnp.int32)[:, None, None]
    named = jnp.any(match, axis=1)
    before = jnp.arange(token_count)[:, None] < jnp.arange(token_count)[None, :]
    rank = jnp.dot(named.astype(bf16), before.astype(bf16), preferred_element_type=f32)
    rank = jnp.where(named, rank, -1.0)
    weight_of = jnp.sum(jnp.where(match, gate_weights.T[None, :, :], 0.0), axis=1)
    meta = jnp.concatenate([rank, weight_of], axis=0)
    token_grad, found, gate_grads, up_grads, down_grads = fused(
        tokens, out_grad, meta, w_gate[0], w_up[0], w_down[0], capacity, width
    )
    gate_grad = jnp.sum(jnp.where(match, found, 0.0), axis=0).T
    return (token_grad, gate_grad, gate_grads[None], up_grads[None], down_grads[None])


def chosen(*args):
    tokens, w_gate = args[0], args[4]
    block_bytes = lax.axis_size("ep") * tokens.size * 2
    if block_bytes <= 16 * 1024 * 1024 and w_gate.shape[0] == 1:
        return gathered(*args)
    return local(*args)


def solution(mesh):
    return jax.shard_map(
        chosen,
        mesh=mesh,
        in_specs=(
            P("ep", None),
            P("ep", None),
            P("ep", None),
            P("ep", None),
            P("ep", None, "tp"),
            P("ep", None, "tp"),
            P("ep", "tp", None),
        ),
        out_specs=(
            P("ep", "tp"),
            P("ep", None),
            P("ep", None, "tp"),
            P("ep", None, "tp"),
            P("ep", "tp", None),
        ),
        check_vma=False,
    )
```

```python
import jax
import jax.numpy as jnp
from jax import lax
from jax.experimental import pallas as pl
from jax.experimental.pallas import tpu as pltpu
from jax.sharding import PartitionSpec as P

clamp_limit = 7.0
sigmoid_slope = 1.702
MESH = pl.DeviceIdType.MESH
far_step = 2


def partners():
    ep_count = lax.axis_size("ep")
    tp_count = lax.axis_size("tp")
    here = lax.axis_index("ep")
    part = lax.axis_index("tp")
    beside = part + 1 - 2 * (part % 2)
    across = (part + tp_count // 2) % tp_count
    return ep_count, here, part, beside, across


def greet(ep_count, here, part, beside, across):
    barrier = pltpu.get_barrier_semaphore()
    pl.semaphore_signal(barrier, inc=1, device_id=(here, beside), device_id_type=MESH)
    pl.semaphore_signal(barrier, inc=1, device_id=(here, across), device_id_type=MESH)

    def call(j, carry):
        peer = (here + j) % ep_count
        pl.semaphore_signal(barrier, inc=1, device_id=(peer, part), device_id_type=MESH)
        return carry

    lax.fori_loop(1, ep_count, call, 0)
    pl.semaphore_wait(barrier, ep_count + 1)


def remote(src, dst, sent, got, device):
    return pltpu.make_async_remote_copy(
        src_ref=src, dst_ref=dst, send_sem=sent, recv_sem=got, device_id=device, device_id_type=MESH
    )


def dispatch_kernel(
    token_ref, grad_ref, weight_ref, token_rows, grad_rows, weights_out,
    s1, r1, s2, r2, s3, r3, s4, r4, sw, rw, own_sem,
):
    ep_count, here, part, beside, across = partners()
    width = token_ref.shape[2]
    pairs = ((0, token_ref, token_rows), (1, grad_ref, grad_rows))

    def block(rows_ref, source, owner):
        columns = pl.ds(pl.multiple_of(owner * width, width), width)
        return rows_ref.at[source, :, columns]

    greet(ep_count, here, part, beside, across)

    def first(j):
        peer = (here + j) % ep_count
        return [
            remote(send.at[peer], block(rows, here, part), s1.at[i, j], r1.at[i, j], (peer, part))
            for i, send, rows in pairs
        ]

    def first_weight(j):
        peer = (here + j) % ep_count
        return remote(
            weight_ref.at[peer], weights_out.at[here], sw.at[j], rw.at[j], (peer, part)
        )

    def forward(j, owner, sent, got, to):
        source = (here + ep_count - j) % ep_count
        return [
            remote(
                block(rows, source, owner), block(rows, source, owner),
                sent.at[i, j], got.at[i, j], (here, to),
            )
            for i, _, rows in pairs
        ]

    def near(j):
        return forward(j, part, s2, r2, beside)

    def far(j):
        return forward(j, part, s3, r3, across)

    def onward(j):
        return forward(j, across, s4, r4, beside)

    owns = [
        pltpu.make_async_copy(send.at[here], block(rows, here, part), own_sem.at[i])
        for i, send, rows in pairs
    ]
    owns.append(pltpu.make_async_copy(weight_ref.at[here], weights_out.at[here], own_sem.at[2]))
    for copy in owns:
        copy.start()

    def launch(j, carry):
        first_weight(j).start()
        for copy in first(j):
            copy.start()
        return carry

    lax.fori_loop(1, ep_count, launch, 0)
    for copy in owns:
        copy.wait()
    for copy in far(0) + near(0):
        copy.start()

    def pass_on(j, carry):
        @pl.when(j < ep_count)
        def _():
            for i in range(2):
                first(j)[i].wait_recv()
                far(j)[i].start()
                near(j)[i].start()

        @pl.when(j >= 2)
        def _():
            for i in range(2):
                far(j - 2)[i].wait_recv()
                onward(j - 2)[i].start()

        return carry

    lax.fori_loop(1, ep_count + 2, pass_on, 0)

    def finish(j, carry):
        for i in range(2):
            near(j)[i].wait()
            onward(j)[i].wait()
            far(j)[i].wait_send()

        @pl.when(j >= 1)
        def _():
            for copy in first(j):
                copy.wait_send()
            first_weight(j).wait()

        return carry

    lax.fori_loop(0, ep_count, finish, 0)


def dispatch(send_tokens, send_grads, weights, model_width):
    ep_count, capacity, width = send_tokens.shape
    sems = [pltpu.SemaphoreType.DMA((2, ep_count)) for _ in range(8)]
    sems += [pltpu.SemaphoreType.DMA((ep_count,)) for _ in range(2)]
    whole = jax.ShapeDtypeStruct((ep_count, capacity, model_width), jnp.bfloat16)
    return pl.pallas_call(
        dispatch_kernel,
        out_shape=(whole, whole, jax.ShapeDtypeStruct(weights.shape, jnp.float32)),
        in_specs=[pl.BlockSpec(memory_space=pltpu.VMEM)] * 3,
        out_specs=(
            pl.BlockSpec(memory_space=pl.ANY),
            pl.BlockSpec(memory_space=pl.ANY),
            pl.BlockSpec(memory_space=pltpu.VMEM),
        ),
        scratch_shapes=sems + [pltpu.SemaphoreType.DMA((3,))],
        compiler_params=pltpu.CompilerParams(collective_id=0, has_side_effects=True),
    )(send_tokens, send_grads, weights)


def combine_kernel(
    rows_ref, product_ref, back_ref, back_product, near_buf, far_send, far_buf, last_send,
    product_near, product_sum, product_far, product_send,
    s1, r1, s2, r2, s3, r3, sw, rw, small_send, small_recv,
):
    ep_count, here, part, beside, across = partners()
    width = back_ref.shape[2]
    beside_far = (beside + lax.axis_size("tp") // 2) % lax.axis_size("tp")

    def columns(owner):
        return pl.ds(pl.multiple_of(owner * width, width), width)

    greet(ep_count, here, part, beside, across)

    def near(which, j):
        target = (here + j) % ep_count
        owner = beside_far if which == 0 else beside
        return remote(
            rows_ref.at[target, :, columns(owner)], near_buf.at[which, j],
            s1.at[which, j], r1.at[which, j], (here, beside),
        )

    def far(j):
        return remote(far_send.at[j], far_buf.at[j], s2.at[j], r2.at[j], (here, across))

    def last(j):
        peer = (here + j) % ep_count
        return remote(last_send.at[j], back_ref.at[here], s3.at[j], r3.at[j], (peer, part))

    def last_product(j):
        peer = (here + j) % ep_count
        return remote(
            product_send.at[peer], back_product.at[here], sw.at[j], rw.at[j], (peer, part)
        )

    small_near = remote(product_ref, product_near, small_send.at[0], small_recv.at[0], (here, beside))
    small_far = remote(product_sum, product_far, small_send.at[1], small_recv.at[1], (here, across))
    small_near.start()

    def launch(step, carry):
        j = (step + 1) % ep_count
        near(0, j).start()
        near(1, j).start()
        return carry

    lax.fori_loop(0, ep_count, launch, 0)
    small_near.wait_recv()
    product_sum[...] = product_ref[...] + product_near[...]
    small_far.start()

    def middle(step, carry):
        j = (step + 1) % ep_count
        near(0, j).wait_recv()
        target = (here + j) % ep_count
        mine = rows_ref[target, :, columns(across)].astype(jnp.float32)
        far_send[j] = (mine + near_buf[0, j].astype(jnp.float32)).astype(jnp.bfloat16)
        far(j).start()
        return carry

    lax.fori_loop(0, ep_count, middle, 0)
    small_far.wait_recv()
    product_send[...] = product_sum[...] + product_far[...]

    def total(j):
        near(1, j).wait_recv()
        far(j).wait_recv()
        target = (here + j) % ep_count
        mine = rows_ref[target, :, columns(part)].astype(jnp.float32)
        added = mine + near_buf[1, j].astype(jnp.float32) + far_buf[j].astype(jnp.float32)
        return added.astype(jnp.bfloat16)

    def end(j, carry):
        last_send[j] = total(j)
        last(j).start()
        last_product(j).start()
        return carry

    lax.fori_loop(1, ep_count, end, 0)
    back_ref[here] = total(0)
    back_product[here] = product_send[here]

    small_near.wait_send()
    small_far.wait_send()

    def finish(j, carry):
        near(0, j).wait_send()
        near(1, j).wait_send()
        far(j).wait_send()

        @pl.when(j >= 1)
        def _():
            last(j).wait()
            last_product(j).wait()

        return carry

    lax.fori_loop(0, ep_count, finish, 0)


def combine(rows, products, width):
    ep_count, capacity, _ = rows.shape
    one = (ep_count, capacity, width)
    small = pltpu.VMEM(products.shape, jnp.float32)
    dma = pltpu.SemaphoreType.DMA
    return pl.pallas_call(
        combine_kernel,
        out_shape=(
            jax.ShapeDtypeStruct(one, jnp.bfloat16),
            jax.ShapeDtypeStruct(products.shape, jnp.float32),
        ),
        in_specs=[pl.BlockSpec(memory_space=pltpu.VMEM)] * 2,
        out_specs=(pl.BlockSpec(memory_space=pltpu.VMEM),) * 2,
        scratch_shapes=[
            pltpu.VMEM((2,) + one, jnp.bfloat16),
            pltpu.VMEM(one, jnp.bfloat16),
            pltpu.VMEM(one, jnp.bfloat16),
            pltpu.VMEM(one, jnp.bfloat16),
            small, small, small, small,
            dma((2, ep_count)), dma((2, ep_count)),
            dma((ep_count,)), dma((ep_count,)), dma((ep_count,)), dma((ep_count,)),
            dma((ep_count,)), dma((ep_count,)), dma((2,)), dma((2,)),
        ],
        compiler_params=pltpu.CompilerParams(
            collective_id=1, has_side_effects=True, vmem_limit_bytes=48 * 1024 * 1024
        ),
    )(rows, products)


def local(tokens, routes, gate_weights, out_grad, w_gate, w_up, w_down):
    f32, bf16 = jnp.float32, jnp.bfloat16
    ep_count = lax.axis_size("ep")
    tp_count = lax.axis_size("tp")
    part = lax.axis_index("tp")
    token_count, model_width = tokens.shape
    top_count = routes.shape[1]
    experts = ep_count * w_gate.shape[0]
    capacity = token_count * top_count * 5 // (4 * experts)
    width = model_width // tp_count

    match = routes[:, :, None] == jnp.arange(experts, dtype=jnp.int32)[None, None, :]
    named = jnp.any(match, axis=1)
    before = jnp.arange(token_count)[:, None] > jnp.arange(token_count)[None, :]
    rank = jnp.dot(before.astype(bf16), named.astype(bf16), preferred_element_type=f32)
    rank = jnp.where(named, rank.astype(jnp.int32), -1)
    pick = rank.T[:, None, :] == jnp.arange(capacity, dtype=jnp.int32)[None, :, None]
    pick_flat = pick.reshape(experts * capacity, token_count).astype(bf16)
    weight_of = jnp.sum(jnp.where(match, gate_weights[:, :, None], 0.0), axis=1)
    send_weights = jnp.sum(jnp.where(pick, weight_of.T[:, None, :], 0.0), axis=2)
    sends = []
    for array in (tokens, out_grad):
        own = lax.dynamic_slice_in_dim(array, part * width, width, 1)
        picked = jnp.dot(pick_flat, own, preferred_element_type=f32).astype(bf16)
        sends.append(picked.reshape(experts, capacity, width))

    rows, grads, weights = dispatch(*sends, send_weights[:, None, :], model_width)
    row_count = ep_count * capacity
    x_rows = rows.reshape(row_count, model_width)
    dy_rows = grads.reshape(row_count, model_width)
    slot_weights = weights.reshape(row_count, 1)

    gate_pre = jnp.dot(x_rows, w_gate[0], preferred_element_type=f32)
    up_pre = jnp.dot(x_rows, w_up[0], preferred_element_type=f32)
    plain_grad = jnp.einsum("rd,fd->rf", dy_rows, w_down[0], preferred_element_type=f32)
    glu = jnp.minimum(gate_pre, clamp_limit)
    linear = jnp.clip(up_pre, -clamp_limit, clamp_limit)
    sigma = jax.nn.sigmoid(sigmoid_slope * glu)
    active = glu * sigma
    hidden = active * (linear + 1.0)
    product = jnp.sum(hidden * plain_grad, axis=1)
    hidden_grad = plain_grad * slot_weights
    slope_term = sigma + sigmoid_slope * active * (1.0 - sigma)
    gate_pre_grad = jnp.where(
        gate_pre < clamp_limit, hidden_grad * (linear + 1.0) * slope_term, 0.0
    ).astype(bf16)
    up_pre_grad = jnp.where(jnp.abs(up_pre) < clamp_limit, hidden_grad * active, 0.0).astype(bf16)
    hidden = (hidden * slot_weights).astype(bf16)

    row_term = jnp.einsum("rf,df->rd", gate_pre_grad, w_gate[0], preferred_element_type=f32)
    row_term = row_term + jnp.einsum(
        "rf,df->rd", up_pre_grad, w_up[0], preferred_element_type=f32
    )
    row_term = row_term.astype(bf16).reshape(ep_count, capacity, model_width)
    back_rows, back_products = combine(
        row_term, product.reshape(ep_count, 1, capacity), width
    )
    gate_grads = jnp.einsum("rd,rf->df", x_rows, gate_pre_grad, preferred_element_type=f32)
    up_grads = jnp.einsum("rd,rf->df", x_rows, up_pre_grad, preferred_element_type=f32)
    down_grads = jnp.einsum("rf,rd->fd", hidden, dy_rows, preferred_element_type=f32)
    token_grad = jnp.einsum(
        "rt,rw->tw", pick_flat, back_rows.reshape(row_count, width), preferred_element_type=f32
    ).astype(bf16)
    found = jnp.sum(jnp.where(pick, back_products.reshape(experts, capacity, 1), 0.0), axis=1)
    gate_grad = jnp.sum(jnp.where(match, found.T[:, None, :], 0.0), axis=2)
    return (token_grad, gate_grad, gate_grads[None], up_grads[None], down_grads[None])


def fused_kernel(
    tok_hbm, grd_hbm, route_hbm, share_hbm, gate_hbm, up_hbm, down_hbm,
    token_out, found_out, gate_out, up_out, down_out,
    tok_ref, grd_ref, route_ref, share_ref, gate_ref, up_ref, down_ref, line, metas, pick_send, pick_extra, rows, gate_g, up_g, hid,
    near_send, near_buf, mine, own_sum, back_send, back_buf,
    half_send, half_buf, z_send, z_buf, total, total_half, y_send, y_buf,
    found_loc, found_near, found_sum, found_far, found_send,
    chain_s, chain_r, xm_s, xm_r, x_s, x_r, e_s, e_r, n_s, n_r, f_s, f_r, o_s, o_r,
    c_s, c_r, h_s, h_r, b_s, b_r, z_s, z_r, y_s, y_r, sm_s, sm_r, l_s, l_r, in_s,
):
    f32, bf16 = jnp.float32, jnp.bfloat16
    ep_count, here, part, beside, across = partners()
    count = ep_count // 2
    z, x = here // 2, here % 2
    other = here + 1 - 2 * x
    plane, core = part // 2, part % 2
    capacity = rows.shape[2]
    model_width = tok_ref.shape[1]
    width = token_out.shape[1]
    token_count = tok_ref.shape[0]

    def columns(owner):
        return pl.ds(pl.multiple_of(owner * width, width), width)

    def order(i):
        mixed, bit = 0, 1
        while bit < count:
            mixed = mixed + ((z // bit + i // bit) % 2) * bit
            bit = 2 * bit
        return mixed

    def chain(kind, zi, way):
        ref = metas.at[2 * zi + x] if kind == 2 else line.at[kind, zi]
        to = here + 2 - 4 * way
        return remote(ref, ref, chain_s.at[way, kind, zi], chain_r.at[kind, zi], (to, part))

    def cross_meta(zi):
        ref = metas.at[2 * zi + x]
        return remote(ref, ref, xm_s.at[zi], xm_r.at[zi], (other, part))

    def cross(kind, zi):
        return remote(
            pick_send.at[kind, zi], rows.at[kind, 2 * zi + x, :, columns(part)],
            x_s.at[kind, zi], x_r.at[kind, zi], (other, part),
        )

    def cross_extra():
        return remote(
            pick_extra, rows.at[1, here, :, columns(across)],
            e_s.at[0], e_r.at[0], (other, part),
        )

    def forward(kind, source, owner, sent, got, to):
        ref = rows.at[kind, source, :, columns(owner)]
        return remote(ref, ref, sent.at[kind, source], got.at[kind, source], (here, to))

    def near(kind, source):
        return forward(kind, source, part, n_s, n_r, beside)

    def far(kind, source):
        return forward(kind, source, part, f_s, f_r, across)

    def onward(kind, source):
        return forward(kind, source, across, o_s, o_r, beside)

    def pair(source):
        return remote(
            near_send.at[source], near_buf.at[source], c_s.at[source], c_r.at[source],
            (here, beside),
        )

    def half_over(source):
        return remote(
            half_send.at[source], half_buf.at[source], h_s.at[source], h_r.at[source],
            (here, across),
        )

    def is_far(zi):
        return order(zi) >= far_step

    def cut(ref, zi, small):
        return ref.at[zi, :, pl.ds(0, width)] if small else ref.at[zi]

    def cross_back(zi, small):
        return remote(
            cut(back_send, zi, small), cut(back_buf, zi, small),
            b_s.at[zi], b_r.at[zi], (other, part),
        )

    def line_back(zi, small):
        return remote(
            cut(z_send, zi, small), cut(z_buf, z, small),
            z_s.at[zi], z_r.at[z], (2 * zi + x, part),
        )

    def line_got(zi, small):
        return remote(
            cut(z_send, zi, small), cut(z_buf, zi, small),
            z_s.at[zi], z_r.at[zi], (2 * zi + x, part),
        )

    def either(zi, act):
        @pl.when(is_far(zi))
        def _():
            act(True)

        @pl.when(jnp.logical_not(is_far(zi)))
        def _():
            act(False)

    last_y = remote(y_send, y_buf, y_s.at[0], y_r.at[0], (here, across))
    small_near = remote(found_loc, found_near, sm_s.at[0], sm_r.at[0], (here, beside))
    small_far = remote(found_sum, found_far, sm_s.at[1], sm_r.at[1], (here, across))

    def last_found(j):
        peer = (here + j) % ep_count
        return remote(found_send.at[peer], found_out.at[here], l_s.at[j], l_r.at[j], (peer, part))

    slots = lax.broadcasted_iota(jnp.int32, (capacity, token_count), 0).astype(f32)

    def matches(source, expert):
        return slots == metas[source, pl.ds(expert, 1), :]

    def pick(source, expert):
        return jnp.where(matches(source, expert), 1.0, 0.0).astype(bf16)

    barrier = pltpu.get_barrier_semaphore()
    pl.semaphore_signal(barrier, inc=1, device_id=(here, beside), device_id_type=MESH)
    pl.semaphore_signal(barrier, inc=1, device_id=(here, across), device_id_type=MESH)

    def hail(j, carry):
        peer = (here + j) % ep_count
        pl.semaphore_signal(barrier, inc=1, device_id=(peer, part), device_id_type=MESH)
        return carry

    lax.fori_loop(1, ep_count, hail, 0)
    loads = [
        pltpu.make_async_copy(src, dst, in_s.at[n])
        for n, (src, dst) in enumerate((
            (route_hbm, route_ref), (share_hbm, share_ref),
            (tok_hbm.at[:, columns(part)], line.at[0, z]),
            (grd_hbm.at[:, columns(part)], line.at[1, z]),
            (tok_hbm, tok_ref), (grd_hbm, grd_ref),
            (gate_hbm, gate_ref), (up_hbm, up_ref), (down_hbm, down_ref),
        ))
    ]
    for load in loads:
        load.start()
    total_half[...] = jnp.zeros(total_half.shape, f32)
    experts = lax.broadcasted_iota(jnp.int32, (ep_count, token_count), 0)
    earlier = lax.broadcasted_iota(jnp.int32, (token_count, token_count), 0)
    later = lax.broadcasted_iota(jnp.int32, (token_count, token_count), 1)
    before = jnp.where(earlier < later, 1.0, 0.0).astype(bf16)
    loads[0].wait()
    loads[1].wait()
    named = jnp.zeros((ep_count, token_count), f32)
    weight_of = jnp.zeros((ep_count, token_count), f32)
    for k in range(route_ref.shape[0]):
        chosen_here = route_ref[pl.ds(k, 1), :] == experts
        named = named + jnp.where(chosen_here, 1.0, 0.0)
        weight_of = weight_of + jnp.where(chosen_here, share_ref[pl.ds(k, 1), :], 0.0)
    rank = jnp.dot(named.astype(bf16), before, preferred_element_type=f32)
    metas[here, pl.ds(0, ep_count), :] = jnp.where(named > 0.0, rank, -1.0)
    metas[here, pl.ds(ep_count, ep_count), :] = weight_of
    loads[2].wait()
    loads[3].wait()
    pl.semaphore_wait(barrier, ep_count + 1)

    @pl.when(z < count - 1)
    def _():
        for kind in (2, 0, 1):
            chain(kind, z, 0).start()

    @pl.when(z > 0)
    def _():
        for kind in (2, 0, 1):
            chain(kind, z, 1).start()

    def take(kind, zi):
        chain(kind, zi, 0).wait_recv()

        @pl.when((zi < z) & (z < count - 1))
        def _():
            chain(kind, zi, 0).start()

        @pl.when((zi > z) & (z > 0))
        def _():
            chain(kind, zi, 1).start()

    def is_early(i):
        return (i >= far_step) & ((order(i) - z) * (order(i) - z) == 1)

    def relay(kind):
        def one(i, carry):
            @pl.when(is_early(i))
            def _():
                if kind == 0:
                    take(2, order(i))
                take(kind, order(i))

            return carry

        lax.fori_loop(far_step, count, one, 0)

    def picks(kind, i):
        zi = order(i)
        source = 2 * zi + x

        @pl.when((i >= 1) & jnp.logical_not(is_early(i)))
        def _():
            if kind == 0:
                take(2, zi)
            take(kind, zi)

        if kind == 0:
            cross_meta(zi).start()
        picked = jnp.dot(pick(source, other), line[kind, zi], preferred_element_type=f32)
        pick_send[kind, zi] = picked.astype(bf16)
        cross(kind, zi).start()

        @pl.when(i >= 1)
        def _():
            own = jnp.dot(pick(source, here), line[kind, zi], preferred_element_type=f32)
            rows[kind, source, :, columns(part)] = own.astype(bf16)
            far(kind, source).start()
            near(kind, source).start()

    def local_picks():
        loads[4].wait()
        loads[5].wait()
        extra = jnp.dot(
            pick(here, other), grd_ref[:, columns(across)], preferred_element_type=f32
        )
        pick_extra[...] = extra.astype(bf16)
        cross_extra().start()
        for kind, whole in enumerate((tok_ref, grd_ref)):
            for q in range(model_width // width):
                at = pl.ds(q * width, width)
                own = jnp.dot(pick(here, here), whole[:, at], preferred_element_type=f32)
                rows[kind, here, :, at] = own.astype(bf16)

    def arrive(kind, i):
        source = 2 * order(i) + 1 - x
        cross(kind, order(i)).wait_recv()
        if kind == 0:
            far(kind, source).start()
        else:
            @pl.when(i >= 1)
            def _():
                far(kind, source).start()

        near(kind, source).start()

        if kind == 1:
            cross_meta(order(i)).wait_recv()

    def hand_on_first():
        far(0, other).wait_recv()
        onward(0, other).start()
        cross_extra().wait_recv()
        onward(1, other).start()

    def hand_on(source):
        for kind in range(2):
            far(kind, source).wait_recv()
            onward(kind, source).start()

    def compute(source, local_rows):
        @pl.when(local_rows == 0)
        def _():
            for kind in range(2):
                near(kind, source).wait_recv()
                onward(kind, source).wait_recv()

        nt = (((1,), (1,)), ((), ()))
        x_rows = rows[0, source]
        gate_pre = jnp.dot(x_rows, gate_ref[...], preferred_element_type=f32)
        up_pre = jnp.dot(x_rows, up_ref[...], preferred_element_type=f32)
        plain = lax.dot_general(rows[1, source], down_ref[...], nt, preferred_element_type=f32)
        hit = matches(source, here)
        weight_row = metas[source, pl.ds(here + ep_count, 1), :]
        weight = jnp.sum(jnp.where(hit, weight_row, 0.0), axis=1, keepdims=True)
        glu = jnp.minimum(gate_pre, clamp_limit)
        linear = jnp.clip(up_pre, -clamp_limit, clamp_limit)
        sigma = jax.nn.sigmoid(sigmoid_slope * glu)
        active = glu * sigma
        hidden = active * (linear + 1.0)
        product = jnp.sum(hidden * plain, axis=1, keepdims=True)
        found_loc[source] = jnp.sum(jnp.where(hit, product, 0.0), axis=0, keepdims=True)
        hidden_grad = plain * weight
        slope_term = sigma + sigmoid_slope * active * (1.0 - sigma)
        gate_grad = jnp.where(
            gate_pre < clamp_limit, hidden_grad * (linear + 1.0) * slope_term, 0.0
        ).astype(bf16)
        up_grad = jnp.where(jnp.abs(up_pre) < clamp_limit, hidden_grad * active, 0.0).astype(bf16)
        gate_g[source] = gate_grad
        up_g[source] = up_grad
        hid[source] = (hidden * weight).astype(bf16)
        for own in range(2):
            for half in range(2):
                owner = 2 * half + (core if own else 1 - core)
                term = lax.dot_general(
                    gate_g[source], gate_ref[columns(owner), :], nt, preferred_element_type=f32
                ) + lax.dot_general(
                    up_g[source], up_ref[columns(owner), :], nt, preferred_element_type=f32
                )
                at = pl.ds(half * width, width)
                if own:
                    mine[source, :, at] = term.astype(bf16)
                else:
                    near_send[source, :, at] = term.astype(bf16)
            if not own:
                pair(source).start()

    def pair_sum(source, zi, own):
        pair(source).wait_recv()

        def act(small):
            if small:
                at = columns(1 - plane)
                added = mine[source, :, at].astype(f32) + near_buf[source, :, at].astype(f32)
                half_send[source] = added.astype(bf16)
                half_over(source).start()
                return
            added = (mine[source].astype(f32) + near_buf[source].astype(f32)).astype(bf16)
            if own:
                own_sum[zi] = added
            else:
                back_send[zi] = added
                cross_back(zi, False).start()

        either(zi, act)

    def half_sum(source, zi, own):
        @pl.when(is_far(zi))
        def _():
            half_over(source).wait_recv()
            at = columns(plane)
            added = mine[source, :, at].astype(f32) + near_buf[source, :, at].astype(f32)
            added = (added + half_buf[source].astype(f32)).astype(bf16)
            if own:
                own_sum[zi, :, pl.ds(0, width)] = added
            else:
                back_send[zi, :, pl.ds(0, width)] = added
                cross_back(zi, True).start()

    def merge(i):
        zi = order(i)
        source = 2 * zi + x
        tn = (((0,), (0,)), ((), ()))

        def act(small):
            cross_back(zi, small).wait_recv()
            for half in range(1 if small else 2):
                at = pl.ds(half * width, width)
                added = lax.dot_general(
                    pick(source, here), own_sum[zi, :, at], tn, preferred_element_type=f32
                ) + lax.dot_general(
                    pick(source, other), back_buf[zi, :, at], tn, preferred_element_type=f32
                )
                if small:
                    z_send[zi, :, at] = added.astype(bf16)
                else:
                    @pl.when(i == 0)
                    def _():
                        total[:, at] = added

                    @pl.when(i >= 1)
                    def _():
                        z_send[zi, :, at] = added.astype(bf16)

            @pl.when(i >= 1)
            def _():
                line_back(zi, small).start()

        either(zi, act)

    def own_at(i):
        return 2 * order(i) + x

    def other_at(i):
        return 2 * order(i) + 1 - x

    last = count + 1

    def body(i, carry):
        @pl.when(i == count - 1)
        def _():
            pair_sum(other_at(0), order(0), False)

        @pl.when((i >= 1) & (i <= count))
        def _():
            arrive(0, i - 1)

        @pl.when(i == 2)
        def _():
            hand_on_first()

        @pl.when(i >= 3)
        def _():
            hand_on(other_at(i - 2))

        @pl.when(i >= 2)
        def _():
            compute(other_at(i - 2), 0)

        @pl.when(i < count)
        def _():
            picks(0, i)

        @pl.when(i == 1)
        def _():
            relay(0)

        @pl.when((i >= 1) & (i <= count))
        def _():
            arrive(1, i - 1)

        @pl.when((i >= 2) & (i <= count))
        def _():
            hand_on(own_at(i - 1))

        @pl.when(i < count)
        def _():
            picks(1, i)

        @pl.when(i == 1)
        def _():
            relay(1)

        @pl.when(i == 0)
        def _():
            local_picks()
            for load in loads[6:]:
                load.wait()

        @pl.when((i == 0) | ((i >= 2) & (i <= count)))
        def _():
            step = i - (i + count - 1) // count
            compute(own_at(step), 1 - (step + count - 1) // count)

        @pl.when(i == last)
        def _():
            small_near.start()
            merge(0)
            merge(1)
            half_sum(other_at(count - 2), order(count - 2), False)
            lax.fori_loop(0, chunks // 4, weights, 0)

        @pl.when(i == 1)
        def _():
            pair_sum(own_at(0), order(0), True)

        @pl.when((i >= 2) & (i <= count))
        def _():
            @pl.when(i >= 3)
            def _():
                pair_sum(other_at(i - 2), order(i - 2), False)

            pair_sum(own_at(i - 1), order(i - 1), True)

        return carry

    def weights(n, carry):
        chunk = 256
        tn = (((0,), (0,)), ((), ()))
        at = pl.ds(pl.multiple_of(n * chunk, chunk), chunk)
        flat = ep_count * capacity
        x_part = rows[0, :, :, at].reshape(flat, chunk)
        g_part = rows[1, :, :, at].reshape(flat, chunk)
        units = gate_g.shape[2]
        gate_out[at, :] = lax.dot_general(
            x_part, gate_g[...].reshape(flat, units), tn, preferred_element_type=f32
        )
        up_out[at, :] = lax.dot_general(
            x_part, up_g[...].reshape(flat, units), tn, preferred_element_type=f32
        )
        down_out[:, at] = lax.dot_general(
            hid[...].reshape(flat, units), g_part, tn, preferred_element_type=f32
        )
        return carry

    chunks = model_width // 256
    lax.fori_loop(0, last + 1, body, 0)
    pair_sum(other_at(count - 1), order(count - 1), False)
    half_sum(own_at(count - 2), order(count - 2), True)
    half_sum(own_at(count - 1), order(count - 1), True)
    merge(count - 2)
    small_near.wait_recv()
    found_sum[...] = found_loc[...] + found_near[...]
    small_far.start()
    lax.fori_loop(chunks // 4, chunks // 2, weights, 0)
    half_sum(other_at(count - 1), order(count - 1), False)
    small_far.wait_recv()
    found_send[...] = found_sum[...] + found_far[...]
    found_out[here] = found_send[here]

    def share(j, carry):
        last_found(j).start()
        return carry

    lax.fori_loop(1, ep_count, share, 0)
    lax.fori_loop(chunks // 2, chunks, weights, 0)
    merge(count - 1)

    def add(i, carry):
        zi = order(i)

        @pl.when(jnp.logical_not(is_far(zi)))
        def _():
            line_got(zi, False).wait_recv()
            total[...] = total[...] + z_buf[zi].astype(f32)

        return carry

    def add_far(i, carry):
        zi = order(i)

        @pl.when(is_far(zi))
        def _():
            line_got(zi, True).wait_recv()
            total_half[...] = total_half[...] + z_buf[zi, :, pl.ds(0, width)].astype(f32)

        return carry

    lax.fori_loop(1, count, add, 0)
    y_send[...] = total[:, columns(1 - plane)].astype(bf16)
    last_y.start()
    lax.fori_loop(1, count, add_far, 0)
    last_y.wait_recv()
    token_out[...] = (
        total[:, columns(plane)] + total_half[...] + y_buf[...].astype(f32)
    ).astype(bf16)

    def finish(zi, carry):
        for kind in range(3):
            @pl.when((zi <= z) & (z < count - 1))
            def _():
                chain(kind, zi, 0).wait_send()

            @pl.when((zi >= z) & (z > 0))
            def _():
                chain(kind, zi, 1).wait_send()

        cross_meta(zi).wait_send()
        either(zi, lambda small: cross_back(zi, small).wait_send())
        for kind in range(2):
            cross(kind, zi).wait_send()

        @pl.when((zi < z) | (zi > z))
        def _():
            either(zi, lambda small: line_back(zi, small).wait_send())

        return carry

    lax.fori_loop(0, count, finish, 0)

    def finish_source(source, carry):
        pair(source).wait_send()

        @pl.when(is_far(source // 2))
        def _():
            half_over(source).wait_send()

        @pl.when((source < here) | (source > here))
        def _():
            for kind in range(2):
                near(kind, source).wait_send()
                onward(kind, source).wait_send()

        @pl.when((source < here) | (source > here))
        def _():
            far(0, source).wait_send()

        @pl.when((source // 2 < z) | (source // 2 > z))
        def _():
            far(1, source).wait_send()

        return carry

    lax.fori_loop(0, ep_count, finish_source, 0)

    def finish_found(j, carry):
        last_found(j).wait()
        return carry

    lax.fori_loop(1, ep_count, finish_found, 0)
    cross_extra().wait_send()
    last_y.wait_send()
    small_near.wait_send()
    small_far.wait_send()


def fused(tokens, grads, routes, shares, w_gate, w_up, w_down, capacity, width):
    f32, bf16 = jnp.float32, jnp.bfloat16
    ep_count = lax.axis_size("ep")
    count = ep_count // 2
    token_count, model_width = tokens.shape
    units = w_gate.shape[1]
    vm = pltpu.VMEM
    dma = pltpu.SemaphoreType.DMA
    small = vm((ep_count, 1, token_count), f32)
    half = (capacity, 2 * width)
    scratch = [
        vm(tokens.shape, bf16),
        vm(tokens.shape, bf16),
        vm(routes.shape, jnp.int32),
        vm(routes.shape, f32),
        vm(w_gate.shape, bf16),
        vm(w_up.shape, bf16),
        vm(w_down.shape, bf16),
        vm((2, count, token_count, width), bf16),
        vm((ep_count, 2 * ep_count, token_count), f32),
        vm((2, count, capacity, width), bf16),
        vm((capacity, width), bf16),
        vm((2, ep_count, capacity, model_width), bf16),
        vm((ep_count, capacity, units), bf16),
        vm((ep_count, capacity, units), bf16),
        vm((ep_count, capacity, units), bf16),
        vm((ep_count,) + half, bf16),
        vm((ep_count,) + half, bf16),
        vm((ep_count,) + half, bf16),
        vm((count,) + half, bf16),
        vm((count,) + half, bf16),
        vm((count,) + half, bf16),
        vm((ep_count, capacity, width), bf16),
        vm((ep_count, capacity, width), bf16),
        vm((count, token_count, 2 * width), bf16),
        vm((count, token_count, 2 * width), bf16),
        vm((token_count, 2 * width), f32),
        vm((token_count, width), f32),
        vm((token_count, width), bf16),
        vm((token_count, width), bf16),
        small, small, small, small, small,
        dma((2, 3, count)), dma((3, count)),
        dma((count,)), dma((count,)),
        dma((2, count)), dma((2, count)),
        dma((1,)), dma((1,)),
        dma((2, ep_count)), dma((2, ep_count)),
        dma((2, ep_count)), dma((2, ep_count)),
        dma((2, ep_count)), dma((2, ep_count)),
        dma((ep_count,)), dma((ep_count,)),
        dma((ep_count,)), dma((ep_count,)),
        dma((count,)), dma((count,)),
        dma((count,)), dma((count,)),
        dma((1,)), dma((1,)), dma((2,)), dma((2,)),
        dma((ep_count,)), dma((ep_count,)), dma((9,)),
    ]
    return pl.pallas_call(
        fused_kernel,
        out_shape=(
            jax.ShapeDtypeStruct((token_count, width), bf16),
            jax.ShapeDtypeStruct((ep_count, 1, token_count), f32),
            jax.ShapeDtypeStruct((model_width, units), f32),
            jax.ShapeDtypeStruct((model_width, units), f32),
            jax.ShapeDtypeStruct((units, model_width), f32),
        ),
        in_specs=[pl.BlockSpec(memory_space=pltpu.HBM)] * 7,
        out_specs=(pl.BlockSpec(memory_space=pltpu.VMEM),) * 5,
        scratch_shapes=scratch,
        compiler_params=pltpu.CompilerParams(
            collective_id=2, has_side_effects=True, vmem_limit_bytes=46 * 1024 * 1024
        ),
    )(tokens, grads, routes, shares, w_gate, w_up, w_down)


def store_kernel(
    token_ref, found_ref, gate_ref, up_ref, down_ref, route_ref,
    token_out, found_out, gate_out, up_out, down_out, found_buf, sems,
):
    copies = [
        pltpu.make_async_copy(src, dst, sems.at[n])
        for n, (src, dst) in enumerate((
            (gate_ref, gate_out), (up_ref, up_out), (down_ref, down_out), (token_ref, token_out),
        ))
    ]
    for copy in copies:
        copy.start()
    for k in range(route_ref.shape[0]):
        row = jnp.zeros((1, route_ref.shape[1]), jnp.float32)
        for expert in range(found_ref.shape[0]):
            hit = route_ref[pl.ds(k, 1), :] == expert
            row = row + jnp.where(hit, found_ref[expert], 0.0)
        found_buf[pl.ds(k, 1), :] = row
    last = pltpu.make_async_copy(found_buf, found_out, sems.at[4])
    last.start()
    for copy in copies:
        copy.wait()
    last.wait()


def store(token_grad, found, gate_grads, up_grads, down_grads, routes):
    arrays = (token_grad, found, gate_grads, up_grads, down_grads)
    outs = [jax.ShapeDtypeStruct(a.shape, a.dtype) for a in arrays]
    outs[1] = jax.ShapeDtypeStruct(routes.shape, jnp.float32)
    return pl.pallas_call(
        store_kernel,
        out_shape=tuple(outs),
        in_specs=[pl.BlockSpec(memory_space=pltpu.VMEM)] * 6,
        out_specs=(pl.BlockSpec(memory_space=pltpu.HBM),) * 5,
        scratch_shapes=[pltpu.VMEM(routes.shape, jnp.float32), pltpu.SemaphoreType.DMA((5,))],
        compiler_params=pltpu.CompilerParams(vmem_limit_bytes=8 * 1024 * 1024),
    )(*arrays, routes)


def gathered(tokens, routes, gate_weights, out_grad, w_gate, w_up, w_down):
    ep_count = lax.axis_size("ep")
    token_count, model_width = tokens.shape
    capacity = token_count * routes.shape[1] * 5 // (4 * ep_count)
    width = model_width // lax.axis_size("tp")
    arrays = (tokens, out_grad, routes.T, gate_weights.T, w_gate[0], w_up[0], w_down[0])
    arrays = [pltpu.with_memory_space_constraint(array, pltpu.HBM) for array in arrays]
    parts = fused(*arrays, capacity, width)
    token_grad, gate_grad, gate_grads, up_grads, down_grads = store(*parts, routes.T)
    return (token_grad, gate_grad.T, gate_grads[None], up_grads[None], down_grads[None])


def chosen(*args):
    tokens, w_gate = args[0], args[4]
    ep_count = lax.axis_size("ep")
    block_bytes = ep_count * tokens.size * 2
    if block_bytes <= 16 * 1024 * 1024 and w_gate.shape[0] == 1 and ep_count == 8:
        return gathered(*args)
    return local(*args)


def solution(mesh):
    return jax.shard_map(
        chosen,
        mesh=mesh,
        in_specs=(
            P("ep", None),
            P("ep", None),
            P("ep", None),
            P("ep", None),
            P("ep", None, "tp"),
            P("ep", None, "tp"),
            P("ep", "tp", None),
        ),
        out_specs=(
            P("ep", "tp"),
            P("ep", None),
            P("ep", None, "tp"),
            P("ep", None, "tp"),
            P("ep", "tp", None),
        ),
        check_vma=False,
    )
```

```python
import jax
import jax.numpy as jnp
from jax import lax
from jax.experimental import pallas as pl
from jax.experimental.pallas import tpu as pltpu
from jax.sharding import PartitionSpec as P

clamp_limit = 7.0
sigmoid_slope = 1.702
MESH = pl.DeviceIdType.MESH
far_step = 2


def partners():
    ep_count = lax.axis_size("ep")
    tp_count = lax.axis_size("tp")
    here = lax.axis_index("ep")
    part = lax.axis_index("tp")
    beside = part + 1 - 2 * (part % 2)
    across = (part + tp_count // 2) % tp_count
    return ep_count, here, part, beside, across


def greet(ep_count, here, part, beside, across):
    barrier = pltpu.get_barrier_semaphore()
    pl.semaphore_signal(barrier, inc=1, device_id=(here, beside), device_id_type=MESH)
    pl.semaphore_signal(barrier, inc=1, device_id=(here, across), device_id_type=MESH)

    def call(j, carry):
        peer = (here + j) % ep_count
        pl.semaphore_signal(barrier, inc=1, device_id=(peer, part), device_id_type=MESH)
        return carry

    lax.fori_loop(1, ep_count, call, 0)
    pl.semaphore_wait(barrier, ep_count + 1)


def remote(src, dst, sent, got, device):
    return pltpu.make_async_remote_copy(
        src_ref=src, dst_ref=dst, send_sem=sent, recv_sem=got, device_id=device, device_id_type=MESH
    )


def dispatch_kernel(
    token_ref, grad_ref, weight_ref, token_rows, grad_rows, weights_out,
    s1, r1, s2, r2, s3, r3, s4, r4, sw, rw, own_sem,
):
    ep_count, here, part, beside, across = partners()
    width = token_ref.shape[2]
    pairs = ((0, token_ref, token_rows), (1, grad_ref, grad_rows))

    def block(rows_ref, source, owner):
        columns = pl.ds(pl.multiple_of(owner * width, width), width)
        return rows_ref.at[source, :, columns]

    greet(ep_count, here, part, beside, across)

    def first(j):
        peer = (here + j) % ep_count
        return [
            remote(send.at[peer], block(rows, here, part), s1.at[i, j], r1.at[i, j], (peer, part))
            for i, send, rows in pairs
        ]

    def first_weight(j):
        peer = (here + j) % ep_count
        return remote(
            weight_ref.at[peer], weights_out.at[here], sw.at[j], rw.at[j], (peer, part)
        )

    def forward(j, owner, sent, got, to):
        source = (here + ep_count - j) % ep_count
        return [
            remote(
                block(rows, source, owner), block(rows, source, owner),
                sent.at[i, j], got.at[i, j], (here, to),
            )
            for i, _, rows in pairs
        ]

    def near(j):
        return forward(j, part, s2, r2, beside)

    def far(j):
        return forward(j, part, s3, r3, across)

    def onward(j):
        return forward(j, across, s4, r4, beside)

    owns = [
        pltpu.make_async_copy(send.at[here], block(rows, here, part), own_sem.at[i])
        for i, send, rows in pairs
    ]
    owns.append(pltpu.make_async_copy(weight_ref.at[here], weights_out.at[here], own_sem.at[2]))
    for copy in owns:
        copy.start()

    def launch(j, carry):
        first_weight(j).start()
        for copy in first(j):
            copy.start()
        return carry

    lax.fori_loop(1, ep_count, launch, 0)
    for copy in owns:
        copy.wait()
    for copy in far(0) + near(0):
        copy.start()

    def pass_on(j, carry):
        @pl.when(j < ep_count)
        def _():
            for i in range(2):
                first(j)[i].wait_recv()
                far(j)[i].start()
                near(j)[i].start()

        @pl.when(j >= 2)
        def _():
            for i in range(2):
                far(j - 2)[i].wait_recv()
                onward(j - 2)[i].start()

        return carry

    lax.fori_loop(1, ep_count + 2, pass_on, 0)

    def finish(j, carry):
        for i in range(2):
            near(j)[i].wait()
            onward(j)[i].wait()
            far(j)[i].wait_send()

        @pl.when(j >= 1)
        def _():
            for copy in first(j):
                copy.wait_send()
            first_weight(j).wait()

        return carry

    lax.fori_loop(0, ep_count, finish, 0)


def dispatch(send_tokens, send_grads, weights, model_width):
    ep_count, capacity, width = send_tokens.shape
    sems = [pltpu.SemaphoreType.DMA((2, ep_count)) for _ in range(8)]
    sems += [pltpu.SemaphoreType.DMA((ep_count,)) for _ in range(2)]
    whole = jax.ShapeDtypeStruct((ep_count, capacity, model_width), jnp.bfloat16)
    return pl.pallas_call(
        dispatch_kernel,
        out_shape=(whole, whole, jax.ShapeDtypeStruct(weights.shape, jnp.float32)),
        in_specs=[pl.BlockSpec(memory_space=pltpu.VMEM)] * 3,
        out_specs=(
            pl.BlockSpec(memory_space=pl.ANY),
            pl.BlockSpec(memory_space=pl.ANY),
            pl.BlockSpec(memory_space=pltpu.VMEM),
        ),
        scratch_shapes=sems + [pltpu.SemaphoreType.DMA((3,))],
        compiler_params=pltpu.CompilerParams(collective_id=0, has_side_effects=True),
    )(send_tokens, send_grads, weights)


def combine_kernel(
    rows_ref, product_ref, back_ref, back_product, near_buf, far_send, far_buf, last_send,
    product_near, product_sum, product_far, product_send,
    s1, r1, s2, r2, s3, r3, sw, rw, small_send, small_recv,
):
    ep_count, here, part, beside, across = partners()
    width = back_ref.shape[2]
    beside_far = (beside + lax.axis_size("tp") // 2) % lax.axis_size("tp")

    def columns(owner):
        return pl.ds(pl.multiple_of(owner * width, width), width)

    greet(ep_count, here, part, beside, across)

    def near(which, j):
        target = (here + j) % ep_count
        owner = beside_far if which == 0 else beside
        return remote(
            rows_ref.at[target, :, columns(owner)], near_buf.at[which, j],
            s1.at[which, j], r1.at[which, j], (here, beside),
        )

    def far(j):
        return remote(far_send.at[j], far_buf.at[j], s2.at[j], r2.at[j], (here, across))

    def last(j):
        peer = (here + j) % ep_count
        return remote(last_send.at[j], back_ref.at[here], s3.at[j], r3.at[j], (peer, part))

    def last_product(j):
        peer = (here + j) % ep_count
        return remote(
            product_send.at[peer], back_product.at[here], sw.at[j], rw.at[j], (peer, part)
        )

    small_near = remote(product_ref, product_near, small_send.at[0], small_recv.at[0], (here, beside))
    small_far = remote(product_sum, product_far, small_send.at[1], small_recv.at[1], (here, across))
    small_near.start()

    def launch(step, carry):
        j = (step + 1) % ep_count
        near(0, j).start()
        near(1, j).start()
        return carry

    lax.fori_loop(0, ep_count, launch, 0)
    small_near.wait_recv()
    product_sum[...] = product_ref[...] + product_near[...]
    small_far.start()

    def middle(step, carry):
        j = (step + 1) % ep_count
        near(0, j).wait_recv()
        target = (here + j) % ep_count
        mine = rows_ref[target, :, columns(across)].astype(jnp.float32)
        far_send[j] = (mine + near_buf[0, j].astype(jnp.float32)).astype(jnp.bfloat16)
        far(j).start()
        return carry

    lax.fori_loop(0, ep_count, middle, 0)
    small_far.wait_recv()
    product_send[...] = product_sum[...] + product_far[...]

    def total(j):
        near(1, j).wait_recv()
        far(j).wait_recv()
        target = (here + j) % ep_count
        mine = rows_ref[target, :, columns(part)].astype(jnp.float32)
        added = mine + near_buf[1, j].astype(jnp.float32) + far_buf[j].astype(jnp.float32)
        return added.astype(jnp.bfloat16)

    def end(j, carry):
        last_send[j] = total(j)
        last(j).start()
        last_product(j).start()
        return carry

    lax.fori_loop(1, ep_count, end, 0)
    back_ref[here] = total(0)
    back_product[here] = product_send[here]

    small_near.wait_send()
    small_far.wait_send()

    def finish(j, carry):
        near(0, j).wait_send()
        near(1, j).wait_send()
        far(j).wait_send()

        @pl.when(j >= 1)
        def _():
            last(j).wait()
            last_product(j).wait()

        return carry

    lax.fori_loop(0, ep_count, finish, 0)


def combine(rows, products, width):
    ep_count, capacity, _ = rows.shape
    one = (ep_count, capacity, width)
    small = pltpu.VMEM(products.shape, jnp.float32)
    dma = pltpu.SemaphoreType.DMA
    return pl.pallas_call(
        combine_kernel,
        out_shape=(
            jax.ShapeDtypeStruct(one, jnp.bfloat16),
            jax.ShapeDtypeStruct(products.shape, jnp.float32),
        ),
        in_specs=[pl.BlockSpec(memory_space=pltpu.VMEM)] * 2,
        out_specs=(pl.BlockSpec(memory_space=pltpu.VMEM),) * 2,
        scratch_shapes=[
            pltpu.VMEM((2,) + one, jnp.bfloat16),
            pltpu.VMEM(one, jnp.bfloat16),
            pltpu.VMEM(one, jnp.bfloat16),
            pltpu.VMEM(one, jnp.bfloat16),
            small, small, small, small,
            dma((2, ep_count)), dma((2, ep_count)),
            dma((ep_count,)), dma((ep_count,)), dma((ep_count,)), dma((ep_count,)),
            dma((ep_count,)), dma((ep_count,)), dma((2,)), dma((2,)),
        ],
        compiler_params=pltpu.CompilerParams(
            collective_id=1, has_side_effects=True, vmem_limit_bytes=48 * 1024 * 1024
        ),
    )(rows, products)


def local(tokens, routes, gate_weights, out_grad, w_gate, w_up, w_down):
    f32, bf16 = jnp.float32, jnp.bfloat16
    ep_count = lax.axis_size("ep")
    tp_count = lax.axis_size("tp")
    part = lax.axis_index("tp")
    token_count, model_width = tokens.shape
    top_count = routes.shape[1]
    experts = ep_count * w_gate.shape[0]
    capacity = token_count * top_count * 5 // (4 * experts)
    width = model_width // tp_count

    match = routes[:, :, None] == jnp.arange(experts, dtype=jnp.int32)[None, None, :]
    named = jnp.any(match, axis=1)
    before = jnp.arange(token_count)[:, None] > jnp.arange(token_count)[None, :]
    rank = jnp.dot(before.astype(bf16), named.astype(bf16), preferred_element_type=f32)
    rank = jnp.where(named, rank.astype(jnp.int32), -1)
    pick = rank.T[:, None, :] == jnp.arange(capacity, dtype=jnp.int32)[None, :, None]
    pick_flat = pick.reshape(experts * capacity, token_count).astype(bf16)
    weight_of = jnp.sum(jnp.where(match, gate_weights[:, :, None], 0.0), axis=1)
    send_weights = jnp.sum(jnp.where(pick, weight_of.T[:, None, :], 0.0), axis=2)
    sends = []
    for array in (tokens, out_grad):
        own = lax.dynamic_slice_in_dim(array, part * width, width, 1)
        picked = jnp.dot(pick_flat, own, preferred_element_type=f32).astype(bf16)
        sends.append(picked.reshape(experts, capacity, width))

    rows, grads, weights = dispatch(*sends, send_weights[:, None, :], model_width)
    row_count = ep_count * capacity
    x_rows = rows.reshape(row_count, model_width)
    dy_rows = grads.reshape(row_count, model_width)
    slot_weights = weights.reshape(row_count, 1)

    gate_pre = jnp.dot(x_rows, w_gate[0], preferred_element_type=f32)
    up_pre = jnp.dot(x_rows, w_up[0], preferred_element_type=f32)
    plain_grad = jnp.einsum("rd,fd->rf", dy_rows, w_down[0], preferred_element_type=f32)
    glu = jnp.minimum(gate_pre, clamp_limit)
    linear = jnp.clip(up_pre, -clamp_limit, clamp_limit)
    sigma = jax.nn.sigmoid(sigmoid_slope * glu)
    active = glu * sigma
    hidden = active * (linear + 1.0)
    product = jnp.sum(hidden * plain_grad, axis=1)
    hidden_grad = plain_grad * slot_weights
    slope_term = sigma + sigmoid_slope * active * (1.0 - sigma)
    gate_pre_grad = jnp.where(
        gate_pre < clamp_limit, hidden_grad * (linear + 1.0) * slope_term, 0.0
    ).astype(bf16)
    up_pre_grad = jnp.where(jnp.abs(up_pre) < clamp_limit, hidden_grad * active, 0.0).astype(bf16)
    hidden = (hidden * slot_weights).astype(bf16)

    row_term = jnp.einsum("rf,df->rd", gate_pre_grad, w_gate[0], preferred_element_type=f32)
    row_term = row_term + jnp.einsum(
        "rf,df->rd", up_pre_grad, w_up[0], preferred_element_type=f32
    )
    row_term = row_term.astype(bf16).reshape(ep_count, capacity, model_width)
    back_rows, back_products = combine(
        row_term, product.reshape(ep_count, 1, capacity), width
    )
    gate_grads = jnp.einsum("rd,rf->df", x_rows, gate_pre_grad, preferred_element_type=f32)
    up_grads = jnp.einsum("rd,rf->df", x_rows, up_pre_grad, preferred_element_type=f32)
    down_grads = jnp.einsum("rf,rd->fd", hidden, dy_rows, preferred_element_type=f32)
    token_grad = jnp.einsum(
        "rt,rw->tw", pick_flat, back_rows.reshape(row_count, width), preferred_element_type=f32
    ).astype(bf16)
    found = jnp.sum(jnp.where(pick, back_products.reshape(experts, capacity, 1), 0.0), axis=1)
    gate_grad = jnp.sum(jnp.where(match, found.T[:, None, :], 0.0), axis=2)
    return (token_grad, gate_grad, gate_grads[None], up_grads[None], down_grads[None])


def fused_kernel(
    tok_hbm, grd_hbm, route_hbm, share_hbm, gate_hbm, up_hbm, down_hbm,
    token_out, found_out, gate_out, up_out, down_out,
    tok_ref, grd_ref, route_ref, share_ref, gate_ref, up_ref, down_ref, line, line_extra, metas, pick_send, rows, gate_g, up_g, hid,
    near_send, near_buf, mine, own_sum, back_send, back_buf,
    half_send, half_buf, z_send, z_buf, total, total_half, y_send, y_buf,
    found_loc, found_near, found_sum, found_far, found_send,
    chain_s, chain_r, xm_s, xm_r, x_s, x_r, u_s, u_r, n_s, n_r, f_s, f_r, o_s, o_r,
    c_s, c_r, h_s, h_r, b_s, b_r, z_s, z_r, y_s, y_r, sm_s, sm_r, l_s, l_r, in_s,
):
    f32, bf16 = jnp.float32, jnp.bfloat16
    ep_count, here, part, beside, across = partners()
    count = ep_count // 2
    z, x = here // 2, here % 2
    other = here + 1 - 2 * x
    plane, core = part // 2, part % 2
    capacity = rows.shape[2]
    model_width = tok_ref.shape[1]
    width = token_out.shape[1]
    token_count = tok_ref.shape[0]

    def columns(owner):
        return pl.ds(pl.multiple_of(owner * width, width), width)

    def order(i):
        mixed, bit = 0, 1
        while bit < count:
            mixed = mixed + ((z // bit + i // bit) % 2) * bit
            bit = 2 * bit
        return mixed

    inward = (2 * z) // count
    middle = (2 * z * (count - 1 - z) + count * count - 1) // (count * count)

    def place(i):
        return order(i + middle * (i // far_step) * (1 - 2 * (i % 2)))

    def chain(kind, zi, way):
        ref = metas.at[2 * zi + x] if kind == 2 else line.at[kind, zi]
        to = here + 2 - 4 * way
        return remote(ref, ref, chain_s.at[way, kind, zi], chain_r.at[kind, zi], (to, part))

    def chain_extra(kind, way):
        whole = grd_ref if kind else tok_ref
        return remote(
            whole.at[:, columns(across)], line_extra.at[way, kind],
            u_s.at[way, kind], u_r.at[way, kind], (here + 2 - 4 * way, part),
        )

    def cross_meta(zi):
        ref = metas.at[2 * zi + x]
        return remote(ref, ref, xm_s.at[zi], xm_r.at[zi], (other, part))

    def cross(kind, zi):
        return remote(
            pick_send.at[kind, zi], rows.at[kind, 2 * zi + x, :, columns(part)],
            x_s.at[kind, zi], x_r.at[kind, zi], (other, part),
        )

    def forward(kind, source, owner, sent, got, to):
        ref = rows.at[kind, source, :, columns(owner)]
        return remote(ref, ref, sent.at[kind, source], got.at[kind, source], (here, to))

    def near(kind, source):
        return forward(kind, source, part, n_s, n_r, beside)

    def far(kind, source):
        return forward(kind, source, part, f_s, f_r, across)

    def onward(kind, source):
        return forward(kind, source, across, o_s, o_r, beside)

    def pair(source):
        return remote(
            near_send.at[source], near_buf.at[source], c_s.at[source], c_r.at[source],
            (here, beside),
        )

    def half_over(source):
        return remote(
            half_send.at[source], half_buf.at[source], h_s.at[source], h_r.at[source],
            (here, across),
        )

    def is_far(zi):
        return order(zi) >= far_step

    def cut(ref, zi, small):
        return ref.at[zi, :, pl.ds(0, width)] if small else ref.at[zi]

    def cross_back(zi, small):
        return remote(
            cut(back_send, zi, small), cut(back_buf, zi, small),
            b_s.at[zi], b_r.at[zi], (other, part),
        )

    def line_back(zi, small, half=0):
        at = pl.ds(0, width) if small else columns(half)
        return remote(
            z_send.at[zi, :, at], z_buf.at[z, :, at],
            z_s.at[half, zi], z_r.at[half, z], (2 * zi + x, part),
        )

    def line_got(zi, small, half=0):
        at = pl.ds(0, width) if small else columns(half)
        return remote(
            z_send.at[zi, :, at], z_buf.at[zi, :, at],
            z_s.at[half, zi], z_r.at[half, zi], (2 * zi + x, part),
        )

    def either(zi, act):
        @pl.when(is_far(zi))
        def _():
            act(True)

        @pl.when(jnp.logical_not(is_far(zi)))
        def _():
            act(False)

    last_y = remote(y_send, y_buf, y_s.at[0], y_r.at[0], (here, across))
    small_near = remote(found_loc, found_near, sm_s.at[0], sm_r.at[0], (here, beside))
    small_far = remote(found_sum, found_far, sm_s.at[1], sm_r.at[1], (here, across))

    def last_found(j):
        peer = (here + j) % ep_count
        return remote(found_send.at[peer], found_out.at[here], l_s.at[j], l_r.at[j], (peer, part))

    slots = lax.broadcasted_iota(jnp.int32, (capacity, token_count), 0).astype(f32)

    def matches(source, expert):
        return slots == metas[source, pl.ds(expert, 1), :]

    def pick(source, expert):
        return jnp.where(matches(source, expert), 1.0, 0.0).astype(bf16)

    barrier = pltpu.get_barrier_semaphore()
    pl.semaphore_signal(barrier, inc=1, device_id=(here, beside), device_id_type=MESH)
    pl.semaphore_signal(barrier, inc=1, device_id=(here, across), device_id_type=MESH)

    pl.semaphore_signal(barrier, inc=1, device_id=(other, part), device_id_type=MESH)

    @pl.when(z > 0)
    def _():
        pl.semaphore_signal(barrier, inc=1, device_id=(here - 2, part), device_id_type=MESH)

    @pl.when(z < count - 1)
    def _():
        pl.semaphore_signal(barrier, inc=1, device_id=(here + 2, part), device_id_type=MESH)

    loads = [
        pltpu.make_async_copy(src, dst, in_s.at[n])
        for n, (src, dst) in enumerate((
            (route_hbm, route_ref), (share_hbm, share_ref),
            (tok_hbm.at[:, columns(part)], line.at[0, z]),
            (grd_hbm.at[:, columns(part)], line.at[1, z]),
            (tok_hbm, tok_ref), (grd_hbm, grd_ref),
            (gate_hbm, gate_ref), (up_hbm, up_ref), (down_hbm, down_ref),
        ))
    ]
    for load in loads:
        load.start()
    total_half[...] = jnp.zeros(total_half.shape, f32)
    experts = lax.broadcasted_iota(jnp.int32, (ep_count, token_count), 0)
    earlier = lax.broadcasted_iota(jnp.int32, (token_count, token_count), 0)
    later = lax.broadcasted_iota(jnp.int32, (token_count, token_count), 1)
    before = jnp.where(earlier < later, 1.0, 0.0).astype(bf16)
    loads[0].wait()
    loads[1].wait()
    named = jnp.zeros((ep_count, token_count), f32)
    weight_of = jnp.zeros((ep_count, token_count), f32)
    for k in range(route_ref.shape[0]):
        chosen_here = route_ref[pl.ds(k, 1), :] == experts
        named = named + jnp.where(chosen_here, 1.0, 0.0)
        weight_of = weight_of + jnp.where(chosen_here, share_ref[pl.ds(k, 1), :], 0.0)
    rank = jnp.dot(named.astype(bf16), before, preferred_element_type=f32)
    metas[here, pl.ds(0, ep_count), :] = jnp.where(named > 0.0, rank, -1.0)
    metas[here, pl.ds(ep_count, ep_count), :] = weight_of
    loads[2].wait()
    loads[3].wait()
    pl.semaphore_wait(barrier, 4 + middle)

    @pl.when(z < count - 1)
    def _():
        for kind in (2, 0, 1):
            chain(kind, z, 0).start()

    @pl.when(z > 0)
    def _():
        for kind in (2, 0, 1):
            chain(kind, z, 1).start()

    def take(kind, zi):
        chain(kind, zi, 0).wait_recv()

        @pl.when((zi < z) & (z < count - 1))
        def _():
            chain(kind, zi, 0).start()

        @pl.when((zi > z) & (z > 0))
        def _():
            chain(kind, zi, 1).start()

    def is_next(zi):
        return (zi - z) * (zi - z) == 1

    def send_extra(way):
        chain_extra(0, way).start()
        chain_extra(1, way).start()

    def hand_on_extra(i):
        zi = place(i)
        source = 2 * zi + x
        way = (zi - z + 1) // 2
        for kind in range(2):
            chain_extra(kind, way).wait_recv()
            own = jnp.dot(
                pick(source, here), line_extra[way, kind], preferred_element_type=f32
            )
            rows[kind, source, :, columns(across)] = own.astype(bf16)
            onward(kind, source).start()

    def relay(kind, i):
        @pl.when(middle == 1)
        def _():
            if kind == 0:
                take(2, place(i))
            take(kind, place(i))

    def picks(kind, i):
        zi = place(i)
        source = 2 * zi + x

        @pl.when((i == 1) | ((i > 1) & (middle == 0)))
        def _():
            if kind == 0:
                take(2, zi)
            take(kind, zi)

        if kind == 0:
            cross_meta(zi).start()
        picked = jnp.dot(pick(source, other), line[kind, zi], preferred_element_type=f32)
        pick_send[kind, zi] = picked.astype(bf16)
        cross(kind, zi).start()

        @pl.when(i >= 1)
        def _():
            own = jnp.dot(pick(source, here), line[kind, zi], preferred_element_type=f32)
            rows[kind, source, :, columns(part)] = own.astype(bf16)

            @pl.when(jnp.logical_not(is_next(zi)))
            def _():
                far(kind, source).start()

            near(kind, source).start()

    def local_picks():
        loads[4].wait()
        loads[5].wait()
        for kind, whole in enumerate((tok_ref, grd_ref)):
            for q in range(model_width // width):
                at = pl.ds(q * width, width)
                own = jnp.dot(pick(here, here), whole[:, at], preferred_element_type=f32)
                rows[kind, here, :, at] = own.astype(bf16)

    def arrive(kind, i):
        source = 2 * place(i) + 1 - x
        cross(kind, place(i)).wait_recv()
        far(kind, source).start()
        near(kind, source).start()
        if kind == 1:
            cross_meta(place(i)).wait_recv()

    def hand_on(source):
        for kind in range(2):
            far(kind, source).wait_recv()
            onward(kind, source).start()

    def compute(source, local_rows):
        @pl.when(local_rows == 0)
        def _():
            for kind in range(2):
                near(kind, source).wait_recv()
                onward(kind, source).wait_recv()

        nt = (((1,), (1,)), ((), ()))
        x_rows = rows[0, source]
        gate_pre = jnp.dot(x_rows, gate_ref[...], preferred_element_type=f32)
        up_pre = jnp.dot(x_rows, up_ref[...], preferred_element_type=f32)
        plain = lax.dot_general(rows[1, source], down_ref[...], nt, preferred_element_type=f32)
        hit = matches(source, here)
        weight_row = metas[source, pl.ds(here + ep_count, 1), :]
        weight = jnp.sum(jnp.where(hit, weight_row, 0.0), axis=1, keepdims=True)
        glu = jnp.minimum(gate_pre, clamp_limit)
        linear = jnp.clip(up_pre, -clamp_limit, clamp_limit)
        sigma = jax.nn.sigmoid(sigmoid_slope * glu)
        active = glu * sigma
        hidden = active * (linear + 1.0)
        product = jnp.sum(hidden * plain, axis=1, keepdims=True)
        found_loc[source] = jnp.sum(jnp.where(hit, product, 0.0), axis=0, keepdims=True)
        hidden_grad = plain * weight
        slope_term = sigma + sigmoid_slope * active * (1.0 - sigma)
        gate_grad = jnp.where(
            gate_pre < clamp_limit, hidden_grad * (linear + 1.0) * slope_term, 0.0
        ).astype(bf16)
        up_grad = jnp.where(jnp.abs(up_pre) < clamp_limit, hidden_grad * active, 0.0).astype(bf16)
        gate_g[source] = gate_grad
        up_g[source] = up_grad
        hid[source] = (hidden * weight).astype(bf16)
        for own in range(2):
            for half in range(2):
                owner = 2 * half + (core if own else 1 - core)
                term = lax.dot_general(
                    gate_g[source], gate_ref[columns(owner), :], nt, preferred_element_type=f32
                ) + lax.dot_general(
                    up_g[source], up_ref[columns(owner), :], nt, preferred_element_type=f32
                )
                at = pl.ds(half * width, width)
                if own:
                    mine[source, :, at] = term.astype(bf16)
                else:
                    near_send[source, :, at] = term.astype(bf16)
            if not own:
                pair(source).start()

    def pair_sum(source, zi, own):
        pair(source).wait_recv()

        def act(small):
            if small:
                at = columns(1 - plane)
                added = mine[source, :, at].astype(f32) + near_buf[source, :, at].astype(f32)
                half_send[source] = added.astype(bf16)
                half_over(source).start()
                return
            added = (mine[source].astype(f32) + near_buf[source].astype(f32)).astype(bf16)
            if own:
                own_sum[zi] = added
            else:
                back_send[zi] = added
                cross_back(zi, False).start()

        either(zi, act)

    def half_sum(source, zi, own):
        @pl.when(is_far(zi))
        def _():
            half_over(source).wait_recv()
            at = columns(plane)
            added = mine[source, :, at].astype(f32) + near_buf[source, :, at].astype(f32)
            added = (added + half_buf[source].astype(f32)).astype(bf16)
            if own:
                own_sum[zi, :, pl.ds(0, width)] = added
            else:
                back_send[zi, :, pl.ds(0, width)] = added
                cross_back(zi, True).start()

    def merge(i):
        zi = place(i)
        source = 2 * zi + x
        tn = (((0,), (0,)), ((), ()))

        def act(small):
            cross_back(zi, small).wait_recv()
            for half in range(1 if small else 2):
                at = pl.ds(half * width, width)
                added = lax.dot_general(
                    pick(source, here), own_sum[zi, :, at], tn, preferred_element_type=f32
                ) + lax.dot_general(
                    pick(source, other), back_buf[zi, :, at], tn, preferred_element_type=f32
                )
                if small:
                    z_send[zi, :, at] = added.astype(bf16)
                else:
                    @pl.when(i == 0)
                    def _():
                        total[:, at] = added

                    @pl.when(i >= 1)
                    def _():
                        z_send[zi, :, at] = added.astype(bf16)

            if small:
                line_back(zi, True).start()
            else:
                @pl.when(i >= 1)
                def _():
                    line_back(zi, False, 1 - plane).start()
                    line_back(zi, False, plane).start()

        either(zi, act)

    def own_at(i):
        return 2 * place(i) + x

    def other_at(i):
        return 2 * place(i) + 1 - x

    last = count - 1

    def body(i, carry):
        @pl.when(i == last)
        def _():
            pair_sum(other_at(0), place(0), False)

        @pl.when(i >= 1)
        def _():
            arrive(0, i - 1)

        @pl.when(i >= 2)
        def _():
            hand_on(other_at(i - 2))
            compute(other_at(i - 2), 0)

        @pl.when(i < count)
        def _():
            picks(0, i)

        @pl.when((i == 1) | (i == 2))
        def _():
            relay(0, i + 1)

        @pl.when(i >= 1)
        def _():
            arrive(1, i - 1)

        @pl.when(i == count)
        def _():
            pair_sum(own_at(last - 1), place(last - 1), True)
            pair_sum(other_at(last - 1), place(last - 1), False)

        @pl.when(i < count)
        def _():
            picks(1, i)

        @pl.when((i == 1) | (i == 2))
        def _():
            relay(1, i + 1)

        @pl.when(i == 0)
        def _():
            local_picks()

            @pl.when(middle == 0)
            def _():
                send_extra(inward)

            for load in loads[6:]:
                load.wait()

        @pl.when((i == 1) & (middle == 1))
        def _():
            send_extra(inward)

        @pl.when((i == 2) & (middle == 1))
        def _():
            send_extra(1 - inward)

        @pl.when(i >= 3)
        def _():
            @pl.when(is_next(place(i - 1)))
            def _():
                hand_on_extra(i - 1)

            @pl.when(jnp.logical_not(is_next(place(i - 1))))
            def _():
                hand_on(own_at(i - 1))

        @pl.when(i == count)
        def _():
            hand_on_extra(1)

        @pl.when((i == 0) | (i >= 3))
        def _():
            step = i - (i + count - 1) // count
            compute(own_at(step), 1 - (step + count - 1) // count)

        @pl.when(i == count)
        def _():
            pair_sum(own_at(last), place(last), True)

        @pl.when(i == 1)
        def _():
            pair_sum(own_at(0), place(0), True)

        @pl.when(i == last)
        def _():
            pair_sum(other_at(1), place(1), False)

        return carry

    def closing(j, carry):
        is_other = middle + j - 2 * middle * j

        @pl.when(is_other == 1)
        def _():
            hand_on(other_at(last))

        compute(own_at(1) + (other_at(last) - own_at(1)) * is_other, 0)
        return carry

    def weights(n, carry):
        chunk = 256
        tn = (((0,), (0,)), ((), ()))
        at = pl.ds(pl.multiple_of(n * chunk, chunk), chunk)
        flat = ep_count * capacity
        x_part = rows[0, :, :, at].reshape(flat, chunk)
        g_part = rows[1, :, :, at].reshape(flat, chunk)
        units = gate_g.shape[2]
        gate_out[at, :] = lax.dot_general(
            x_part, gate_g[...].reshape(flat, units), tn, preferred_element_type=f32
        )
        up_out[at, :] = lax.dot_general(
            x_part, up_g[...].reshape(flat, units), tn, preferred_element_type=f32
        )
        down_out[:, at] = lax.dot_general(
            hid[...].reshape(flat, units), g_part, tn, preferred_element_type=f32
        )
        return carry

    chunks = model_width // 256
    lax.fori_loop(0, count + 1, body, 0)
    lax.fori_loop(0, 2, closing, 0)
    small_near.start()
    pair_sum(other_at(last), place(last), False)
    pair_sum(own_at(1), place(1), True)
    merge(1)
    half_sum(other_at(last - 1), place(last - 1), False)
    half_sum(own_at(last - 1), place(last - 1), True)
    merge(0)
    small_near.wait_recv()
    found_sum[...] = found_loc[...] + found_near[...]
    small_far.start()
    lax.fori_loop(0, chunks // 4, weights, 0)
    half_sum(own_at(last), place(last), True)
    merge(last - 1)
    half_sum(other_at(last), place(last), False)
    small_far.wait_recv()
    found_send[...] = found_sum[...] + found_far[...]
    found_out[here] = found_send[here]

    def share(j, carry):
        last_found(j).start()
        return carry

    lax.fori_loop(1, ep_count, share, 0)
    lax.fori_loop(chunks // 4, chunks, weights, 0)
    merge(last)

    def add(half):
        def one(i, carry):
            zi = order(i)

            @pl.when(jnp.logical_not(is_far(zi)))
            def _():
                at = columns(half)
                line_got(zi, False, half).wait_recv()
                total[:, at] = total[:, at] + z_buf[zi, :, at].astype(f32)

            return carry

        lax.fori_loop(1, count, one, 0)

    def add_far(i, carry):
        zi = order(i)

        @pl.when(is_far(zi))
        def _():
            line_got(zi, True).wait_recv()
            total_half[...] = total_half[...] + z_buf[zi, :, pl.ds(0, width)].astype(f32)

        return carry

    def finish(zi, carry):
        for kind in range(3):
            @pl.when((zi <= z) & (z < count - 1))
            def _():
                chain(kind, zi, 0).wait_send()

            @pl.when((zi >= z) & (z > 0))
            def _():
                chain(kind, zi, 1).wait_send()

        cross_meta(zi).wait_send()
        either(zi, lambda small: cross_back(zi, small).wait_send())
        for kind in range(2):
            cross(kind, zi).wait_send()

        return carry

    def finish_source(source, carry):
        pair(source).wait_send()

        @pl.when(is_far(source // 2))
        def _():
            half_over(source).wait_send()

        @pl.when((source < here) | (source > here))
        def _():
            for kind in range(2):
                near(kind, source).wait_send()
                onward(kind, source).wait_send()

        gap = source // 2 - z
        across_line = (source - x) % 2

        @pl.when((across_line == 1) | (gap * gap > 1))
        def _():
            for kind in range(2):
                far(kind, source).wait_send()

        return carry

    def finish_extra(way):
        chain_extra(0, way).wait_send()
        chain_extra(1, way).wait_send()

    add(1 - plane)
    y_send[...] = total[:, columns(1 - plane)].astype(bf16)
    last_y.start()
    lax.fori_loop(0, count, finish, 0)
    lax.fori_loop(0, ep_count, finish_source, 0)
    add(plane)
    finish_extra(inward)

    @pl.when(middle == 1)
    def _():
        finish_extra(1 - inward)

    small_near.wait_send()
    small_far.wait_send()

    def finish_found(j, carry):
        last_found(j).wait()
        return carry

    lax.fori_loop(1, ep_count, finish_found, 0)
    lax.fori_loop(1, count, add_far, 0)
    last_y.wait_recv()
    token_out[...] = (
        total[:, columns(plane)] + total_half[...] + y_buf[...].astype(f32)
    ).astype(bf16)

    def finish_line(i, carry):
        zi = order(i)

        @pl.when(is_far(zi))
        def _():
            line_back(zi, True).wait_send()

        @pl.when(jnp.logical_not(is_far(zi)))
        def _():
            line_back(zi, False, 0).wait_send()
            line_back(zi, False, 1).wait_send()

        return carry

    lax.fori_loop(1, count, finish_line, 0)
    last_y.wait_send()


def fused(tokens, grads, routes, shares, w_gate, w_up, w_down, capacity, width):
    f32, bf16 = jnp.float32, jnp.bfloat16
    ep_count = lax.axis_size("ep")
    count = ep_count // 2
    token_count, model_width = tokens.shape
    units = w_gate.shape[1]
    vm = pltpu.VMEM
    dma = pltpu.SemaphoreType.DMA
    small = vm((ep_count, 1, token_count), f32)
    half = (capacity, 2 * width)
    scratch = [
        vm(tokens.shape, bf16),
        vm(tokens.shape, bf16),
        vm(routes.shape, jnp.int32),
        vm(routes.shape, f32),
        vm(w_gate.shape, bf16),
        vm(w_up.shape, bf16),
        vm(w_down.shape, bf16),
        vm((2, count, token_count, width), bf16),
        vm((2, 2, token_count, width), bf16),
        vm((ep_count, 2 * ep_count, token_count), f32),
        vm((2, count, capacity, width), bf16),
        vm((2, ep_count, capacity, model_width), bf16),
        vm((ep_count, capacity, units), bf16),
        vm((ep_count, capacity, units), bf16),
        vm((ep_count, capacity, units), bf16),
        vm((ep_count,) + half, bf16),
        vm((ep_count,) + half, bf16),
        vm((ep_count,) + half, bf16),
        vm((count,) + half, bf16),
        vm((count,) + half, bf16),
        vm((count,) + half, bf16),
        vm((ep_count, capacity, width), bf16),
        vm((ep_count, capacity, width), bf16),
        vm((count, token_count, 2 * width), bf16),
        vm((count, token_count, 2 * width), bf16),
        vm((token_count, 2 * width), f32),
        vm((token_count, width), f32),
        vm((token_count, width), bf16),
        vm((token_count, width), bf16),
        small, small, small, small, small,
        dma((2, 3, count)), dma((3, count)),
        dma((count,)), dma((count,)),
        dma((2, count)), dma((2, count)),
        dma((2, 2)), dma((2, 2)),
        dma((2, ep_count)), dma((2, ep_count)),
        dma((2, ep_count)), dma((2, ep_count)),
        dma((2, ep_count)), dma((2, ep_count)),
        dma((ep_count,)), dma((ep_count,)),
        dma((ep_count,)), dma((ep_count,)),
        dma((count,)), dma((count,)),
        dma((2, count)), dma((2, count)),
        dma((1,)), dma((1,)), dma((2,)), dma((2,)),
        dma((ep_count,)), dma((ep_count,)), dma((9,)),
    ]
    return pl.pallas_call(
        fused_kernel,
        out_shape=(
            jax.ShapeDtypeStruct((token_count, width), bf16),
            jax.ShapeDtypeStruct((ep_count, 1, token_count), f32),
            jax.ShapeDtypeStruct((model_width, units), f32),
            jax.ShapeDtypeStruct((model_width, units), f32),
            jax.ShapeDtypeStruct((units, model_width), f32),
        ),
        in_specs=[pl.BlockSpec(memory_space=pltpu.HBM)] * 7,
        out_specs=(pl.BlockSpec(memory_space=pltpu.VMEM),) * 5,
        scratch_shapes=scratch,
        compiler_params=pltpu.CompilerParams(
            collective_id=2, has_side_effects=True, vmem_limit_bytes=47 * 1024 * 1024
        ),
    )(tokens, grads, routes, shares, w_gate, w_up, w_down)


def store_kernel(
    token_ref, found_ref, gate_ref, up_ref, down_ref, route_ref,
    token_out, found_out, gate_out, up_out, down_out, found_buf, sems,
):
    copies = [
        pltpu.make_async_copy(src, dst, sems.at[n])
        for n, (src, dst) in enumerate((
            (gate_ref, gate_out), (up_ref, up_out), (down_ref, down_out), (token_ref, token_out),
        ))
    ]
    for copy in copies:
        copy.start()
    for k in range(route_ref.shape[0]):
        row = jnp.zeros((1, route_ref.shape[1]), jnp.float32)
        for expert in range(found_ref.shape[0]):
            hit = route_ref[pl.ds(k, 1), :] == expert
            row = row + jnp.where(hit, found_ref[expert], 0.0)
        found_buf[pl.ds(k, 1), :] = row
    last = pltpu.make_async_copy(found_buf, found_out, sems.at[4])
    last.start()
    for copy in copies:
        copy.wait()
    last.wait()


def store(token_grad, found, gate_grads, up_grads, down_grads, routes):
    arrays = (token_grad, found, gate_grads, up_grads, down_grads)
    outs = [jax.ShapeDtypeStruct(a.shape, a.dtype) for a in arrays]
    outs[1] = jax.ShapeDtypeStruct(routes.shape, jnp.float32)
    return pl.pallas_call(
        store_kernel,
        out_shape=tuple(outs),
        in_specs=[pl.BlockSpec(memory_space=pltpu.VMEM)] * 6,
        out_specs=(pl.BlockSpec(memory_space=pltpu.HBM),) * 5,
        scratch_shapes=[pltpu.VMEM(routes.shape, jnp.float32), pltpu.SemaphoreType.DMA((5,))],
        compiler_params=pltpu.CompilerParams(vmem_limit_bytes=8 * 1024 * 1024),
    )(*arrays, routes)


def gathered(tokens, routes, gate_weights, out_grad, w_gate, w_up, w_down):
    ep_count = lax.axis_size("ep")
    token_count, model_width = tokens.shape
    capacity = token_count * routes.shape[1] * 5 // (4 * ep_count)
    width = model_width // lax.axis_size("tp")
    arrays = (tokens, out_grad, routes.T, gate_weights.T, w_gate[0], w_up[0], w_down[0])
    arrays = [pltpu.with_memory_space_constraint(array, pltpu.HBM) for array in arrays]
    parts = fused(*arrays, capacity, width)
    token_grad, gate_grad, gate_grads, up_grads, down_grads = store(*parts, routes.T)
    return (token_grad, gate_grad.T, gate_grads[None], up_grads[None], down_grads[None])


def chosen(*args):
    tokens, w_gate = args[0], args[4]
    ep_count = lax.axis_size("ep")
    block_bytes = ep_count * tokens.size * 2
    if block_bytes <= 16 * 1024 * 1024 and w_gate.shape[0] == 1 and ep_count == 8:
        return gathered(*args)
    return local(*args)


def solution(mesh):
    return jax.shard_map(
        chosen,
        mesh=mesh,
        in_specs=(
            P("ep", None),
            P("ep", None),
            P("ep", None),
            P("ep", None),
            P("ep", None, "tp"),
            P("ep", None, "tp"),
            P("ep", "tp", None),
        ),
        out_specs=(
            P("ep", "tp"),
            P("ep", None),
            P("ep", None, "tp"),
            P("ep", None, "tp"),
            P("ep", "tp", None),
        ),
        check_vma=False,
    )
```

```python
import jax
import jax.numpy as jnp
from jax import lax
from jax.experimental import pallas as pl
from jax.experimental.pallas import tpu as pltpu
from jax.sharding import PartitionSpec as P

clamp_limit = 7.0
sigmoid_slope = 1.702
MESH = pl.DeviceIdType.MESH
far_step = 2


def partners():
    ep_count = lax.axis_size("ep")
    tp_count = lax.axis_size("tp")
    here = lax.axis_index("ep")
    part = lax.axis_index("tp")
    beside = part + 1 - 2 * (part % 2)
    across = (part + tp_count // 2) % tp_count
    return ep_count, here, part, beside, across


def greet(ep_count, here, part, beside, across):
    barrier = pltpu.get_barrier_semaphore()
    pl.semaphore_signal(barrier, inc=1, device_id=(here, beside), device_id_type=MESH)
    pl.semaphore_signal(barrier, inc=1, device_id=(here, across), device_id_type=MESH)

    def call(j, carry):
        peer = (here + j) % ep_count
        pl.semaphore_signal(barrier, inc=1, device_id=(peer, part), device_id_type=MESH)
        return carry

    lax.fori_loop(1, ep_count, call, 0)
    pl.semaphore_wait(barrier, ep_count + 1)


def remote(src, dst, sent, got, device):
    return pltpu.make_async_remote_copy(
        src_ref=src, dst_ref=dst, send_sem=sent, recv_sem=got, device_id=device, device_id_type=MESH
    )


def dispatch_kernel(
    token_ref, grad_ref, weight_ref, token_rows, grad_rows, weights_out,
    s1, r1, s2, r2, s3, r3, s4, r4, sw, rw, own_sem,
):
    ep_count, here, part, beside, across = partners()
    width = token_ref.shape[2]
    pairs = ((0, token_ref, token_rows), (1, grad_ref, grad_rows))

    def block(rows_ref, source, owner):
        columns = pl.ds(pl.multiple_of(owner * width, width), width)
        return rows_ref.at[source, :, columns]

    greet(ep_count, here, part, beside, across)

    def first(j):
        peer = (here + j) % ep_count
        return [
            remote(send.at[peer], block(rows, here, part), s1.at[i, j], r1.at[i, j], (peer, part))
            for i, send, rows in pairs
        ]

    def first_weight(j):
        peer = (here + j) % ep_count
        return remote(
            weight_ref.at[peer], weights_out.at[here], sw.at[j], rw.at[j], (peer, part)
        )

    def forward(j, owner, sent, got, to):
        source = (here + ep_count - j) % ep_count
        return [
            remote(
                block(rows, source, owner), block(rows, source, owner),
                sent.at[i, j], got.at[i, j], (here, to),
            )
            for i, _, rows in pairs
        ]

    def near(j):
        return forward(j, part, s2, r2, beside)

    def far(j):
        return forward(j, part, s3, r3, across)

    def onward(j):
        return forward(j, across, s4, r4, beside)

    owns = [
        pltpu.make_async_copy(send.at[here], block(rows, here, part), own_sem.at[i])
        for i, send, rows in pairs
    ]
    owns.append(pltpu.make_async_copy(weight_ref.at[here], weights_out.at[here], own_sem.at[2]))
    for copy in owns:
        copy.start()

    def launch(j, carry):
        first_weight(j).start()
        for copy in first(j):
            copy.start()
        return carry

    lax.fori_loop(1, ep_count, launch, 0)
    for copy in owns:
        copy.wait()
    for copy in far(0) + near(0):
        copy.start()

    def pass_on(j, carry):
        @pl.when(j < ep_count)
        def _():
            for i in range(2):
                first(j)[i].wait_recv()
                far(j)[i].start()
                near(j)[i].start()

        @pl.when(j >= 2)
        def _():
            for i in range(2):
                far(j - 2)[i].wait_recv()
                onward(j - 2)[i].start()

        return carry

    lax.fori_loop(1, ep_count + 2, pass_on, 0)

    def finish(j, carry):
        for i in range(2):
            near(j)[i].wait()
            onward(j)[i].wait()
            far(j)[i].wait_send()

        @pl.when(j >= 1)
        def _():
            for copy in first(j):
                copy.wait_send()
            first_weight(j).wait()

        return carry

    lax.fori_loop(0, ep_count, finish, 0)


def dispatch(send_tokens, send_grads, weights, model_width):
    ep_count, capacity, width = send_tokens.shape
    sems = [pltpu.SemaphoreType.DMA((2, ep_count)) for _ in range(8)]
    sems += [pltpu.SemaphoreType.DMA((ep_count,)) for _ in range(2)]
    whole = jax.ShapeDtypeStruct((ep_count, capacity, model_width), jnp.bfloat16)
    return pl.pallas_call(
        dispatch_kernel,
        out_shape=(whole, whole, jax.ShapeDtypeStruct(weights.shape, jnp.float32)),
        in_specs=[pl.BlockSpec(memory_space=pltpu.VMEM)] * 3,
        out_specs=(
            pl.BlockSpec(memory_space=pl.ANY),
            pl.BlockSpec(memory_space=pl.ANY),
            pl.BlockSpec(memory_space=pltpu.VMEM),
        ),
        scratch_shapes=sems + [pltpu.SemaphoreType.DMA((3,))],
        compiler_params=pltpu.CompilerParams(collective_id=0, has_side_effects=True),
    )(send_tokens, send_grads, weights)


def combine_kernel(
    rows_ref, product_ref, back_ref, back_product, near_buf, far_send, far_buf, last_send,
    product_near, product_sum, product_far, product_send,
    s1, r1, s2, r2, s3, r3, sw, rw, small_send, small_recv,
):
    ep_count, here, part, beside, across = partners()
    width = back_ref.shape[2]
    beside_far = (beside + lax.axis_size("tp") // 2) % lax.axis_size("tp")

    def columns(owner):
        return pl.ds(pl.multiple_of(owner * width, width), width)

    greet(ep_count, here, part, beside, across)

    def near(which, j):
        target = (here + j) % ep_count
        owner = beside_far if which == 0 else beside
        return remote(
            rows_ref.at[target, :, columns(owner)], near_buf.at[which, j],
            s1.at[which, j], r1.at[which, j], (here, beside),
        )

    def far(j):
        return remote(far_send.at[j], far_buf.at[j], s2.at[j], r2.at[j], (here, across))

    def last(j):
        peer = (here + j) % ep_count
        return remote(last_send.at[j], back_ref.at[here], s3.at[j], r3.at[j], (peer, part))

    def last_product(j):
        peer = (here + j) % ep_count
        return remote(
            product_send.at[peer], back_product.at[here], sw.at[j], rw.at[j], (peer, part)
        )

    small_near = remote(product_ref, product_near, small_send.at[0], small_recv.at[0], (here, beside))
    small_far = remote(product_sum, product_far, small_send.at[1], small_recv.at[1], (here, across))
    small_near.start()

    def launch(step, carry):
        j = (step + 1) % ep_count
        near(0, j).start()
        near(1, j).start()
        return carry

    lax.fori_loop(0, ep_count, launch, 0)
    small_near.wait_recv()
    product_sum[...] = product_ref[...] + product_near[...]
    small_far.start()

    def middle(step, carry):
        j = (step + 1) % ep_count
        near(0, j).wait_recv()
        target = (here + j) % ep_count
        mine = rows_ref[target, :, columns(across)].astype(jnp.float32)
        far_send[j] = (mine + near_buf[0, j].astype(jnp.float32)).astype(jnp.bfloat16)
        far(j).start()
        return carry

    lax.fori_loop(0, ep_count, middle, 0)
    small_far.wait_recv()
    product_send[...] = product_sum[...] + product_far[...]

    def total(j):
        near(1, j).wait_recv()
        far(j).wait_recv()
        target = (here + j) % ep_count
        mine = rows_ref[target, :, columns(part)].astype(jnp.float32)
        added = mine + near_buf[1, j].astype(jnp.float32) + far_buf[j].astype(jnp.float32)
        return added.astype(jnp.bfloat16)

    def end(j, carry):
        last_send[j] = total(j)
        last(j).start()
        last_product(j).start()
        return carry

    lax.fori_loop(1, ep_count, end, 0)
    back_ref[here] = total(0)
    back_product[here] = product_send[here]

    small_near.wait_send()
    small_far.wait_send()

    def finish(j, carry):
        near(0, j).wait_send()
        near(1, j).wait_send()
        far(j).wait_send()

        @pl.when(j >= 1)
        def _():
            last(j).wait()
            last_product(j).wait()

        return carry

    lax.fori_loop(0, ep_count, finish, 0)


def combine(rows, products, width):
    ep_count, capacity, _ = rows.shape
    one = (ep_count, capacity, width)
    small = pltpu.VMEM(products.shape, jnp.float32)
    dma = pltpu.SemaphoreType.DMA
    return pl.pallas_call(
        combine_kernel,
        out_shape=(
            jax.ShapeDtypeStruct(one, jnp.bfloat16),
            jax.ShapeDtypeStruct(products.shape, jnp.float32),
        ),
        in_specs=[pl.BlockSpec(memory_space=pltpu.VMEM)] * 2,
        out_specs=(pl.BlockSpec(memory_space=pltpu.VMEM),) * 2,
        scratch_shapes=[
            pltpu.VMEM((2,) + one, jnp.bfloat16),
            pltpu.VMEM(one, jnp.bfloat16),
            pltpu.VMEM(one, jnp.bfloat16),
            pltpu.VMEM(one, jnp.bfloat16),
            small, small, small, small,
            dma((2, ep_count)), dma((2, ep_count)),
            dma((ep_count,)), dma((ep_count,)), dma((ep_count,)), dma((ep_count,)),
            dma((ep_count,)), dma((ep_count,)), dma((2,)), dma((2,)),
        ],
        compiler_params=pltpu.CompilerParams(
            collective_id=1, has_side_effects=True, vmem_limit_bytes=48 * 1024 * 1024
        ),
    )(rows, products)


def local(tokens, routes, gate_weights, out_grad, w_gate, w_up, w_down):
    f32, bf16 = jnp.float32, jnp.bfloat16
    ep_count = lax.axis_size("ep")
    tp_count = lax.axis_size("tp")
    part = lax.axis_index("tp")
    token_count, model_width = tokens.shape
    top_count = routes.shape[1]
    experts = ep_count * w_gate.shape[0]
    capacity = token_count * top_count * 5 // (4 * experts)
    width = model_width // tp_count

    match = routes[:, :, None] == jnp.arange(experts, dtype=jnp.int32)[None, None, :]
    named = jnp.any(match, axis=1)
    before = jnp.arange(token_count)[:, None] > jnp.arange(token_count)[None, :]
    rank = jnp.dot(before.astype(bf16), named.astype(bf16), preferred_element_type=f32)
    rank = jnp.where(named, rank.astype(jnp.int32), -1)
    pick = rank.T[:, None, :] == jnp.arange(capacity, dtype=jnp.int32)[None, :, None]
    pick_flat = pick.reshape(experts * capacity, token_count).astype(bf16)
    weight_of = jnp.sum(jnp.where(match, gate_weights[:, :, None], 0.0), axis=1)
    send_weights = jnp.sum(jnp.where(pick, weight_of.T[:, None, :], 0.0), axis=2)
    sends = []
    for array in (tokens, out_grad):
        own = lax.dynamic_slice_in_dim(array, part * width, width, 1)
        picked = jnp.dot(pick_flat, own, preferred_element_type=f32).astype(bf16)
        sends.append(picked.reshape(experts, capacity, width))

    rows, grads, weights = dispatch(*sends, send_weights[:, None, :], model_width)
    row_count = ep_count * capacity
    x_rows = rows.reshape(row_count, model_width)
    dy_rows = grads.reshape(row_count, model_width)
    slot_weights = weights.reshape(row_count, 1)

    gate_pre = jnp.dot(x_rows, w_gate[0], preferred_element_type=f32)
    up_pre = jnp.dot(x_rows, w_up[0], preferred_element_type=f32)
    plain_grad = jnp.einsum("rd,fd->rf", dy_rows, w_down[0], preferred_element_type=f32)
    glu = jnp.minimum(gate_pre, clamp_limit)
    linear = jnp.clip(up_pre, -clamp_limit, clamp_limit)
    sigma = jax.nn.sigmoid(sigmoid_slope * glu)
    active = glu * sigma
    hidden = active * (linear + 1.0)
    product = jnp.sum(hidden * plain_grad, axis=1)
    hidden_grad = plain_grad * slot_weights
    slope_term = sigma + sigmoid_slope * active * (1.0 - sigma)
    gate_pre_grad = jnp.where(
        gate_pre < clamp_limit, hidden_grad * (linear + 1.0) * slope_term, 0.0
    ).astype(bf16)
    up_pre_grad = jnp.where(jnp.abs(up_pre) < clamp_limit, hidden_grad * active, 0.0).astype(bf16)
    hidden = (hidden * slot_weights).astype(bf16)

    row_term = jnp.einsum("rf,df->rd", gate_pre_grad, w_gate[0], preferred_element_type=f32)
    row_term = row_term + jnp.einsum(
        "rf,df->rd", up_pre_grad, w_up[0], preferred_element_type=f32
    )
    row_term = row_term.astype(bf16).reshape(ep_count, capacity, model_width)
    back_rows, back_products = combine(
        row_term, product.reshape(ep_count, 1, capacity), width
    )
    gate_grads = jnp.einsum("rd,rf->df", x_rows, gate_pre_grad, preferred_element_type=f32)
    up_grads = jnp.einsum("rd,rf->df", x_rows, up_pre_grad, preferred_element_type=f32)
    down_grads = jnp.einsum("rf,rd->fd", hidden, dy_rows, preferred_element_type=f32)
    token_grad = jnp.einsum(
        "rt,rw->tw", pick_flat, back_rows.reshape(row_count, width), preferred_element_type=f32
    ).astype(bf16)
    found = jnp.sum(jnp.where(pick, back_products.reshape(experts, capacity, 1), 0.0), axis=1)
    gate_grad = jnp.sum(jnp.where(match, found.T[:, None, :], 0.0), axis=2)
    return (token_grad, gate_grad, gate_grads[None], up_grads[None], down_grads[None])


def fused_kernel(
    tok_hbm, grd_hbm, route_hbm, share_hbm, gate_hbm, up_hbm, down_hbm,
    token_out, found_out, gate_out, up_out, down_out,
    tok_ref, grd_ref, route_ref, share_ref, gate_ref, up_ref, down_ref, line, line_extra, metas, pick_send, rows, gate_g, up_g, hid,
    near_send, near_buf, mine, own_sum, back_send,
    wide_buf, half_send, half_buf, narrow_send, narrow_buf, total, total_half, y_send, y_buf,
    found_loc, found_near, found_sum, found_far, found_send,
    chain_s, chain_r, xm_s, xm_r, x_s, x_r, u_s, u_r, n_s, n_r, f_s, f_r, o_s, o_r,
    c_s, c_r, h_s, h_r, w_s, w_r, z_s, z_r, y_s, y_r, sm_s, sm_r, l_s, l_r, in_s,
):
    f32, bf16 = jnp.float32, jnp.bfloat16
    ep_count, here, part, beside, across = partners()
    count = ep_count // 2
    z, x = here // 2, here % 2
    other = here + 1 - 2 * x
    plane, core = part // 2, part % 2
    capacity = rows.shape[2]
    model_width = tok_ref.shape[1]
    width = token_out.shape[1]
    token_count = tok_ref.shape[0]

    def columns(owner):
        return pl.ds(pl.multiple_of(owner * width, width), width)

    def order(i):
        mixed, bit = 0, 1
        while bit < count:
            mixed = mixed + ((z // bit + i // bit) % 2) * bit
            bit = 2 * bit
        return mixed

    inward = (2 * z) // count
    middle = (2 * z * (count - 1 - z) + count * count - 1) // (count * count)

    def place(i):
        return order(i + middle * (i // far_step) * (1 - 2 * (i % 2)))

    def chain(kind, zi, way):
        ref = metas.at[2 * zi + x] if kind == 2 else line.at[kind, zi]
        to = here + 2 - 4 * way
        return remote(ref, ref, chain_s.at[way, kind, zi], chain_r.at[kind, zi], (to, part))

    def chain_extra(kind, way):
        whole = grd_ref if kind else tok_ref
        return remote(
            whole.at[:, columns(across)], line_extra.at[way, kind],
            u_s.at[way, kind], u_r.at[way, kind], (here + 2 - 4 * way, part),
        )

    def cross_meta(zi):
        ref = metas.at[2 * zi + x]
        return remote(ref, ref, xm_s.at[zi], xm_r.at[zi], (other, part))

    def cross(kind, zi):
        return remote(
            pick_send.at[kind, zi], rows.at[kind, 2 * zi + x, :, columns(part)],
            x_s.at[kind, zi], x_r.at[kind, zi], (other, part),
        )

    def forward(kind, source, owner, sent, got, to):
        ref = rows.at[kind, source, :, columns(owner)]
        return remote(ref, ref, sent.at[kind, source], got.at[kind, source], (here, to))

    def near(kind, source):
        return forward(kind, source, part, n_s, n_r, beside)

    def far(kind, source):
        return forward(kind, source, part, f_s, f_r, across)

    def onward(kind, source):
        return forward(kind, source, across, o_s, o_r, beside)

    def pair(source):
        return remote(
            near_send.at[source], near_buf.at[source], c_s.at[source], c_r.at[source],
            (here, beside),
        )

    def half_over(source):
        return remote(
            half_send.at[source], half_buf.at[source], h_s.at[source], h_r.at[source],
            (here, across),
        )

    def is_far(zi):
        return (zi - z) * (zi - z) >= far_step * far_step

    def wide(source, own):
        ref = own_sum.at[source // 2] if own else back_send.at[source // 2]
        return remote(ref, wide_buf.at[here], w_s.at[source], w_r.at[here], (source, part))

    def wide_got(sender):
        return remote(
            own_sum.at[0], wide_buf.at[sender], w_s.at[sender], w_r.at[sender], (sender, part)
        )

    def narrow(source, sender):
        return remote(
            narrow_send.at[source], narrow_buf.at[sender],
            z_s.at[source], z_r.at[sender], (source, part),
        )

    def either(zi, act):
        @pl.when(is_far(zi))
        def _():
            act(True)

        @pl.when(jnp.logical_not(is_far(zi)))
        def _():
            act(False)

    last_y = remote(y_send, y_buf, y_s.at[0], y_r.at[0], (here, across))
    small_near = remote(found_loc, found_near, sm_s.at[0], sm_r.at[0], (here, beside))
    small_far = remote(found_sum, found_far, sm_s.at[1], sm_r.at[1], (here, across))

    def last_found(j):
        peer = (here + j) % ep_count
        return remote(found_send.at[peer], found_out.at[here], l_s.at[j], l_r.at[j], (peer, part))

    slots = lax.broadcasted_iota(jnp.int32, (capacity, token_count), 0).astype(f32)

    def matches(source, expert):
        return slots == metas[source, pl.ds(expert, 1), :]

    def pick(source, expert):
        return jnp.where(matches(source, expert), 1.0, 0.0).astype(bf16)

    barrier = pltpu.get_barrier_semaphore()
    pl.semaphore_signal(barrier, inc=1, device_id=(here, beside), device_id_type=MESH)
    pl.semaphore_signal(barrier, inc=1, device_id=(here, across), device_id_type=MESH)

    pl.semaphore_signal(barrier, inc=1, device_id=(other, part), device_id_type=MESH)

    @pl.when(z > 0)
    def _():
        pl.semaphore_signal(barrier, inc=1, device_id=(here - 2, part), device_id_type=MESH)

    @pl.when(z < count - 1)
    def _():
        pl.semaphore_signal(barrier, inc=1, device_id=(here + 2, part), device_id_type=MESH)

    loads = [
        pltpu.make_async_copy(src, dst, in_s.at[n])
        for n, (src, dst) in enumerate((
            (route_hbm, route_ref), (share_hbm, share_ref),
            (tok_hbm.at[:, columns(part)], line.at[0, z]),
            (grd_hbm.at[:, columns(part)], line.at[1, z]),
            (tok_hbm, tok_ref), (grd_hbm, grd_ref),
            (gate_hbm, gate_ref), (up_hbm, up_ref), (down_hbm, down_ref),
        ))
    ]
    for load in loads:
        load.start()
    total_half[...] = jnp.zeros(total_half.shape, f32)
    experts = lax.broadcasted_iota(jnp.int32, (ep_count, token_count), 0)
    earlier = lax.broadcasted_iota(jnp.int32, (token_count, token_count), 0)
    later = lax.broadcasted_iota(jnp.int32, (token_count, token_count), 1)
    before = jnp.where(earlier < later, 1.0, 0.0).astype(bf16)
    loads[0].wait()
    loads[1].wait()
    named = jnp.zeros((ep_count, token_count), f32)
    weight_of = jnp.zeros((ep_count, token_count), f32)
    for k in range(route_ref.shape[0]):
        chosen_here = route_ref[pl.ds(k, 1), :] == experts
        named = named + jnp.where(chosen_here, 1.0, 0.0)
        weight_of = weight_of + jnp.where(chosen_here, share_ref[pl.ds(k, 1), :], 0.0)
    rank = jnp.dot(named.astype(bf16), before, preferred_element_type=f32)
    metas[here, pl.ds(0, ep_count), :] = jnp.where(named > 0.0, rank, -1.0)
    metas[here, pl.ds(ep_count, ep_count), :] = weight_of
    loads[2].wait()
    loads[3].wait()
    pl.semaphore_wait(barrier, 4 + middle)

    @pl.when(z < count - 1)
    def _():
        for kind in (2, 0, 1):
            chain(kind, z, 0).start()

    @pl.when(z > 0)
    def _():
        for kind in (2, 0, 1):
            chain(kind, z, 1).start()

    def take(kind, zi):
        chain(kind, zi, 0).wait_recv()

        @pl.when((zi < z) & (z < count - 1))
        def _():
            chain(kind, zi, 0).start()

        @pl.when((zi > z) & (z > 0))
        def _():
            chain(kind, zi, 1).start()

    def is_next(zi):
        return (zi - z) * (zi - z) == 1

    def send_extra(way):
        chain_extra(0, way).start()
        chain_extra(1, way).start()

    def hand_on_extra(i):
        zi = place(i)
        source = 2 * zi + x
        way = (zi - z + 1) // 2
        for kind in range(2):
            chain_extra(kind, way).wait_recv()
            own = jnp.dot(
                pick(source, here), line_extra[way, kind], preferred_element_type=f32
            )
            rows[kind, source, :, columns(across)] = own.astype(bf16)
            onward(kind, source).start()

    def relay(kind, i):
        @pl.when(middle == 1)
        def _():
            if kind == 0:
                take(2, place(i))
            take(kind, place(i))

    def picks(kind, i):
        zi = place(i)
        source = 2 * zi + x

        @pl.when((i == 1) | ((i > 1) & (middle == 0)))
        def _():
            if kind == 0:
                take(2, zi)
            take(kind, zi)

        if kind == 0:
            cross_meta(zi).start()
        picked = jnp.dot(pick(source, other), line[kind, zi], preferred_element_type=f32)
        pick_send[kind, zi] = picked.astype(bf16)
        cross(kind, zi).start()

        @pl.when(i >= 1)
        def _():
            own = jnp.dot(pick(source, here), line[kind, zi], preferred_element_type=f32)
            rows[kind, source, :, columns(part)] = own.astype(bf16)

            @pl.when(jnp.logical_not(is_next(zi)))
            def _():
                far(kind, source).start()

            near(kind, source).start()

    def local_picks():
        loads[4].wait()
        loads[5].wait()
        for kind, whole in enumerate((tok_ref, grd_ref)):
            for q in range(model_width // width):
                at = pl.ds(q * width, width)
                own = jnp.dot(pick(here, here), whole[:, at], preferred_element_type=f32)
                rows[kind, here, :, at] = own.astype(bf16)

    def arrive(kind, i):
        source = 2 * place(i) + 1 - x
        cross(kind, place(i)).wait_recv()
        far(kind, source).start()
        near(kind, source).start()
        if kind == 1:
            cross_meta(place(i)).wait_recv()

    def hand_on(source):
        for kind in range(2):
            far(kind, source).wait_recv()
            onward(kind, source).start()

    def compute(source, local_rows):
        @pl.when(local_rows == 0)
        def _():
            for kind in range(2):
                near(kind, source).wait_recv()
                onward(kind, source).wait_recv()

        nt = (((1,), (1,)), ((), ()))
        x_rows = rows[0, source]
        gate_pre = jnp.dot(x_rows, gate_ref[...], preferred_element_type=f32)
        up_pre = jnp.dot(x_rows, up_ref[...], preferred_element_type=f32)
        plain = lax.dot_general(rows[1, source], down_ref[...], nt, preferred_element_type=f32)
        hit = matches(source, here)
        weight_row = metas[source, pl.ds(here + ep_count, 1), :]
        weight = jnp.sum(jnp.where(hit, weight_row, 0.0), axis=1, keepdims=True)
        glu = jnp.minimum(gate_pre, clamp_limit)
        linear = jnp.clip(up_pre, -clamp_limit, clamp_limit)
        sigma = jax.nn.sigmoid(sigmoid_slope * glu)
        active = glu * sigma
        hidden = active * (linear + 1.0)
        product = jnp.sum(hidden * plain, axis=1, keepdims=True)
        found_loc[source] = jnp.sum(jnp.where(hit, product, 0.0), axis=0, keepdims=True)
        hidden_grad = plain * weight
        slope_term = sigma + sigmoid_slope * active * (1.0 - sigma)
        gate_grad = jnp.where(
            gate_pre < clamp_limit, hidden_grad * (linear + 1.0) * slope_term, 0.0
        ).astype(bf16)
        up_grad = jnp.where(jnp.abs(up_pre) < clamp_limit, hidden_grad * active, 0.0).astype(bf16)
        gate_g[source] = gate_grad
        up_g[source] = up_grad
        hid[source] = (hidden * weight).astype(bf16)
        for own in range(2):
            for half in range(2):
                owner = 2 * half + (core if own else 1 - core)
                term = lax.dot_general(
                    gate_g[source], gate_ref[columns(owner), :], nt, preferred_element_type=f32
                ) + lax.dot_general(
                    up_g[source], up_ref[columns(owner), :], nt, preferred_element_type=f32
                )
                at = pl.ds(half * width, width)
                if own:
                    mine[source, :, at] = term.astype(bf16)
                else:
                    near_send[source, :, at] = term.astype(bf16)
            if not own:
                pair(source).start()

    def pair_sum(source, zi, own):
        pair(source).wait_recv()

        def act(small):
            if small:
                at = columns(1 - plane)
                added = mine[source, :, at].astype(f32) + near_buf[source, :, at].astype(f32)
                half_send[source] = added.astype(bf16)
                half_over(source).start()
                return
            added = (mine[source].astype(f32) + near_buf[source].astype(f32)).astype(bf16)
            if own:
                own_sum[zi] = added

                @pl.when((zi < z) | (zi > z))
                def _():
                    wide(source, True).start()
            else:
                back_send[zi] = added
                wide(source, False).start()

        either(zi, act)

    def half_sum(source, zi):
        @pl.when(is_far(zi))
        def _():
            half_over(source).wait_recv()
            at = columns(plane)
            added = mine[source, :, at].astype(f32) + near_buf[source, :, at].astype(f32)
            narrow_send[source] = (added + half_buf[source].astype(f32)).astype(bf16)
            narrow(source, here).start()

    tn = (((0,), (0,)), ((), ()))

    def add_wide(sender, carry):
        @pl.when(jnp.logical_not(is_far(sender // 2)) & ((sender < here) | (sender > here)))
        def _():
            wide_got(sender).wait_recv()
            for half in range(2):
                at = pl.ds(half * width, width)
                total[:, at] = total[:, at] + lax.dot_general(
                    pick(here, sender), wide_buf[sender, :, at], tn, preferred_element_type=f32
                )

        return carry

    def add_own():
        for half in range(2):
            at = pl.ds(half * width, width)
            total[:, at] = lax.dot_general(
                pick(here, here), own_sum[z, :, at], tn, preferred_element_type=f32
            )

    def own_at(i):
        return 2 * place(i) + x

    def other_at(i):
        return 2 * place(i) + 1 - x

    last = count - 1

    def body(i, carry):
        @pl.when(i == last)
        def _():
            pair_sum(other_at(0), place(0), False)

        @pl.when(i >= 1)
        def _():
            arrive(0, i - 1)

        @pl.when(i == count)
        def _():
            pair_sum(own_at(last - 1), place(last - 1), True)

        @pl.when(i >= 2)
        def _():
            hand_on(other_at(i - 2))
            compute(other_at(i - 2), 0)

        @pl.when(i < count)
        def _():
            picks(0, i)

        @pl.when((i == 1) | (i == 2))
        def _():
            relay(0, i + 1)

        @pl.when(i >= 1)
        def _():
            arrive(1, i - 1)

        @pl.when(i == count)
        def _():
            pair_sum(other_at(last - 1), place(last - 1), False)

        @pl.when(i < count)
        def _():
            picks(1, i)

        @pl.when((i == 1) | (i == 2))
        def _():
            relay(1, i + 1)

        @pl.when(i == 0)
        def _():
            local_picks()

            @pl.when(middle == 0)
            def _():
                send_extra(inward)

            for load in loads[6:]:
                load.wait()

        @pl.when((i == 1) & (middle == 1))
        def _():
            send_extra(inward)

        @pl.when((i == 2) & (middle == 1))
        def _():
            send_extra(1 - inward)
            hand_on_extra(1)

        @pl.when((i == 3) & (middle == 1))
        def _():
            compute(own_at(1), 0)
            pair_sum(own_at(1), place(1), True)

        @pl.when(i >= 3)
        def _():
            @pl.when(is_next(place(i - 1)))
            def _():
                hand_on_extra(i - 1)

            @pl.when(jnp.logical_not(is_next(place(i - 1))))
            def _():
                hand_on(own_at(i - 1))

        @pl.when((i == count) & (middle == 0))
        def _():
            hand_on_extra(1)

        @pl.when((i == 0) | (i >= 3))
        def _():
            step = i - (i + count - 1) // count
            compute(own_at(step), 1 - (step + count - 1) // count)

        @pl.when(i == count)
        def _():
            pair_sum(own_at(last), place(last), True)

        @pl.when(i == 1)
        def _():
            pair_sum(own_at(0), place(0), True)

        @pl.when(i == last)
        def _():
            pair_sum(other_at(1), place(1), False)

        return carry

    def closing(j, carry):
        @pl.when(j == 1)
        def _():
            half_sum(own_at(last - 1), place(last - 1))
            hand_on(other_at(last))

        @pl.when((j == 1) | (middle == 0))
        def _():
            compute(own_at(1) + (other_at(last) - own_at(1)) * j, 0)

        @pl.when((j == 0) & (middle == 0))
        def _():
            pair_sum(own_at(1), place(1), True)

        @pl.when(j == 1)
        def _():
            small_near.start()
            small_near.wait_recv()
            found_sum[...] = found_loc[...] + found_near[...]
            small_far.start()
            pair_sum(other_at(last), place(last), False)

        return carry

    def weights(n, carry):
        chunk = 256
        tn = (((0,), (0,)), ((), ()))
        at = pl.ds(pl.multiple_of(n * chunk, chunk), chunk)
        flat = ep_count * capacity
        x_part = rows[0, :, :, at].reshape(flat, chunk)
        g_part = rows[1, :, :, at].reshape(flat, chunk)
        units = gate_g.shape[2]
        gate_out[at, :] = lax.dot_general(
            x_part, gate_g[...].reshape(flat, units), tn, preferred_element_type=f32
        )
        up_out[at, :] = lax.dot_general(
            x_part, up_g[...].reshape(flat, units), tn, preferred_element_type=f32
        )
        down_out[:, at] = lax.dot_general(
            hid[...].reshape(flat, units), g_part, tn, preferred_element_type=f32
        )
        return carry

    chunks = model_width // 256
    lax.fori_loop(0, count + 1, body, 0)
    lax.fori_loop(0, 2, closing, 0)

    @pl.when(middle == 1)
    def _():
        half_sum(own_at(last), place(last))

    half_sum(other_at(last - 1), place(last - 1))
    small_far.wait_recv()
    found_send[...] = found_sum[...] + found_far[...]
    found_out[here] = found_send[here]

    def share(j, carry):
        last_found(j).start()
        return carry

    lax.fori_loop(1, ep_count, share, 0)
    add_own()
    lax.fori_loop(0, chunks // 8, weights, 0)

    @pl.when(middle == 0)
    def _():
        half_sum(own_at(last), place(last))

    lax.fori_loop(chunks // 8, chunks // 4, weights, 0)
    half_sum(other_at(last), place(last))
    lax.fori_loop(chunks // 4, chunks // 4 + 1, weights, 0)
    lax.fori_loop(0, ep_count, add_wide, 0)
    y_send[...] = total[:, columns(1 - plane)].astype(bf16)
    last_y.start()
    lax.fori_loop(chunks // 4 + 1, chunks // 2, weights, 0)

    def add_far(sender, carry):
        @pl.when(is_far(sender // 2))
        def _():
            narrow(here, sender).wait_recv()
            total_half[...] = total_half[...] + lax.dot_general(
                pick(here, sender), narrow_buf[sender], tn, preferred_element_type=f32
            )

        return carry

    def finish(zi, carry):
        for kind in range(3):
            @pl.when((zi <= z) & (z < count - 1))
            def _():
                chain(kind, zi, 0).wait_send()

            @pl.when((zi >= z) & (z > 0))
            def _():
                chain(kind, zi, 1).wait_send()

        cross_meta(zi).wait_send()
        for kind in range(2):
            cross(kind, zi).wait_send()

        return carry

    def finish_source(source, carry):
        pair(source).wait_send()

        @pl.when(is_far(source // 2))
        def _():
            half_over(source).wait_send()

        @pl.when(jnp.logical_not(is_far(source // 2)) & ((source < here) | (source > here)))
        def _():
            wide(source, False).wait_send()

        @pl.when((source < here) | (source > here))
        def _():
            for kind in range(2):
                near(kind, source).wait_send()
                onward(kind, source).wait_send()

        gap = source // 2 - z
        across_line = (source - x) % 2

        @pl.when((across_line == 1) | (gap * gap > 1))
        def _():
            for kind in range(2):
                far(kind, source).wait_send()

        return carry

    def finish_extra(way):
        chain_extra(0, way).wait_send()
        chain_extra(1, way).wait_send()

    lax.fori_loop(chunks // 2, chunks, weights, 0)
    lax.fori_loop(0, count, finish, 0)
    lax.fori_loop(0, ep_count, finish_source, 0)
    finish_extra(inward)

    @pl.when(middle == 1)
    def _():
        finish_extra(1 - inward)

    small_near.wait_send()
    small_far.wait_send()

    def finish_found(j, carry):
        last_found(j).wait()
        return carry

    lax.fori_loop(0, ep_count, add_far, 0)
    last_y.wait_recv()
    token_out[...] = (
        total[:, columns(plane)] + total_half[...] + y_buf[...].astype(f32)
    ).astype(bf16)

    def finish_narrow(source, carry):
        @pl.when(is_far(source // 2))
        def _():
            narrow(source, here).wait_send()

        return carry

    lax.fori_loop(1, ep_count, finish_found, 0)
    lax.fori_loop(0, ep_count, finish_narrow, 0)
    last_y.wait_send()


def fused(tokens, grads, routes, shares, w_gate, w_up, w_down, capacity, width):
    f32, bf16 = jnp.float32, jnp.bfloat16
    ep_count = lax.axis_size("ep")
    count = ep_count // 2
    token_count, model_width = tokens.shape
    units = w_gate.shape[1]
    vm = pltpu.VMEM
    dma = pltpu.SemaphoreType.DMA
    small = vm((ep_count, 1, token_count), f32)
    half = (capacity, 2 * width)
    scratch = [
        vm(tokens.shape, bf16),
        vm(tokens.shape, bf16),
        vm(routes.shape, jnp.int32),
        vm(routes.shape, f32),
        vm(w_gate.shape, bf16),
        vm(w_up.shape, bf16),
        vm(w_down.shape, bf16),
        vm((2, count, token_count, width), bf16),
        vm((2, 2, token_count, width), bf16),
        vm((ep_count, 2 * ep_count, token_count), f32),
        vm((2, count, capacity, width), bf16),
        vm((2, ep_count, capacity, model_width), bf16),
        vm((ep_count, capacity, units), bf16),
        vm((ep_count, capacity, units), bf16),
        vm((ep_count, capacity, units), bf16),
        vm((ep_count,) + half, bf16),
        vm((ep_count,) + half, bf16),
        vm((ep_count,) + half, bf16),
        vm((count,) + half, bf16),
        vm((count,) + half, bf16),
        vm((ep_count,) + half, bf16),
        vm((ep_count, capacity, width), bf16),
        vm((ep_count, capacity, width), bf16),
        vm((ep_count, capacity, width), bf16),
        vm((ep_count, capacity, width), bf16),
        vm((token_count, 2 * width), f32),
        vm((token_count, width), f32),
        vm((token_count, width), bf16),
        vm((token_count, width), bf16),
        small, small, small, small, small,
        dma((2, 3, count)), dma((3, count)),
        dma((count,)), dma((count,)),
        dma((2, count)), dma((2, count)),
        dma((2, 2)), dma((2, 2)),
        dma((2, ep_count)), dma((2, ep_count)),
        dma((2, ep_count)), dma((2, ep_count)),
        dma((2, ep_count)), dma((2, ep_count)),
        dma((ep_count,)), dma((ep_count,)),
        dma((ep_count,)), dma((ep_count,)),
        dma((ep_count,)), dma((ep_count,)),
        dma((ep_count,)), dma((ep_count,)),
        dma((1,)), dma((1,)), dma((2,)), dma((2,)),
        dma((ep_count,)), dma((ep_count,)), dma((9,)),
    ]
    return pl.pallas_call(
        fused_kernel,
        out_shape=(
            jax.ShapeDtypeStruct((token_count, width), bf16),
            jax.ShapeDtypeStruct((ep_count, 1, token_count), f32),
            jax.ShapeDtypeStruct((model_width, units), f32),
            jax.ShapeDtypeStruct((model_width, units), f32),
            jax.ShapeDtypeStruct((units, model_width), f32),
        ),
        in_specs=[pl.BlockSpec(memory_space=pltpu.HBM)] * 7,
        out_specs=(pl.BlockSpec(memory_space=pltpu.VMEM),) * 5,
        scratch_shapes=scratch,
        compiler_params=pltpu.CompilerParams(
            collective_id=2, has_side_effects=True, vmem_limit_bytes=47 * 1024 * 1024
        ),
    )(tokens, grads, routes, shares, w_gate, w_up, w_down)


def store_kernel(
    token_ref, found_ref, gate_ref, up_ref, down_ref, route_ref,
    token_out, found_out, gate_out, up_out, down_out, found_buf, sems,
):
    copies = [
        pltpu.make_async_copy(src, dst, sems.at[n])
        for n, (src, dst) in enumerate((
            (gate_ref, gate_out), (up_ref, up_out), (down_ref, down_out), (token_ref, token_out),
        ))
    ]
    for copy in copies:
        copy.start()
    for k in range(route_ref.shape[0]):
        row = jnp.zeros((1, route_ref.shape[1]), jnp.float32)
        for expert in range(found_ref.shape[0]):
            hit = route_ref[pl.ds(k, 1), :] == expert
            row = row + jnp.where(hit, found_ref[expert], 0.0)
        found_buf[pl.ds(k, 1), :] = row
    last = pltpu.make_async_copy(found_buf, found_out, sems.at[4])
    last.start()
    for copy in copies:
        copy.wait()
    last.wait()


def store(token_grad, found, gate_grads, up_grads, down_grads, routes):
    arrays = (token_grad, found, gate_grads, up_grads, down_grads)
    outs = [jax.ShapeDtypeStruct(a.shape, a.dtype) for a in arrays]
    outs[1] = jax.ShapeDtypeStruct(routes.shape, jnp.float32)
    return pl.pallas_call(
        store_kernel,
        out_shape=tuple(outs),
        in_specs=[pl.BlockSpec(memory_space=pltpu.VMEM)] * 6,
        out_specs=(pl.BlockSpec(memory_space=pltpu.HBM),) * 5,
        scratch_shapes=[pltpu.VMEM(routes.shape, jnp.float32), pltpu.SemaphoreType.DMA((5,))],
        compiler_params=pltpu.CompilerParams(vmem_limit_bytes=8 * 1024 * 1024),
    )(*arrays, routes)


def gathered(tokens, routes, gate_weights, out_grad, w_gate, w_up, w_down):
    ep_count = lax.axis_size("ep")
    token_count, model_width = tokens.shape
    capacity = token_count * routes.shape[1] * 5 // (4 * ep_count)
    width = model_width // lax.axis_size("tp")
    arrays = (tokens, out_grad, routes.T, gate_weights.T, w_gate[0], w_up[0], w_down[0])
    arrays = [pltpu.with_memory_space_constraint(array, pltpu.HBM) for array in arrays]
    parts = fused(*arrays, capacity, width)
    token_grad, gate_grad, gate_grads, up_grads, down_grads = store(*parts, routes.T)
    return (token_grad, gate_grad.T, gate_grads[None], up_grads[None], down_grads[None])


def chosen(*args):
    tokens, w_gate = args[0], args[4]
    ep_count = lax.axis_size("ep")
    block_bytes = ep_count * tokens.size * 2
    if block_bytes <= 16 * 1024 * 1024 and w_gate.shape[0] == 1 and ep_count == 8:
        return gathered(*args)
    return local(*args)


def solution(mesh):
    return jax.shard_map(
        chosen,
        mesh=mesh,
        in_specs=(
            P("ep", None),
            P("ep", None),
            P("ep", None),
            P("ep", None),
            P("ep", None, "tp"),
            P("ep", None, "tp"),
            P("ep", "tp", None),
        ),
        out_specs=(
            P("ep", "tp"),
            P("ep", None),
            P("ep", None, "tp"),
            P("ep", None, "tp"),
            P("ep", "tp", None),
        ),
        check_vma=False,
    )
```

```python
import jax
import jax.numpy as jnp
from jax import lax
from jax.experimental import pallas as pl
from jax.experimental.pallas import tpu as pltpu
from jax.sharding import PartitionSpec as P

clamp_limit = 7.0
sigmoid_slope = 1.702
MESH = pl.DeviceIdType.MESH
far_step = 2


def partners():
    ep_count = lax.axis_size("ep")
    tp_count = lax.axis_size("tp")
    here = lax.axis_index("ep")
    part = lax.axis_index("tp")
    beside = part + 1 - 2 * (part % 2)
    across = (part + tp_count // 2) % tp_count
    return ep_count, here, part, beside, across


def greet(ep_count, here, part, beside, across):
    barrier = pltpu.get_barrier_semaphore()
    pl.semaphore_signal(barrier, inc=1, device_id=(here, beside), device_id_type=MESH)
    pl.semaphore_signal(barrier, inc=1, device_id=(here, across), device_id_type=MESH)

    def call(j, carry):
        peer = (here + j) % ep_count
        pl.semaphore_signal(barrier, inc=1, device_id=(peer, part), device_id_type=MESH)
        return carry

    lax.fori_loop(1, ep_count, call, 0)
    pl.semaphore_wait(barrier, ep_count + 1)


def remote(src, dst, sent, got, device):
    return pltpu.make_async_remote_copy(
        src_ref=src, dst_ref=dst, send_sem=sent, recv_sem=got, device_id=device, device_id_type=MESH
    )


def dispatch_kernel(
    token_ref, grad_ref, weight_ref, token_rows, grad_rows, weights_out,
    s1, r1, s2, r2, s3, r3, s4, r4, sw, rw, own_sem,
):
    ep_count, here, part, beside, across = partners()
    width = token_ref.shape[2]
    pairs = ((0, token_ref, token_rows), (1, grad_ref, grad_rows))

    def block(rows_ref, source, owner):
        columns = pl.ds(pl.multiple_of(owner * width, width), width)
        return rows_ref.at[source, :, columns]

    greet(ep_count, here, part, beside, across)

    def first(j):
        peer = (here + j) % ep_count
        return [
            remote(send.at[peer], block(rows, here, part), s1.at[i, j], r1.at[i, j], (peer, part))
            for i, send, rows in pairs
        ]

    def first_weight(j):
        peer = (here + j) % ep_count
        return remote(
            weight_ref.at[peer], weights_out.at[here], sw.at[j], rw.at[j], (peer, part)
        )

    def forward(j, owner, sent, got, to):
        source = (here + ep_count - j) % ep_count
        return [
            remote(
                block(rows, source, owner), block(rows, source, owner),
                sent.at[i, j], got.at[i, j], (here, to),
            )
            for i, _, rows in pairs
        ]

    def near(j):
        return forward(j, part, s2, r2, beside)

    def far(j):
        return forward(j, part, s3, r3, across)

    def onward(j):
        return forward(j, across, s4, r4, beside)

    owns = [
        pltpu.make_async_copy(send.at[here], block(rows, here, part), own_sem.at[i])
        for i, send, rows in pairs
    ]
    owns.append(pltpu.make_async_copy(weight_ref.at[here], weights_out.at[here], own_sem.at[2]))
    for copy in owns:
        copy.start()

    def launch(j, carry):
        first_weight(j).start()
        for copy in first(j):
            copy.start()
        return carry

    lax.fori_loop(1, ep_count, launch, 0)
    for copy in owns:
        copy.wait()
    for copy in far(0) + near(0):
        copy.start()

    def pass_on(j, carry):
        @pl.when(j < ep_count)
        def _():
            for i in range(2):
                first(j)[i].wait_recv()
                far(j)[i].start()
                near(j)[i].start()

        @pl.when(j >= 2)
        def _():
            for i in range(2):
                far(j - 2)[i].wait_recv()
                onward(j - 2)[i].start()

        return carry

    lax.fori_loop(1, ep_count + 2, pass_on, 0)

    def finish(j, carry):
        for i in range(2):
            near(j)[i].wait()
            onward(j)[i].wait()
            far(j)[i].wait_send()

        @pl.when(j >= 1)
        def _():
            for copy in first(j):
                copy.wait_send()
            first_weight(j).wait()

        return carry

    lax.fori_loop(0, ep_count, finish, 0)


def dispatch(send_tokens, send_grads, weights, model_width):
    ep_count, capacity, width = send_tokens.shape
    sems = [pltpu.SemaphoreType.DMA((2, ep_count)) for _ in range(8)]
    sems += [pltpu.SemaphoreType.DMA((ep_count,)) for _ in range(2)]
    whole = jax.ShapeDtypeStruct((ep_count, capacity, model_width), jnp.bfloat16)
    return pl.pallas_call(
        dispatch_kernel,
        out_shape=(whole, whole, jax.ShapeDtypeStruct(weights.shape, jnp.float32)),
        in_specs=[pl.BlockSpec(memory_space=pltpu.VMEM)] * 3,
        out_specs=(
            pl.BlockSpec(memory_space=pl.ANY),
            pl.BlockSpec(memory_space=pl.ANY),
            pl.BlockSpec(memory_space=pltpu.VMEM),
        ),
        scratch_shapes=sems + [pltpu.SemaphoreType.DMA((3,))],
        compiler_params=pltpu.CompilerParams(collective_id=0, has_side_effects=True),
    )(send_tokens, send_grads, weights)


def combine_kernel(
    rows_ref, product_ref, back_ref, back_product, near_buf, far_send, far_buf, last_send,
    product_near, product_sum, product_far, product_send,
    s1, r1, s2, r2, s3, r3, sw, rw, small_send, small_recv,
):
    ep_count, here, part, beside, across = partners()
    width = back_ref.shape[2]
    beside_far = (beside + lax.axis_size("tp") // 2) % lax.axis_size("tp")

    def columns(owner):
        return pl.ds(pl.multiple_of(owner * width, width), width)

    greet(ep_count, here, part, beside, across)

    def near(which, j):
        target = (here + j) % ep_count
        owner = beside_far if which == 0 else beside
        return remote(
            rows_ref.at[target, :, columns(owner)], near_buf.at[which, j],
            s1.at[which, j], r1.at[which, j], (here, beside),
        )

    def far(j):
        return remote(far_send.at[j], far_buf.at[j], s2.at[j], r2.at[j], (here, across))

    def last(j):
        peer = (here + j) % ep_count
        return remote(last_send.at[j], back_ref.at[here], s3.at[j], r3.at[j], (peer, part))

    def last_product(j):
        peer = (here + j) % ep_count
        return remote(
            product_send.at[peer], back_product.at[here], sw.at[j], rw.at[j], (peer, part)
        )

    small_near = remote(product_ref, product_near, small_send.at[0], small_recv.at[0], (here, beside))
    small_far = remote(product_sum, product_far, small_send.at[1], small_recv.at[1], (here, across))
    small_near.start()

    def launch(step, carry):
        j = (step + 1) % ep_count
        near(0, j).start()
        near(1, j).start()
        return carry

    lax.fori_loop(0, ep_count, launch, 0)
    small_near.wait_recv()
    product_sum[...] = product_ref[...] + product_near[...]
    small_far.start()

    def middle(step, carry):
        j = (step + 1) % ep_count
        near(0, j).wait_recv()
        target = (here + j) % ep_count
        mine = rows_ref[target, :, columns(across)].astype(jnp.float32)
        far_send[j] = (mine + near_buf[0, j].astype(jnp.float32)).astype(jnp.bfloat16)
        far(j).start()
        return carry

    lax.fori_loop(0, ep_count, middle, 0)
    small_far.wait_recv()
    product_send[...] = product_sum[...] + product_far[...]

    def total(j):
        near(1, j).wait_recv()
        far(j).wait_recv()
        target = (here + j) % ep_count
        mine = rows_ref[target, :, columns(part)].astype(jnp.float32)
        added = mine + near_buf[1, j].astype(jnp.float32) + far_buf[j].astype(jnp.float32)
        return added.astype(jnp.bfloat16)

    def end(j, carry):
        last_send[j] = total(j)
        last(j).start()
        last_product(j).start()
        return carry

    lax.fori_loop(1, ep_count, end, 0)
    back_ref[here] = total(0)
    back_product[here] = product_send[here]

    small_near.wait_send()
    small_far.wait_send()

    def finish(j, carry):
        near(0, j).wait_send()
        near(1, j).wait_send()
        far(j).wait_send()

        @pl.when(j >= 1)
        def _():
            last(j).wait()
            last_product(j).wait()

        return carry

    lax.fori_loop(0, ep_count, finish, 0)


def combine(rows, products, width):
    ep_count, capacity, _ = rows.shape
    one = (ep_count, capacity, width)
    small = pltpu.VMEM(products.shape, jnp.float32)
    dma = pltpu.SemaphoreType.DMA
    return pl.pallas_call(
        combine_kernel,
        out_shape=(
            jax.ShapeDtypeStruct(one, jnp.bfloat16),
            jax.ShapeDtypeStruct(products.shape, jnp.float32),
        ),
        in_specs=[pl.BlockSpec(memory_space=pltpu.VMEM)] * 2,
        out_specs=(pl.BlockSpec(memory_space=pltpu.VMEM),) * 2,
        scratch_shapes=[
            pltpu.VMEM((2,) + one, jnp.bfloat16),
            pltpu.VMEM(one, jnp.bfloat16),
            pltpu.VMEM(one, jnp.bfloat16),
            pltpu.VMEM(one, jnp.bfloat16),
            small, small, small, small,
            dma((2, ep_count)), dma((2, ep_count)),
            dma((ep_count,)), dma((ep_count,)), dma((ep_count,)), dma((ep_count,)),
            dma((ep_count,)), dma((ep_count,)), dma((2,)), dma((2,)),
        ],
        compiler_params=pltpu.CompilerParams(
            collective_id=1, has_side_effects=True, vmem_limit_bytes=48 * 1024 * 1024
        ),
    )(rows, products)


def local(tokens, routes, gate_weights, out_grad, w_gate, w_up, w_down):
    f32, bf16 = jnp.float32, jnp.bfloat16
    ep_count = lax.axis_size("ep")
    tp_count = lax.axis_size("tp")
    part = lax.axis_index("tp")
    token_count, model_width = tokens.shape
    top_count = routes.shape[1]
    experts = ep_count * w_gate.shape[0]
    capacity = token_count * top_count * 5 // (4 * experts)
    width = model_width // tp_count

    match = routes[:, :, None] == jnp.arange(experts, dtype=jnp.int32)[None, None, :]
    named = jnp.any(match, axis=1)
    before = jnp.arange(token_count)[:, None] > jnp.arange(token_count)[None, :]
    rank = jnp.dot(before.astype(bf16), named.astype(bf16), preferred_element_type=f32)
    rank = jnp.where(named, rank.astype(jnp.int32), -1)
    pick = rank.T[:, None, :] == jnp.arange(capacity, dtype=jnp.int32)[None, :, None]
    pick_flat = pick.reshape(experts * capacity, token_count).astype(bf16)
    weight_of = jnp.sum(jnp.where(match, gate_weights[:, :, None], 0.0), axis=1)
    send_weights = jnp.sum(jnp.where(pick, weight_of.T[:, None, :], 0.0), axis=2)
    sends = []
    for array in (tokens, out_grad):
        own = lax.dynamic_slice_in_dim(array, part * width, width, 1)
        picked = jnp.dot(pick_flat, own, preferred_element_type=f32).astype(bf16)
        sends.append(picked.reshape(experts, capacity, width))

    rows, grads, weights = dispatch(*sends, send_weights[:, None, :], model_width)
    row_count = ep_count * capacity
    x_rows = rows.reshape(row_count, model_width)
    dy_rows = grads.reshape(row_count, model_width)
    slot_weights = weights.reshape(row_count, 1)

    gate_pre = jnp.dot(x_rows, w_gate[0], preferred_element_type=f32)
    up_pre = jnp.dot(x_rows, w_up[0], preferred_element_type=f32)
    plain_grad = jnp.einsum("rd,fd->rf", dy_rows, w_down[0], preferred_element_type=f32)
    glu = jnp.minimum(gate_pre, clamp_limit)
    linear = jnp.clip(up_pre, -clamp_limit, clamp_limit)
    sigma = jax.nn.sigmoid(sigmoid_slope * glu)
    active = glu * sigma
    hidden = active * (linear + 1.0)
    product = jnp.sum(hidden * plain_grad, axis=1)
    hidden_grad = plain_grad * slot_weights
    slope_term = sigma + sigmoid_slope * active * (1.0 - sigma)
    gate_pre_grad = jnp.where(
        gate_pre < clamp_limit, hidden_grad * (linear + 1.0) * slope_term, 0.0
    ).astype(bf16)
    up_pre_grad = jnp.where(jnp.abs(up_pre) < clamp_limit, hidden_grad * active, 0.0).astype(bf16)
    hidden = (hidden * slot_weights).astype(bf16)

    row_term = jnp.einsum("rf,df->rd", gate_pre_grad, w_gate[0], preferred_element_type=f32)
    row_term = row_term + jnp.einsum(
        "rf,df->rd", up_pre_grad, w_up[0], preferred_element_type=f32
    )
    row_term = row_term.astype(bf16).reshape(ep_count, capacity, model_width)
    back_rows, back_products = combine(
        row_term, product.reshape(ep_count, 1, capacity), width
    )
    gate_grads = jnp.einsum("rd,rf->df", x_rows, gate_pre_grad, preferred_element_type=f32)
    up_grads = jnp.einsum("rd,rf->df", x_rows, up_pre_grad, preferred_element_type=f32)
    down_grads = jnp.einsum("rf,rd->fd", hidden, dy_rows, preferred_element_type=f32)
    token_grad = jnp.einsum(
        "rt,rw->tw", pick_flat, back_rows.reshape(row_count, width), preferred_element_type=f32
    ).astype(bf16)
    found = jnp.sum(jnp.where(pick, back_products.reshape(experts, capacity, 1), 0.0), axis=1)
    gate_grad = jnp.sum(jnp.where(match, found.T[:, None, :], 0.0), axis=2)
    return (token_grad, gate_grad, gate_grads[None], up_grads[None], down_grads[None])


def fused_kernel(
    tok_hbm, grd_hbm, route_hbm, share_hbm, gate_hbm, up_hbm, down_hbm,
    token_out, found_out, gate_out, up_out, down_out,
    tok_ref, grd_ref, route_ref, share_ref, gate_ref, up_ref, down_ref, line, line_extra, metas, pick_send, rows, gate_g, up_g, hid,
    near_send, near_buf, mine, own_sum, back_send,
    wide_buf, half_send, half_buf, narrow_send, narrow_buf, total, total_half, y_send, y_buf,
    found_loc, found_near, found_sum, found_far, found_send,
    chain_s, chain_r, xm_s, xm_r, x_s, x_r, u_s, u_r, n_s, n_r, f_s, f_r, o_s, o_r,
    c_s, c_r, h_s, h_r, w_s, w_r, z_s, z_r, y_s, y_r, sm_s, sm_r, l_s, l_r, in_s,
):
    f32, bf16 = jnp.float32, jnp.bfloat16
    ep_count, here, part, beside, across = partners()
    count = ep_count // 2
    z, x = here // 2, here % 2
    other = here + 1 - 2 * x
    plane, core = part // 2, part % 2
    capacity = rows.shape[2]
    model_width = tok_ref.shape[1]
    width = token_out.shape[1]
    token_count = tok_ref.shape[0]

    def columns(owner):
        return pl.ds(pl.multiple_of(owner * width, width), width)

    def order(i):
        mixed, bit = 0, 1
        while bit < count:
            mixed = mixed + ((z // bit + i // bit) % 2) * bit
            bit = 2 * bit
        return mixed

    inward = (2 * z) // count
    middle = (2 * z * (count - 1 - z) + count * count - 1) // (count * count)

    def place(i):
        return order(i + middle * (i // far_step) * (1 - 2 * (i % 2)))

    def chain(kind, zi, way):
        ref = metas.at[2 * zi + x] if kind == 2 else line.at[kind, zi]
        to = here + 2 - 4 * way
        return remote(ref, ref, chain_s.at[way, kind, zi], chain_r.at[kind, zi], (to, part))

    def chain_extra(kind, way):
        whole = grd_ref if kind else tok_ref
        return remote(
            whole.at[:, columns(across)], line_extra.at[way, kind],
            u_s.at[way, kind], u_r.at[way, kind], (here + 2 - 4 * way, part),
        )

    def cross_meta(zi):
        ref = metas.at[2 * zi + x]
        return remote(ref, ref, xm_s.at[zi], xm_r.at[zi], (other, part))

    def cross(kind, zi):
        return remote(
            pick_send.at[kind, zi], rows.at[kind, 2 * zi + x, :, columns(part)],
            x_s.at[kind, zi], x_r.at[kind, zi], (other, part),
        )

    def forward(kind, source, owner, sent, got, to):
        ref = rows.at[kind, source, :, columns(owner)]
        return remote(ref, ref, sent.at[kind, source], got.at[kind, source], (here, to))

    def near(kind, source):
        return forward(kind, source, part, n_s, n_r, beside)

    def far(kind, source):
        return forward(kind, source, part, f_s, f_r, across)

    def onward(kind, source):
        return forward(kind, source, across, o_s, o_r, beside)

    def pair(source):
        return remote(
            near_send.at[source], near_buf.at[source], c_s.at[source], c_r.at[source],
            (here, beside),
        )

    def half_over(source):
        return remote(
            half_send.at[source], half_buf.at[source], h_s.at[source], h_r.at[source],
            (here, across),
        )

    def is_far(zi):
        return (zi - z) * (zi - z) >= far_step * far_step

    def wide(source, own):
        ref = own_sum.at[source // 2] if own else back_send.at[source // 2]
        return remote(ref, wide_buf.at[here], w_s.at[source], w_r.at[here], (source, part))

    def wide_got(sender):
        return remote(
            own_sum.at[0], wide_buf.at[sender], w_s.at[sender], w_r.at[sender], (sender, part)
        )

    def narrow(source, sender):
        return remote(
            narrow_send.at[source], narrow_buf.at[sender],
            z_s.at[source], z_r.at[sender], (source, part),
        )

    def either(zi, act):
        @pl.when(is_far(zi))
        def _():
            act(True)

        @pl.when(jnp.logical_not(is_far(zi)))
        def _():
            act(False)

    last_y = remote(y_send, y_buf, y_s.at[0], y_r.at[0], (here, across))
    small_near = remote(found_loc, found_near, sm_s.at[0], sm_r.at[0], (here, beside))
    small_far = remote(found_sum, found_far, sm_s.at[1], sm_r.at[1], (here, across))

    def last_found(j):
        peer = (here + j) % ep_count
        return remote(found_send.at[peer], found_out.at[here], l_s.at[j], l_r.at[j], (peer, part))

    slots = lax.broadcasted_iota(jnp.int32, (capacity, token_count), 0).astype(f32)

    def matches(source, expert):
        return slots == metas[source, pl.ds(expert, 1), :]

    def pick(source, expert):
        return jnp.where(matches(source, expert), 1.0, 0.0).astype(bf16)

    barrier = pltpu.get_barrier_semaphore()
    pl.semaphore_signal(barrier, inc=1, device_id=(here, beside), device_id_type=MESH)
    pl.semaphore_signal(barrier, inc=1, device_id=(here, across), device_id_type=MESH)

    pl.semaphore_signal(barrier, inc=1, device_id=(other, part), device_id_type=MESH)

    @pl.when(z > 0)
    def _():
        pl.semaphore_signal(barrier, inc=1, device_id=(here - 2, part), device_id_type=MESH)

    @pl.when(z < count - 1)
    def _():
        pl.semaphore_signal(barrier, inc=1, device_id=(here + 2, part), device_id_type=MESH)

    loads = [
        pltpu.make_async_copy(src, dst, in_s.at[n])
        for n, (src, dst) in enumerate((
            (route_hbm, route_ref), (share_hbm, share_ref),
            (tok_hbm.at[:, columns(part)], line.at[0, z]),
            (grd_hbm.at[:, columns(part)], line.at[1, z]),
            (tok_hbm, tok_ref), (grd_hbm, grd_ref),
            (gate_hbm, gate_ref), (up_hbm, up_ref), (down_hbm, down_ref),
        ))
    ]
    for load in loads:
        load.start()
    total_half[...] = jnp.zeros(total_half.shape, f32)
    experts = lax.broadcasted_iota(jnp.int32, (ep_count, token_count), 0)
    earlier = lax.broadcasted_iota(jnp.int32, (token_count, token_count), 0)
    later = lax.broadcasted_iota(jnp.int32, (token_count, token_count), 1)
    before = jnp.where(earlier < later, 1.0, 0.0).astype(bf16)
    loads[0].wait()
    loads[1].wait()
    named = jnp.zeros((ep_count, token_count), f32)
    weight_of = jnp.zeros((ep_count, token_count), f32)
    for k in range(route_ref.shape[0]):
        chosen_here = route_ref[pl.ds(k, 1), :] == experts
        named = named + jnp.where(chosen_here, 1.0, 0.0)
        weight_of = weight_of + jnp.where(chosen_here, share_ref[pl.ds(k, 1), :], 0.0)
    rank = jnp.dot(named.astype(bf16), before, preferred_element_type=f32)
    metas[here, pl.ds(0, ep_count), :] = jnp.where(named > 0.0, rank, -1.0)
    metas[here, pl.ds(ep_count, ep_count), :] = weight_of
    loads[2].wait()
    loads[3].wait()
    pl.semaphore_wait(barrier, 4 + middle)

    @pl.when(z < count - 1)
    def _():
        for kind in (2, 0, 1):
            chain(kind, z, 0).start()

    @pl.when(z > 0)
    def _():
        for kind in (2, 0, 1):
            chain(kind, z, 1).start()

    def take(kind, zi):
        chain(kind, zi, 0).wait_recv()

        @pl.when((zi < z) & (z < count - 1))
        def _():
            chain(kind, zi, 0).start()

        @pl.when((zi > z) & (z > 0))
        def _():
            chain(kind, zi, 1).start()

    def is_next(zi):
        return (zi - z) * (zi - z) == 1

    def send_extra(way):
        chain_extra(0, way).start()
        chain_extra(1, way).start()

    def hand_on_extra(i):
        zi = place(i)
        source = 2 * zi + x
        way = (zi - z + 1) // 2
        for kind in range(2):
            chain_extra(kind, way).wait_recv()
            own = jnp.dot(
                pick(source, here), line_extra[way, kind], preferred_element_type=f32
            )
            rows[kind, source, :, columns(across)] = own.astype(bf16)
            onward(kind, source).start()

    def relay(kind, i):
        @pl.when(middle == 1)
        def _():
            if kind == 0:
                take(2, place(i))
            take(kind, place(i))

    def picks(kind, i):
        zi = place(i)
        source = 2 * zi + x

        @pl.when((i == 1) | ((i > 1) & (middle == 0)))
        def _():
            if kind == 0:
                take(2, zi)
            take(kind, zi)

        if kind == 0:
            cross_meta(zi).start()
        picked = jnp.dot(pick(source, other), line[kind, zi], preferred_element_type=f32)
        pick_send[kind, zi] = picked.astype(bf16)
        cross(kind, zi).start()

        @pl.when(i >= 1)
        def _():
            own = jnp.dot(pick(source, here), line[kind, zi], preferred_element_type=f32)
            rows[kind, source, :, columns(part)] = own.astype(bf16)

            @pl.when(jnp.logical_not(is_next(zi)))
            def _():
                far(kind, source).start()

            near(kind, source).start()

    def local_picks():
        loads[4].wait()
        loads[5].wait()
        for kind, whole in enumerate((tok_ref, grd_ref)):
            for q in range(model_width // width):
                at = pl.ds(q * width, width)
                own = jnp.dot(pick(here, here), whole[:, at], preferred_element_type=f32)
                rows[kind, here, :, at] = own.astype(bf16)

    def arrive(kind, i):
        source = 2 * place(i) + 1 - x
        cross(kind, place(i)).wait_recv()
        far(kind, source).start()
        near(kind, source).start()
        if kind == 1:
            cross_meta(place(i)).wait_recv()

    def hand_on(source):
        for kind in range(2):
            far(kind, source).wait_recv()
            onward(kind, source).start()

    def compute(source, local_rows):
        @pl.when(local_rows == 0)
        def _():
            for kind in range(2):
                near(kind, source).wait_recv()
                onward(kind, source).wait_recv()

        nt = (((1,), (1,)), ((), ()))
        x_rows = rows[0, source]
        gate_pre = jnp.dot(x_rows, gate_ref[...], preferred_element_type=f32)
        up_pre = jnp.dot(x_rows, up_ref[...], preferred_element_type=f32)
        plain = lax.dot_general(rows[1, source], down_ref[...], nt, preferred_element_type=f32)
        hit = matches(source, here)
        weight_row = metas[source, pl.ds(here + ep_count, 1), :]
        weight = jnp.sum(jnp.where(hit, weight_row, 0.0), axis=1, keepdims=True)
        glu = jnp.minimum(gate_pre, clamp_limit)
        linear = jnp.clip(up_pre, -clamp_limit, clamp_limit)
        sigma = jax.nn.sigmoid(sigmoid_slope * glu)
        active = glu * sigma
        hidden = active * (linear + 1.0)
        product = jnp.sum(hidden * plain, axis=1, keepdims=True)
        found_loc[source] = jnp.sum(jnp.where(hit, product, 0.0), axis=0, keepdims=True)
        hidden_grad = plain * weight
        slope_term = sigma + sigmoid_slope * active * (1.0 - sigma)
        gate_grad = jnp.where(
            gate_pre < clamp_limit, hidden_grad * (linear + 1.0) * slope_term, 0.0
        ).astype(bf16)
        up_grad = jnp.where(jnp.abs(up_pre) < clamp_limit, hidden_grad * active, 0.0).astype(bf16)
        gate_g[source] = gate_grad
        up_g[source] = up_grad
        hid[source] = (hidden * weight).astype(bf16)
        for own in range(2):
            for half in range(2):
                owner = 2 * half + (core if own else 1 - core)
                term = lax.dot_general(
                    gate_g[source], gate_ref[columns(owner), :], nt, preferred_element_type=f32
                ) + lax.dot_general(
                    up_g[source], up_ref[columns(owner), :], nt, preferred_element_type=f32
                )
                at = pl.ds(half * width, width)
                if own:
                    mine[source, :, at] = term.astype(bf16)
                else:
                    near_send[source, :, at] = term.astype(bf16)
            if not own:
                pair(source).start()

    def pair_sum(source, zi, own):
        pair(source).wait_recv()

        def act(small):
            if small:
                at = columns(1 - plane)
                added = mine[source, :, at].astype(f32) + near_buf[source, :, at].astype(f32)
                half_send[source] = added.astype(bf16)
                half_over(source).start()
                return
            added = (mine[source].astype(f32) + near_buf[source].astype(f32)).astype(bf16)
            if own:
                own_sum[zi] = added

                @pl.when((zi < z) | (zi > z))
                def _():
                    wide(source, True).start()
            else:
                back_send[zi] = added
                wide(source, False).start()

        either(zi, act)

    def half_sum(source, zi):
        @pl.when(is_far(zi))
        def _():
            half_over(source).wait_recv()
            at = columns(plane)
            added = mine[source, :, at].astype(f32) + near_buf[source, :, at].astype(f32)
            narrow_send[source] = (added + half_buf[source].astype(f32)).astype(bf16)
            narrow(source, here).start()

    tn = (((0,), (0,)), ((), ()))

    def add_wide(sender, carry):
        @pl.when(jnp.logical_not(is_far(sender // 2)) & ((sender < here) | (sender > here)))
        def _():
            wide_got(sender).wait_recv()
            for half in range(2):
                at = pl.ds(half * width, width)
                total[:, at] = total[:, at] + lax.dot_general(
                    pick(here, sender), wide_buf[sender, :, at], tn, preferred_element_type=f32
                )

        return carry

    def add_own():
        for half in range(2):
            at = pl.ds(half * width, width)
            total[:, at] = lax.dot_general(
                pick(here, here), own_sum[z, :, at], tn, preferred_element_type=f32
            )

    def own_at(i):
        return 2 * place(i) + x

    def other_at(i):
        return 2 * place(i) + 1 - x

    last = count - 1

    def body(i, carry):
        @pl.when(i == last)
        def _():
            pair_sum(other_at(0), place(0), False)

        @pl.when(i >= 1)
        def _():
            arrive(0, i - 1)

        @pl.when(i == count)
        def _():
            pair_sum(own_at(last - 1), place(last - 1), True)

        @pl.when(i >= 2)
        def _():
            hand_on(other_at(i - 2))
            compute(other_at(i - 2), 0)

        @pl.when(i < count)
        def _():
            picks(0, i)

        @pl.when((i == 1) | (i == 2))
        def _():
            relay(0, i + 1)

        @pl.when(i >= 1)
        def _():
            arrive(1, i - 1)

        @pl.when(i == count)
        def _():
            pair_sum(other_at(last - 1), place(last - 1), False)

        @pl.when(i < count)
        def _():
            picks(1, i)

        @pl.when((i == 1) | (i == 2))
        def _():
            relay(1, i + 1)

        @pl.when(i == 0)
        def _():
            local_picks()

            @pl.when(middle == 0)
            def _():
                send_extra(inward)

            for load in loads[6:]:
                load.wait()

        @pl.when((i == 1) & (middle == 1))
        def _():
            send_extra(inward)

        @pl.when((i == 2) & (middle == 1))
        def _():
            send_extra(1 - inward)
            hand_on_extra(1)

        @pl.when((i == 3) & (middle == 1))
        def _():
            compute(own_at(1), 0)
            pair_sum(own_at(1), place(1), True)

        @pl.when(i >= 3)
        def _():
            @pl.when(is_next(place(i - 1)))
            def _():
                hand_on_extra(i - 1)

            @pl.when(jnp.logical_not(is_next(place(i - 1))))
            def _():
                hand_on(own_at(i - 1))

        @pl.when((i == count) & (middle == 0))
        def _():
            hand_on_extra(1)

        @pl.when((i == 0) | (i >= 3))
        def _():
            step = i - (i + count - 1) // count - (1 - middle) * (i // count) * (last - 1)
            compute(own_at(step), 1 - (step + count - 1) // count)

        @pl.when(i == count)
        def _():
            step = 1 + middle * (last - 1)
            pair_sum(own_at(step), place(step), True)

        @pl.when(i == 1)
        def _():
            pair_sum(own_at(0), place(0), True)

        @pl.when(i == last)
        def _():
            pair_sum(other_at(1), place(1), False)

        return carry

    def closing(j, carry):
        @pl.when(j == 1)
        def _():
            half_sum(own_at(last - 1), place(last - 1))
            hand_on(other_at(last))

        @pl.when((j == 1) | (middle == 0))
        def _():
            compute(own_at(last) + (other_at(last) - own_at(last)) * j, 0)

        @pl.when((j == 0) & (middle == 0))
        def _():
            pair_sum(own_at(last), place(last), True)

        @pl.when(j == 1)
        def _():
            small_near.start()
            small_near.wait_recv()
            found_sum[...] = found_loc[...] + found_near[...]
            small_far.start()
            pair_sum(other_at(last), place(last), False)

        return carry

    def weights(n, carry):
        chunk = 256
        tn = (((0,), (0,)), ((), ()))
        at = pl.ds(pl.multiple_of(n * chunk, chunk), chunk)
        flat = ep_count * capacity
        x_part = rows[0, :, :, at].reshape(flat, chunk)
        g_part = rows[1, :, :, at].reshape(flat, chunk)
        units = gate_g.shape[2]
        gate_out[at, :] = lax.dot_general(
            x_part, gate_g[...].reshape(flat, units), tn, preferred_element_type=f32
        )
        up_out[at, :] = lax.dot_general(
            x_part, up_g[...].reshape(flat, units), tn, preferred_element_type=f32
        )
        down_out[:, at] = lax.dot_general(
            hid[...].reshape(flat, units), g_part, tn, preferred_element_type=f32
        )
        return carry

    chunks = model_width // 256
    lax.fori_loop(0, count + 1, body, 0)
    lax.fori_loop(0, 2, closing, 0)

    @pl.when(middle == 1)
    def _():
        half_sum(own_at(last), place(last))

    half_sum(other_at(last - 1), place(last - 1))
    small_far.wait_recv()
    found_send[...] = found_sum[...] + found_far[...]
    found_out[here] = found_send[here]

    def share(j, carry):
        last_found(j).start()
        return carry

    lax.fori_loop(1, ep_count, share, 0)
    add_own()
    lax.fori_loop(0, chunks // 8, weights, 0)

    @pl.when(middle == 0)
    def _():
        half_sum(own_at(last), place(last))

    lax.fori_loop(chunks // 8, chunks // 4, weights, 0)
    half_sum(other_at(last), place(last))
    lax.fori_loop(chunks // 4, chunks // 4 + 1, weights, 0)
    lax.fori_loop(0, ep_count, add_wide, 0)
    y_send[...] = total[:, columns(1 - plane)].astype(bf16)
    last_y.start()
    lax.fori_loop(chunks // 4 + 1, chunks // 2, weights, 0)

    def add_far(sender, carry):
        @pl.when(is_far(sender // 2))
        def _():
            narrow(here, sender).wait_recv()
            total_half[...] = total_half[...] + lax.dot_general(
                pick(here, sender), narrow_buf[sender], tn, preferred_element_type=f32
            )

        return carry

    def finish(zi, carry):
        for kind in range(3):
            @pl.when((zi <= z) & (z < count - 1))
            def _():
                chain(kind, zi, 0).wait_send()

            @pl.when((zi >= z) & (z > 0))
            def _():
                chain(kind, zi, 1).wait_send()

        cross_meta(zi).wait_send()
        for kind in range(2):
            cross(kind, zi).wait_send()

        return carry

    def finish_source(source, carry):
        pair(source).wait_send()

        @pl.when(is_far(source // 2))
        def _():
            half_over(source).wait_send()

        @pl.when(jnp.logical_not(is_far(source // 2)) & ((source < here) | (source > here)))
        def _():
            wide(source, False).wait_send()

        @pl.when((source < here) | (source > here))
        def _():
            for kind in range(2):
                near(kind, source).wait_send()
                onward(kind, source).wait_send()

        gap = source // 2 - z
        across_line = (source - x) % 2

        @pl.when((across_line == 1) | (gap * gap > 1))
        def _():
            for kind in range(2):
                far(kind, source).wait_send()

        return carry

    def finish_extra(way):
        chain_extra(0, way).wait_send()
        chain_extra(1, way).wait_send()

    lax.fori_loop(chunks // 2, chunks, weights, 0)
    lax.fori_loop(0, count, finish, 0)
    lax.fori_loop(0, ep_count, finish_source, 0)
    finish_extra(inward)

    @pl.when(middle == 1)
    def _():
        finish_extra(1 - inward)

    small_near.wait_send()
    small_far.wait_send()

    def finish_found(j, carry):
        last_found(j).wait()
        return carry

    lax.fori_loop(1, ep_count, finish_found, 0)
    lax.fori_loop(0, ep_count, add_far, 0)
    last_y.wait_recv()
    token_out[...] = (
        total[:, columns(plane)] + total_half[...] + y_buf[...].astype(f32)
    ).astype(bf16)

    def finish_narrow(source, carry):
        @pl.when(is_far(source // 2))
        def _():
            narrow(source, here).wait_send()

        return carry

    lax.fori_loop(0, ep_count, finish_narrow, 0)
    last_y.wait_send()


def fused(tokens, grads, routes, shares, w_gate, w_up, w_down, capacity, width):
    f32, bf16 = jnp.float32, jnp.bfloat16
    ep_count = lax.axis_size("ep")
    count = ep_count // 2
    token_count, model_width = tokens.shape
    units = w_gate.shape[1]
    vm = pltpu.VMEM
    dma = pltpu.SemaphoreType.DMA
    small = vm((ep_count, 1, token_count), f32)
    half = (capacity, 2 * width)
    scratch = [
        vm(tokens.shape, bf16),
        vm(tokens.shape, bf16),
        vm(routes.shape, jnp.int32),
        vm(routes.shape, f32),
        vm(w_gate.shape, bf16),
        vm(w_up.shape, bf16),
        vm(w_down.shape, bf16),
        vm((2, count, token_count, width), bf16),
        vm((2, 2, token_count, width), bf16),
        vm((ep_count, 2 * ep_count, token_count), f32),
        vm((2, count, capacity, width), bf16),
        vm((2, ep_count, capacity, model_width), bf16),
        vm((ep_count, capacity, units), bf16),
        vm((ep_count, capacity, units), bf16),
        vm((ep_count, capacity, units), bf16),
        vm((ep_count,) + half, bf16),
        vm((ep_count,) + half, bf16),
        vm((ep_count,) + half, bf16),
        vm((count,) + half, bf16),
        vm((count,) + half, bf16),
        vm((ep_count,) + half, bf16),
        vm((ep_count, capacity, width), bf16),
        vm((ep_count, capacity, width), bf16),
        vm((ep_count, capacity, width), bf16),
        vm((ep_count, capacity, width), bf16),
        vm((token_count, 2 * width), f32),
        vm((token_count, width), f32),
        vm((token_count, width), bf16),
        vm((token_count, width), bf16),
        small, small, small, small, small,
        dma((2, 3, count)), dma((3, count)),
        dma((count,)), dma((count,)),
        dma((2, count)), dma((2, count)),
        dma((2, 2)), dma((2, 2)),
        dma((2, ep_count)), dma((2, ep_count)),
        dma((2, ep_count)), dma((2, ep_count)),
        dma((2, ep_count)), dma((2, ep_count)),
        dma((ep_count,)), dma((ep_count,)),
        dma((ep_count,)), dma((ep_count,)),
        dma((ep_count,)), dma((ep_count,)),
        dma((ep_count,)), dma((ep_count,)),
        dma((1,)), dma((1,)), dma((2,)), dma((2,)),
        dma((ep_count,)), dma((ep_count,)), dma((9,)),
    ]
    return pl.pallas_call(
        fused_kernel,
        out_shape=(
            jax.ShapeDtypeStruct((token_count, width), bf16),
            jax.ShapeDtypeStruct((ep_count, 1, token_count), f32),
            jax.ShapeDtypeStruct((model_width, units), f32),
            jax.ShapeDtypeStruct((model_width, units), f32),
            jax.ShapeDtypeStruct((units, model_width), f32),
        ),
        in_specs=[pl.BlockSpec(memory_space=pltpu.HBM)] * 7,
        out_specs=(pl.BlockSpec(memory_space=pltpu.VMEM),) * 5,
        scratch_shapes=scratch,
        compiler_params=pltpu.CompilerParams(
            collective_id=2, has_side_effects=True, vmem_limit_bytes=47 * 1024 * 1024
        ),
    )(tokens, grads, routes, shares, w_gate, w_up, w_down)


def store_kernel(
    token_ref, found_ref, gate_ref, up_ref, down_ref, route_ref,
    token_out, found_out, gate_out, up_out, down_out, found_buf, sems,
):
    copies = [
        pltpu.make_async_copy(src, dst, sems.at[n])
        for n, (src, dst) in enumerate((
            (gate_ref, gate_out), (up_ref, up_out), (down_ref, down_out), (token_ref, token_out),
        ))
    ]
    for copy in copies:
        copy.start()
    for k in range(route_ref.shape[0]):
        row = jnp.zeros((1, route_ref.shape[1]), jnp.float32)
        for expert in range(found_ref.shape[0]):
            hit = route_ref[pl.ds(k, 1), :] == expert
            row = row + jnp.where(hit, found_ref[expert], 0.0)
        found_buf[pl.ds(k, 1), :] = row
    last = pltpu.make_async_copy(found_buf, found_out, sems.at[4])
    last.start()
    for copy in copies:
        copy.wait()
    last.wait()


def store(token_grad, found, gate_grads, up_grads, down_grads, routes):
    arrays = (token_grad, found, gate_grads, up_grads, down_grads)
    outs = [jax.ShapeDtypeStruct(a.shape, a.dtype) for a in arrays]
    outs[1] = jax.ShapeDtypeStruct(routes.shape, jnp.float32)
    return pl.pallas_call(
        store_kernel,
        out_shape=tuple(outs),
        in_specs=[pl.BlockSpec(memory_space=pltpu.VMEM)] * 6,
        out_specs=(pl.BlockSpec(memory_space=pltpu.HBM),) * 5,
        scratch_shapes=[pltpu.VMEM(routes.shape, jnp.float32), pltpu.SemaphoreType.DMA((5,))],
        compiler_params=pltpu.CompilerParams(vmem_limit_bytes=8 * 1024 * 1024),
    )(*arrays, routes)


def gathered(tokens, routes, gate_weights, out_grad, w_gate, w_up, w_down):
    ep_count = lax.axis_size("ep")
    token_count, model_width = tokens.shape
    capacity = token_count * routes.shape[1] * 5 // (4 * ep_count)
    width = model_width // lax.axis_size("tp")
    arrays = (tokens, out_grad, routes.T, gate_weights.T, w_gate[0], w_up[0], w_down[0])
    arrays = [pltpu.with_memory_space_constraint(array, pltpu.HBM) for array in arrays]
    parts = fused(*arrays, capacity, width)
    token_grad, gate_grad, gate_grads, up_grads, down_grads = store(*parts, routes.T)
    return (token_grad, gate_grad.T, gate_grads[None], up_grads[None], down_grads[None])


def chosen(*args):
    tokens, w_gate = args[0], args[4]
    ep_count = lax.axis_size("ep")
    block_bytes = ep_count * tokens.size * 2
    if block_bytes <= 16 * 1024 * 1024 and w_gate.shape[0] == 1 and ep_count == 8:
        return gathered(*args)
    return local(*args)


def solution(mesh):
    return jax.shard_map(
        chosen,
        mesh=mesh,
        in_specs=(
            P("ep", None),
            P("ep", None),
            P("ep", None),
            P("ep", None),
            P("ep", None, "tp"),
            P("ep", None, "tp"),
            P("ep", "tp", None),
        ),
        out_specs=(
            P("ep", "tp"),
            P("ep", None),
            P("ep", None, "tp"),
            P("ep", None, "tp"),
            P("ep", "tp", None),
        ),
        check_vma=False,
    )
```

```python
import jax
import jax.numpy as jnp
from jax import lax
from jax.experimental import pallas as pl
from jax.experimental.pallas import tpu as pltpu
from jax.sharding import PartitionSpec as P

clamp_limit = 7.0
sigmoid_slope = 1.702
MESH = pl.DeviceIdType.MESH
far_step = 2


def partners():
    ep_count = lax.axis_size("ep")
    tp_count = lax.axis_size("tp")
    here = lax.axis_index("ep")
    part = lax.axis_index("tp")
    beside = part + 1 - 2 * (part % 2)
    across = (part + tp_count // 2) % tp_count
    return ep_count, here, part, beside, across


def greet(ep_count, here, part, beside, across):
    barrier = pltpu.get_barrier_semaphore()
    pl.semaphore_signal(barrier, inc=1, device_id=(here, beside), device_id_type=MESH)
    pl.semaphore_signal(barrier, inc=1, device_id=(here, across), device_id_type=MESH)

    def call(j, carry):
        peer = (here + j) % ep_count
        pl.semaphore_signal(barrier, inc=1, device_id=(peer, part), device_id_type=MESH)
        return carry

    lax.fori_loop(1, ep_count, call, 0)
    pl.semaphore_wait(barrier, ep_count + 1)


def remote(src, dst, sent, got, device):
    return pltpu.make_async_remote_copy(
        src_ref=src, dst_ref=dst, send_sem=sent, recv_sem=got, device_id=device, device_id_type=MESH
    )


def dispatch_kernel(
    token_ref, grad_ref, weight_ref, token_rows, grad_rows, weights_out,
    s1, r1, s2, r2, s3, r3, s4, r4, sw, rw, own_sem,
):
    ep_count, here, part, beside, across = partners()
    width = token_ref.shape[2]
    pairs = ((0, token_ref, token_rows), (1, grad_ref, grad_rows))

    def block(rows_ref, source, owner):
        columns = pl.ds(pl.multiple_of(owner * width, width), width)
        return rows_ref.at[source, :, columns]

    greet(ep_count, here, part, beside, across)

    def first(j):
        peer = (here + j) % ep_count
        return [
            remote(send.at[peer], block(rows, here, part), s1.at[i, j], r1.at[i, j], (peer, part))
            for i, send, rows in pairs
        ]

    def first_weight(j):
        peer = (here + j) % ep_count
        return remote(
            weight_ref.at[peer], weights_out.at[here], sw.at[j], rw.at[j], (peer, part)
        )

    def forward(j, owner, sent, got, to):
        source = (here + ep_count - j) % ep_count
        return [
            remote(
                block(rows, source, owner), block(rows, source, owner),
                sent.at[i, j], got.at[i, j], (here, to),
            )
            for i, _, rows in pairs
        ]

    def near(j):
        return forward(j, part, s2, r2, beside)

    def far(j):
        return forward(j, part, s3, r3, across)

    def onward(j):
        return forward(j, across, s4, r4, beside)

    owns = [
        pltpu.make_async_copy(send.at[here], block(rows, here, part), own_sem.at[i])
        for i, send, rows in pairs
    ]
    owns.append(pltpu.make_async_copy(weight_ref.at[here], weights_out.at[here], own_sem.at[2]))
    for copy in owns:
        copy.start()

    def launch(j, carry):
        first_weight(j).start()
        for copy in first(j):
            copy.start()
        return carry

    lax.fori_loop(1, ep_count, launch, 0)
    for copy in owns:
        copy.wait()
    for copy in far(0) + near(0):
        copy.start()

    def pass_on(j, carry):
        @pl.when(j < ep_count)
        def _():
            for i in range(2):
                first(j)[i].wait_recv()
                far(j)[i].start()
                near(j)[i].start()

        @pl.when(j >= 2)
        def _():
            for i in range(2):
                far(j - 2)[i].wait_recv()
                onward(j - 2)[i].start()

        return carry

    lax.fori_loop(1, ep_count + 2, pass_on, 0)

    def finish(j, carry):
        for i in range(2):
            near(j)[i].wait()
            onward(j)[i].wait()
            far(j)[i].wait_send()

        @pl.when(j >= 1)
        def _():
            for copy in first(j):
                copy.wait_send()
            first_weight(j).wait()

        return carry

    lax.fori_loop(0, ep_count, finish, 0)


def dispatch(send_tokens, send_grads, weights, model_width):
    ep_count, capacity, width = send_tokens.shape
    sems = [pltpu.SemaphoreType.DMA((2, ep_count)) for _ in range(8)]
    sems += [pltpu.SemaphoreType.DMA((ep_count,)) for _ in range(2)]
    whole = jax.ShapeDtypeStruct((ep_count, capacity, model_width), jnp.bfloat16)
    return pl.pallas_call(
        dispatch_kernel,
        out_shape=(whole, whole, jax.ShapeDtypeStruct(weights.shape, jnp.float32)),
        in_specs=[pl.BlockSpec(memory_space=pltpu.VMEM)] * 3,
        out_specs=(
            pl.BlockSpec(memory_space=pl.ANY),
            pl.BlockSpec(memory_space=pl.ANY),
            pl.BlockSpec(memory_space=pltpu.VMEM),
        ),
        scratch_shapes=sems + [pltpu.SemaphoreType.DMA((3,))],
        compiler_params=pltpu.CompilerParams(collective_id=0, has_side_effects=True),
    )(send_tokens, send_grads, weights)


def combine_kernel(
    rows_ref, product_ref, back_ref, back_product, near_buf, far_send, far_buf, last_send,
    product_near, product_sum, product_far, product_send,
    s1, r1, s2, r2, s3, r3, sw, rw, small_send, small_recv,
):
    ep_count, here, part, beside, across = partners()
    width = back_ref.shape[2]
    beside_far = (beside + lax.axis_size("tp") // 2) % lax.axis_size("tp")

    def columns(owner):
        return pl.ds(pl.multiple_of(owner * width, width), width)

    greet(ep_count, here, part, beside, across)

    def near(which, j):
        target = (here + j) % ep_count
        owner = beside_far if which == 0 else beside
        return remote(
            rows_ref.at[target, :, columns(owner)], near_buf.at[which, j],
            s1.at[which, j], r1.at[which, j], (here, beside),
        )

    def far(j):
        return remote(far_send.at[j], far_buf.at[j], s2.at[j], r2.at[j], (here, across))

    def last(j):
        peer = (here + j) % ep_count
        return remote(last_send.at[j], back_ref.at[here], s3.at[j], r3.at[j], (peer, part))

    def last_product(j):
        peer = (here + j) % ep_count
        return remote(
            product_send.at[peer], back_product.at[here], sw.at[j], rw.at[j], (peer, part)
        )

    small_near = remote(product_ref, product_near, small_send.at[0], small_recv.at[0], (here, beside))
    small_far = remote(product_sum, product_far, small_send.at[1], small_recv.at[1], (here, across))
    small_near.start()

    def launch(step, carry):
        j = (step + 1) % ep_count
        near(0, j).start()
        near(1, j).start()
        return carry

    lax.fori_loop(0, ep_count, launch, 0)
    small_near.wait_recv()
    product_sum[...] = product_ref[...] + product_near[...]
    small_far.start()

    def middle(step, carry):
        j = (step + 1) % ep_count
        near(0, j).wait_recv()
        target = (here + j) % ep_count
        mine = rows_ref[target, :, columns(across)].astype(jnp.float32)
        far_send[j] = (mine + near_buf[0, j].astype(jnp.float32)).astype(jnp.bfloat16)
        far(j).start()
        return carry

    lax.fori_loop(0, ep_count, middle, 0)
    small_far.wait_recv()
    product_send[...] = product_sum[...] + product_far[...]

    def total(j):
        near(1, j).wait_recv()
        far(j).wait_recv()
        target = (here + j) % ep_count
        mine = rows_ref[target, :, columns(part)].astype(jnp.float32)
        added = mine + near_buf[1, j].astype(jnp.float32) + far_buf[j].astype(jnp.float32)
        return added.astype(jnp.bfloat16)

    def end(j, carry):
        last_send[j] = total(j)
        last(j).start()
        last_product(j).start()
        return carry

    lax.fori_loop(1, ep_count, end, 0)
    back_ref[here] = total(0)
    back_product[here] = product_send[here]

    small_near.wait_send()
    small_far.wait_send()

    def finish(j, carry):
        near(0, j).wait_send()
        near(1, j).wait_send()
        far(j).wait_send()

        @pl.when(j >= 1)
        def _():
            last(j).wait()
            last_product(j).wait()

        return carry

    lax.fori_loop(0, ep_count, finish, 0)


def combine(rows, products, width):
    ep_count, capacity, _ = rows.shape
    one = (ep_count, capacity, width)
    small = pltpu.VMEM(products.shape, jnp.float32)
    dma = pltpu.SemaphoreType.DMA
    return pl.pallas_call(
        combine_kernel,
        out_shape=(
            jax.ShapeDtypeStruct(one, jnp.bfloat16),
            jax.ShapeDtypeStruct(products.shape, jnp.float32),
        ),
        in_specs=[pl.BlockSpec(memory_space=pltpu.VMEM)] * 2,
        out_specs=(pl.BlockSpec(memory_space=pltpu.VMEM),) * 2,
        scratch_shapes=[
            pltpu.VMEM((2,) + one, jnp.bfloat16),
            pltpu.VMEM(one, jnp.bfloat16),
            pltpu.VMEM(one, jnp.bfloat16),
            pltpu.VMEM(one, jnp.bfloat16),
            small, small, small, small,
            dma((2, ep_count)), dma((2, ep_count)),
            dma((ep_count,)), dma((ep_count,)), dma((ep_count,)), dma((ep_count,)),
            dma((ep_count,)), dma((ep_count,)), dma((2,)), dma((2,)),
        ],
        compiler_params=pltpu.CompilerParams(
            collective_id=1, has_side_effects=True, vmem_limit_bytes=48 * 1024 * 1024
        ),
    )(rows, products)


def local(tokens, routes, gate_weights, out_grad, w_gate, w_up, w_down):
    f32, bf16 = jnp.float32, jnp.bfloat16
    ep_count = lax.axis_size("ep")
    tp_count = lax.axis_size("tp")
    part = lax.axis_index("tp")
    token_count, model_width = tokens.shape
    top_count = routes.shape[1]
    experts = ep_count * w_gate.shape[0]
    capacity = token_count * top_count * 5 // (4 * experts)
    width = model_width // tp_count

    match = routes[:, :, None] == jnp.arange(experts, dtype=jnp.int32)[None, None, :]
    named = jnp.any(match, axis=1)
    before = jnp.arange(token_count)[:, None] > jnp.arange(token_count)[None, :]
    rank = jnp.dot(before.astype(bf16), named.astype(bf16), preferred_element_type=f32)
    rank = jnp.where(named, rank.astype(jnp.int32), -1)
    pick = rank.T[:, None, :] == jnp.arange(capacity, dtype=jnp.int32)[None, :, None]
    pick_flat = pick.reshape(experts * capacity, token_count).astype(bf16)
    weight_of = jnp.sum(jnp.where(match, gate_weights[:, :, None], 0.0), axis=1)
    send_weights = jnp.sum(jnp.where(pick, weight_of.T[:, None, :], 0.0), axis=2)
    sends = []
    for array in (tokens, out_grad):
        own = lax.dynamic_slice_in_dim(array, part * width, width, 1)
        picked = jnp.dot(pick_flat, own, preferred_element_type=f32).astype(bf16)
        sends.append(picked.reshape(experts, capacity, width))

    rows, grads, weights = dispatch(*sends, send_weights[:, None, :], model_width)
    row_count = ep_count * capacity
    x_rows = rows.reshape(row_count, model_width)
    dy_rows = grads.reshape(row_count, model_width)
    slot_weights = weights.reshape(row_count, 1)

    gate_pre = jnp.dot(x_rows, w_gate[0], preferred_element_type=f32)
    up_pre = jnp.dot(x_rows, w_up[0], preferred_element_type=f32)
    plain_grad = jnp.einsum("rd,fd->rf", dy_rows, w_down[0], preferred_element_type=f32)
    glu = jnp.minimum(gate_pre, clamp_limit)
    linear = jnp.clip(up_pre, -clamp_limit, clamp_limit)
    sigma = jax.nn.sigmoid(sigmoid_slope * glu)
    active = glu * sigma
    hidden = active * (linear + 1.0)
    product = jnp.sum(hidden * plain_grad, axis=1)
    hidden_grad = plain_grad * slot_weights
    slope_term = sigma + sigmoid_slope * active * (1.0 - sigma)
    gate_pre_grad = jnp.where(
        gate_pre < clamp_limit, hidden_grad * (linear + 1.0) * slope_term, 0.0
    ).astype(bf16)
    up_pre_grad = jnp.where(jnp.abs(up_pre) < clamp_limit, hidden_grad * active, 0.0).astype(bf16)
    hidden = (hidden * slot_weights).astype(bf16)

    row_term = jnp.einsum("rf,df->rd", gate_pre_grad, w_gate[0], preferred_element_type=f32)
    row_term = row_term + jnp.einsum(
        "rf,df->rd", up_pre_grad, w_up[0], preferred_element_type=f32
    )
    row_term = row_term.astype(bf16).reshape(ep_count, capacity, model_width)
    back_rows, back_products = combine(
        row_term, product.reshape(ep_count, 1, capacity), width
    )
    gate_grads = jnp.einsum("rd,rf->df", x_rows, gate_pre_grad, preferred_element_type=f32)
    up_grads = jnp.einsum("rd,rf->df", x_rows, up_pre_grad, preferred_element_type=f32)
    down_grads = jnp.einsum("rf,rd->fd", hidden, dy_rows, preferred_element_type=f32)
    token_grad = jnp.einsum(
        "rt,rw->tw", pick_flat, back_rows.reshape(row_count, width), preferred_element_type=f32
    ).astype(bf16)
    found = jnp.sum(jnp.where(pick, back_products.reshape(experts, capacity, 1), 0.0), axis=1)
    gate_grad = jnp.sum(jnp.where(match, found.T[:, None, :], 0.0), axis=2)
    return (token_grad, gate_grad, gate_grads[None], up_grads[None], down_grads[None])


def fused_kernel(
    tok_hbm, grd_hbm, route_hbm, share_hbm, gate_hbm, up_hbm, down_hbm,
    token_out, found_out, gate_out, up_out, down_out,
    tok_ref, grd_ref, route_ref, share_ref, gate_ref, up_ref, down_ref, line, line_extra, metas, pick_send, rows, gate_g, up_g, hid,
    near_send, near_buf, mine, own_sum, back_send,
    wide_buf, half_send, half_buf, narrow_send, narrow_buf, total, total_half, y_send, y_buf,
    found_loc, found_near, found_sum, found_far, found_send,
    chain_s, chain_r, xm_s, xm_r, x_s, x_r, u_s, u_r, n_s, n_r, f_s, f_r, o_s, o_r,
    c_s, c_r, h_s, h_r, w_s, w_r, z_s, z_r, y_s, y_r, sm_s, sm_r, l_s, l_r, in_s,
):
    f32, bf16 = jnp.float32, jnp.bfloat16
    ep_count, here, part, beside, across = partners()
    count = ep_count // 2
    z, x = here // 2, here % 2
    other = here + 1 - 2 * x
    plane, core = part // 2, part % 2
    capacity = rows.shape[2]
    model_width = tok_ref.shape[1]
    width = token_out.shape[1]
    token_count = tok_ref.shape[0]

    def columns(owner):
        return pl.ds(pl.multiple_of(owner * width, width), width)

    def order(i):
        mixed, bit = 0, 1
        while bit < count:
            mixed = mixed + ((z // bit + i // bit) % 2) * bit
            bit = 2 * bit
        return mixed

    inward = (2 * z) // count
    middle = (2 * z * (count - 1 - z) + count * count - 1) // (count * count)

    def place(i):
        return order(i + middle * (i // far_step) * (1 - 2 * (i % 2)))

    def chain(kind, zi, way):
        ref = metas.at[2 * zi + x] if kind == 2 else line.at[kind, zi]
        to = here + 2 - 4 * way
        return remote(ref, ref, chain_s.at[way, kind, zi], chain_r.at[kind, zi], (to, part))

    def chain_extra(kind, way):
        whole = grd_ref if kind else tok_ref
        return remote(
            whole.at[:, columns(across)], line_extra.at[way, kind],
            u_s.at[way, kind], u_r.at[way, kind], (here + 2 - 4 * way, part),
        )

    def cross_meta(zi):
        ref = metas.at[2 * zi + x]
        return remote(ref, ref, xm_s.at[zi], xm_r.at[zi], (other, part))

    def cross(kind, zi):
        return remote(
            pick_send.at[kind, zi], rows.at[kind, 2 * zi + x, :, columns(part)],
            x_s.at[kind, zi], x_r.at[kind, zi], (other, part),
        )

    def forward(kind, source, owner, sent, got, to):
        ref = rows.at[kind, source, :, columns(owner)]
        return remote(ref, ref, sent.at[kind, source], got.at[kind, source], (here, to))

    def near(kind, source):
        return forward(kind, source, part, n_s, n_r, beside)

    def far(kind, source):
        return forward(kind, source, part, f_s, f_r, across)

    def onward(kind, source):
        return forward(kind, source, across, o_s, o_r, beside)

    def pair(source):
        return remote(
            near_send.at[source], near_buf.at[source], c_s.at[source], c_r.at[source],
            (here, beside),
        )

    def half_over(source):
        return remote(
            half_send.at[source], half_buf.at[source], h_s.at[source], h_r.at[source],
            (here, across),
        )

    def is_far(zi):
        return (zi - z) * (zi - z) >= far_step * far_step

    def wide(source, own):
        ref = own_sum.at[source // 2] if own else back_send.at[source // 2]
        return remote(ref, wide_buf.at[here], w_s.at[source], w_r.at[here], (source, part))

    def wide_got(sender):
        return remote(
            own_sum.at[0], wide_buf.at[sender], w_s.at[sender], w_r.at[sender], (sender, part)
        )

    def narrow(source, sender):
        return remote(
            narrow_send.at[source], narrow_buf.at[sender],
            z_s.at[source], z_r.at[sender], (source, part),
        )

    def either(zi, act):
        @pl.when(is_far(zi))
        def _():
            act(True)

        @pl.when(jnp.logical_not(is_far(zi)))
        def _():
            act(False)

    last_y = remote(y_send, y_buf, y_s.at[0], y_r.at[0], (here, across))
    small_near = remote(found_loc, found_near, sm_s.at[0], sm_r.at[0], (here, beside))
    small_far = remote(found_sum, found_far, sm_s.at[1], sm_r.at[1], (here, across))

    def last_found(j):
        peer = (here + j) % ep_count
        return remote(found_send.at[peer], found_out.at[here], l_s.at[j], l_r.at[j], (peer, part))

    slots = lax.broadcasted_iota(jnp.int32, (capacity, token_count), 0).astype(f32)

    def matches(source, expert):
        return slots == metas[source, pl.ds(expert, 1), :]

    def pick(source, expert):
        return jnp.where(matches(source, expert), 1.0, 0.0).astype(bf16)

    barrier = pltpu.get_barrier_semaphore()
    pl.semaphore_signal(barrier, inc=1, device_id=(here, beside), device_id_type=MESH)
    pl.semaphore_signal(barrier, inc=1, device_id=(here, across), device_id_type=MESH)

    pl.semaphore_signal(barrier, inc=1, device_id=(other, part), device_id_type=MESH)

    @pl.when(z > 0)
    def _():
        pl.semaphore_signal(barrier, inc=1, device_id=(here - 2, part), device_id_type=MESH)

    @pl.when(z < count - 1)
    def _():
        pl.semaphore_signal(barrier, inc=1, device_id=(here + 2, part), device_id_type=MESH)

    loads = [
        pltpu.make_async_copy(src, dst, in_s.at[n])
        for n, (src, dst) in enumerate((
            (route_hbm, route_ref), (share_hbm, share_ref),
            (tok_hbm.at[:, columns(part)], line.at[0, z]),
            (grd_hbm.at[:, columns(part)], line.at[1, z]),
            (tok_hbm, tok_ref), (grd_hbm, grd_ref),
            (gate_hbm, gate_ref), (up_hbm, up_ref), (down_hbm, down_ref),
        ))
    ]
    for load in loads:
        load.start()
    total_half[...] = jnp.zeros(total_half.shape, f32)
    experts = lax.broadcasted_iota(jnp.int32, (ep_count, token_count), 0)
    earlier = lax.broadcasted_iota(jnp.int32, (token_count, token_count), 0)
    later = lax.broadcasted_iota(jnp.int32, (token_count, token_count), 1)
    before = jnp.where(earlier < later, 1.0, 0.0).astype(bf16)
    loads[0].wait()
    loads[1].wait()
    named = jnp.zeros((ep_count, token_count), f32)
    weight_of = jnp.zeros((ep_count, token_count), f32)
    for k in range(route_ref.shape[0]):
        chosen_here = route_ref[pl.ds(k, 1), :] == experts
        named = named + jnp.where(chosen_here, 1.0, 0.0)
        weight_of = weight_of + jnp.where(chosen_here, share_ref[pl.ds(k, 1), :], 0.0)
    rank = jnp.dot(named.astype(bf16), before, preferred_element_type=f32)
    metas[here, pl.ds(0, ep_count), :] = jnp.where(named > 0.0, rank, -1.0)
    metas[here, pl.ds(ep_count, ep_count), :] = weight_of
    loads[2].wait()
    loads[3].wait()
    pl.semaphore_wait(barrier, 4 + middle)

    @pl.when(z < count - 1)
    def _():
        for kind in (2, 0, 1):
            chain(kind, z, 0).start()

    @pl.when(z > 0)
    def _():
        for kind in (2, 0, 1):
            chain(kind, z, 1).start()

    def take(kind, zi):
        chain(kind, zi, 0).wait_recv()

        @pl.when((zi < z) & (z < count - 1))
        def _():
            chain(kind, zi, 0).start()

        @pl.when((zi > z) & (z > 0))
        def _():
            chain(kind, zi, 1).start()

    def is_next(zi):
        return (zi - z) * (zi - z) == 1

    def send_extra(way):
        chain_extra(0, way).start()
        chain_extra(1, way).start()

    def hand_on_extra(i):
        zi = place(i)
        source = 2 * zi + x
        way = (zi - z + 1) // 2
        for kind in range(2):
            chain_extra(kind, way).wait_recv()
            own = jnp.dot(
                pick(source, here), line_extra[way, kind], preferred_element_type=f32
            )
            rows[kind, source, :, columns(across)] = own.astype(bf16)
            onward(kind, source).start()

    def relay(kind, i):
        @pl.when(middle == 1)
        def _():
            if kind == 0:
                take(2, place(i))
            take(kind, place(i))

    def picks(kind, i):
        zi = place(i)
        source = 2 * zi + x

        @pl.when((i == 1) | ((i > 1) & (middle == 0)))
        def _():
            if kind == 0:
                take(2, zi)
            take(kind, zi)

        if kind == 0:
            cross_meta(zi).start()
        picked = jnp.dot(pick(source, other), line[kind, zi], preferred_element_type=f32)
        pick_send[kind, zi] = picked.astype(bf16)
        cross(kind, zi).start()

        @pl.when(i >= 1)
        def _():
            own = jnp.dot(pick(source, here), line[kind, zi], preferred_element_type=f32)
            rows[kind, source, :, columns(part)] = own.astype(bf16)

            @pl.when(jnp.logical_not(is_next(zi)))
            def _():
                far(kind, source).start()

            near(kind, source).start()

    def local_picks():
        loads[4].wait()
        loads[5].wait()
        for kind, whole in enumerate((tok_ref, grd_ref)):
            for q in range(model_width // width):
                at = pl.ds(q * width, width)
                own = jnp.dot(pick(here, here), whole[:, at], preferred_element_type=f32)
                rows[kind, here, :, at] = own.astype(bf16)

    def arrive(kind, i):
        source = 2 * place(i) + 1 - x
        cross(kind, place(i)).wait_recv()
        far(kind, source).start()
        near(kind, source).start()
        if kind == 1:
            cross_meta(place(i)).wait_recv()

    def hand_on(source):
        for kind in range(2):
            far(kind, source).wait_recv()
            onward(kind, source).start()

    def compute(source, local_rows):
        @pl.when(local_rows == 0)
        def _():
            for kind in range(2):
                near(kind, source).wait_recv()
                onward(kind, source).wait_recv()

        nt = (((1,), (1,)), ((), ()))
        x_rows = rows[0, source]
        gate_pre = jnp.dot(x_rows, gate_ref[...], preferred_element_type=f32)
        up_pre = jnp.dot(x_rows, up_ref[...], preferred_element_type=f32)
        plain = lax.dot_general(rows[1, source], down_ref[...], nt, preferred_element_type=f32)
        hit = matches(source, here)
        weight_row = metas[source, pl.ds(here + ep_count, 1), :]
        weight = jnp.sum(jnp.where(hit, weight_row, 0.0), axis=1, keepdims=True)
        glu = jnp.minimum(gate_pre, clamp_limit)
        linear = jnp.clip(up_pre, -clamp_limit, clamp_limit)
        sigma = jax.nn.sigmoid(sigmoid_slope * glu)
        active = glu * sigma
        hidden = active * (linear + 1.0)
        product = jnp.sum(hidden * plain, axis=1, keepdims=True)
        found_loc[source] = jnp.sum(jnp.where(hit, product, 0.0), axis=0, keepdims=True)
        hidden_grad = plain * weight
        slope_term = sigma + sigmoid_slope * active * (1.0 - sigma)
        gate_grad = jnp.where(
            gate_pre < clamp_limit, hidden_grad * (linear + 1.0) * slope_term, 0.0
        ).astype(bf16)
        up_grad = jnp.where(jnp.abs(up_pre) < clamp_limit, hidden_grad * active, 0.0).astype(bf16)
        gate_g[source] = gate_grad
        up_g[source] = up_grad
        hid[source] = (hidden * weight).astype(bf16)
        for own in range(2):
            for half in range(2):
                owner = 2 * half + (core if own else 1 - core)
                term = lax.dot_general(
                    gate_g[source], gate_ref[columns(owner), :], nt, preferred_element_type=f32
                ) + lax.dot_general(
                    up_g[source], up_ref[columns(owner), :], nt, preferred_element_type=f32
                )
                at = pl.ds(half * width, width)
                if own:
                    mine[source, :, at] = term.astype(bf16)
                else:
                    near_send[source, :, at] = term.astype(bf16)
            if not own:
                pair(source).start()

    def pair_sum(source, zi, own):
        pair(source).wait_recv()

        def act(small):
            if small:
                at = columns(1 - plane)
                added = mine[source, :, at].astype(f32) + near_buf[source, :, at].astype(f32)
                half_send[source] = added.astype(bf16)
                half_over(source).start()
                return
            added = (mine[source].astype(f32) + near_buf[source].astype(f32)).astype(bf16)
            if own:
                own_sum[zi] = added

                @pl.when((zi < z) | (zi > z))
                def _():
                    wide(source, True).start()
            else:
                back_send[zi] = added
                wide(source, False).start()

        either(zi, act)

    def half_sum(source, zi):
        @pl.when(is_far(zi))
        def _():
            half_over(source).wait_recv()
            at = columns(plane)
            added = mine[source, :, at].astype(f32) + near_buf[source, :, at].astype(f32)
            narrow_send[source] = (added + half_buf[source].astype(f32)).astype(bf16)
            narrow(source, here).start()

    tn = (((0,), (0,)), ((), ()))

    def add_wide(sender, carry):
        @pl.when(jnp.logical_not(is_far(sender // 2)) & ((sender < here) | (sender > here)))
        def _():
            wide_got(sender).wait_recv()
            for half in range(2):
                at = pl.ds(half * width, width)
                total[:, at] = total[:, at] + lax.dot_general(
                    pick(here, sender), wide_buf[sender, :, at], tn, preferred_element_type=f32
                )

        return carry

    def add_own():
        for half in range(2):
            at = pl.ds(half * width, width)
            total[:, at] = lax.dot_general(
                pick(here, here), own_sum[z, :, at], tn, preferred_element_type=f32
            )

    def own_at(i):
        return 2 * place(i) + x

    def other_at(i):
        return 2 * place(i) + 1 - x

    last = count - 1

    def body(i, carry):
        @pl.when(i == last)
        def _():
            pair_sum(other_at(0), place(0), False)

        @pl.when(i >= 1)
        def _():
            arrive(0, i - 1)

        @pl.when(i == count)
        def _():
            pair_sum(own_at(last - 1), place(last - 1), True)

        @pl.when(i >= 2)
        def _():
            hand_on(other_at(i - 2))
            compute(other_at(i - 2), 0)

        @pl.when(i < count)
        def _():
            picks(0, i)

        @pl.when((i == 1) | (i == 2))
        def _():
            relay(0, i + 1)

        @pl.when(i >= 1)
        def _():
            arrive(1, i - 1)

        @pl.when(i == count)
        def _():
            pair_sum(other_at(last - 1), place(last - 1), False)

        @pl.when(i < count)
        def _():
            picks(1, i)

        @pl.when((i == 1) | (i == 2))
        def _():
            relay(1, i + 1)

        @pl.when(i == 0)
        def _():
            local_picks()

            @pl.when(middle == 0)
            def _():
                send_extra(inward)

            for load in loads[6:]:
                load.wait()

        @pl.when((i == 1) & (middle == 1))
        def _():
            send_extra(inward)

        @pl.when((i == 2) & (middle == 1))
        def _():
            send_extra(1 - inward)
            hand_on_extra(1)

        @pl.when((i == 3) & (middle == 1))
        def _():
            compute(own_at(1), 0)
            pair_sum(own_at(1), place(1), True)

        @pl.when(i >= 3)
        def _():
            @pl.when(is_next(place(i - 1)))
            def _():
                hand_on_extra(i - 1)

            @pl.when(jnp.logical_not(is_next(place(i - 1))))
            def _():
                hand_on(own_at(i - 1))

        @pl.when((i == count) & (middle == 0))
        def _():
            hand_on_extra(1)

        @pl.when((i == 0) | (i >= 3))
        def _():
            step = i - (i + count - 1) // count - (1 - middle) * (i // count) * (last - 1)
            compute(own_at(step), 1 - (step + count - 1) // count)

        @pl.when(i == count)
        def _():
            step = 1 + middle * (last - 1)
            pair_sum(own_at(step), place(step), True)

        @pl.when(i == 1)
        def _():
            pair_sum(own_at(0), place(0), True)

        @pl.when(i == last)
        def _():
            pair_sum(other_at(1), place(1), False)

        return carry

    def closing(j, carry):
        @pl.when(j == 1)
        def _():
            half_sum(own_at(last - 1), place(last - 1))
            hand_on(other_at(last))

        @pl.when((j == 1) | (middle == 0))
        def _():
            compute(own_at(last) + (other_at(last) - own_at(last)) * j, 0)

        @pl.when((j == 0) & (middle == 0))
        def _():
            pair_sum(own_at(last), place(last), True)

        @pl.when(j == 1)
        def _():
            small_near.start()
            small_near.wait_recv()
            found_sum[...] = found_loc[...] + found_near[...]
            small_far.start()
            pair_sum(other_at(last), place(last), False)

        return carry

    def weights(n, carry):
        chunk = 256
        tn = (((0,), (0,)), ((), ()))
        at = pl.ds(pl.multiple_of(n * chunk, chunk), chunk)
        flat = ep_count * capacity
        x_part = rows[0, :, :, at].reshape(flat, chunk)
        g_part = rows[1, :, :, at].reshape(flat, chunk)
        units = gate_g.shape[2]
        gate_out[at, :] = lax.dot_general(
            x_part, gate_g[...].reshape(flat, units), tn, preferred_element_type=f32
        )
        up_out[at, :] = lax.dot_general(
            x_part, up_g[...].reshape(flat, units), tn, preferred_element_type=f32
        )
        down_out[:, at] = lax.dot_general(
            hid[...].reshape(flat, units), g_part, tn, preferred_element_type=f32
        )
        return carry

    chunks = model_width // 256
    lax.fori_loop(0, count + 1, body, 0)
    lax.fori_loop(0, 2, closing, 0)

    @pl.when(middle == 1)
    def _():
        half_sum(own_at(last), place(last))

    half_sum(other_at(last - 1), place(last - 1))
    small_far.wait_recv()
    found_send[...] = found_sum[...] + found_far[...]
    found_out[here] = found_send[here]

    def share(j, carry):
        last_found(j).start()
        return carry

    lax.fori_loop(1, ep_count, share, 0)
    add_own()
    lax.fori_loop(0, chunks // 8, weights, 0)

    @pl.when(middle == 0)
    def _():
        half_sum(own_at(last), place(last))

    lax.fori_loop(chunks // 8, chunks // 4, weights, 0)
    half_sum(other_at(last), place(last))
    lax.fori_loop(chunks // 4, chunks // 4 + 1, weights, 0)
    lax.fori_loop(0, ep_count, add_wide, 0)
    y_send[...] = total[:, columns(1 - plane)].astype(bf16)
    last_y.start()
    lax.fori_loop(chunks // 4 + 1, chunks // 2, weights, 0)

    def add_far(sender, carry):
        @pl.when(is_far(sender // 2))
        def _():
            narrow(here, sender).wait_recv()
            total_half[...] = total_half[...] + lax.dot_general(
                pick(here, sender), narrow_buf[sender], tn, preferred_element_type=f32
            )

        return carry

    def finish(zi, carry):
        for kind in range(3):
            @pl.when((zi <= z) & (z < count - 1))
            def _():
                chain(kind, zi, 0).wait_send()

            @pl.when((zi >= z) & (z > 0))
            def _():
                chain(kind, zi, 1).wait_send()

        cross_meta(zi).wait_send()
        for kind in range(2):
            cross(kind, zi).wait_send()

        return carry

    def finish_source(source, carry):
        pair(source).wait_send()

        @pl.when(is_far(source // 2))
        def _():
            half_over(source).wait_send()

        @pl.when(jnp.logical_not(is_far(source // 2)) & ((source < here) | (source > here)))
        def _():
            wide(source, False).wait_send()

        @pl.when((source < here) | (source > here))
        def _():
            for kind in range(2):
                near(kind, source).wait_send()
                onward(kind, source).wait_send()

        gap = source // 2 - z
        across_line = (source - x) % 2

        @pl.when((across_line == 1) | (gap * gap > 1))
        def _():
            for kind in range(2):
                far(kind, source).wait_send()

        return carry

    def finish_extra(way):
        chain_extra(0, way).wait_send()
        chain_extra(1, way).wait_send()

    lax.fori_loop(chunks // 2, chunks, weights, 0)
    lax.fori_loop(0, count, finish, 0)
    lax.fori_loop(0, ep_count, finish_source, 0)
    finish_extra(inward)

    @pl.when(middle == 1)
    def _():
        finish_extra(1 - inward)

    small_near.wait_send()
    small_far.wait_send()

    def finish_found(j, carry):
        last_found(j).wait()
        return carry

    lax.fori_loop(1, ep_count, finish_found, 0)
    def finish_narrow(source, carry):
        @pl.when(is_far(source // 2))
        def _():
            narrow(source, here).wait_send()

        return carry

    lax.fori_loop(0, ep_count, finish_narrow, 0)
    lax.fori_loop(0, ep_count, add_far, 0)
    last_y.wait_recv()
    token_out[...] = (
        total[:, columns(plane)] + total_half[...] + y_buf[...].astype(f32)
    ).astype(bf16)

    last_y.wait_send()


def fused(tokens, grads, routes, shares, w_gate, w_up, w_down, capacity, width):
    f32, bf16 = jnp.float32, jnp.bfloat16
    ep_count = lax.axis_size("ep")
    count = ep_count // 2
    token_count, model_width = tokens.shape
    units = w_gate.shape[1]
    vm = pltpu.VMEM
    dma = pltpu.SemaphoreType.DMA
    small = vm((ep_count, 1, token_count), f32)
    half = (capacity, 2 * width)
    scratch = [
        vm(tokens.shape, bf16),
        vm(tokens.shape, bf16),
        vm(routes.shape, jnp.int32),
        vm(routes.shape, f32),
        vm(w_gate.shape, bf16),
        vm(w_up.shape, bf16),
        vm(w_down.shape, bf16),
        vm((2, count, token_count, width), bf16),
        vm((2, 2, token_count, width), bf16),
        vm((ep_count, 2 * ep_count, token_count), f32),
        vm((2, count, capacity, width), bf16),
        vm((2, ep_count, capacity, model_width), bf16),
        vm((ep_count, capacity, units), bf16),
        vm((ep_count, capacity, units), bf16),
        vm((ep_count, capacity, units), bf16),
        vm((ep_count,) + half, bf16),
        vm((ep_count,) + half, bf16),
        vm((ep_count,) + half, bf16),
        vm((count,) + half, bf16),
        vm((count,) + half, bf16),
        vm((ep_count,) + half, bf16),
        vm((ep_count, capacity, width), bf16),
        vm((ep_count, capacity, width), bf16),
        vm((ep_count, capacity, width), bf16),
        vm((ep_count, capacity, width), bf16),
        vm((token_count, 2 * width), f32),
        vm((token_count, width), f32),
        vm((token_count, width), bf16),
        vm((token_count, width), bf16),
        small, small, small, small, small,
        dma((2, 3, count)), dma((3, count)),
        dma((count,)), dma((count,)),
        dma((2, count)), dma((2, count)),
        dma((2, 2)), dma((2, 2)),
        dma((2, ep_count)), dma((2, ep_count)),
        dma((2, ep_count)), dma((2, ep_count)),
        dma((2, ep_count)), dma((2, ep_count)),
        dma((ep_count,)), dma((ep_count,)),
        dma((ep_count,)), dma((ep_count,)),
        dma((ep_count,)), dma((ep_count,)),
        dma((ep_count,)), dma((ep_count,)),
        dma((1,)), dma((1,)), dma((2,)), dma((2,)),
        dma((ep_count,)), dma((ep_count,)), dma((9,)),
    ]
    return pl.pallas_call(
        fused_kernel,
        out_shape=(
            jax.ShapeDtypeStruct((token_count, width), bf16),
            jax.ShapeDtypeStruct((ep_count, 1, token_count), f32),
            jax.ShapeDtypeStruct((model_width, units), f32),
            jax.ShapeDtypeStruct((model_width, units), f32),
            jax.ShapeDtypeStruct((units, model_width), f32),
        ),
        in_specs=[pl.BlockSpec(memory_space=pltpu.HBM)] * 7,
        out_specs=(pl.BlockSpec(memory_space=pltpu.VMEM),) * 5,
        scratch_shapes=scratch,
        compiler_params=pltpu.CompilerParams(
            collective_id=2, has_side_effects=True, vmem_limit_bytes=47 * 1024 * 1024
        ),
    )(tokens, grads, routes, shares, w_gate, w_up, w_down)


def store_kernel(
    token_ref, found_ref, gate_ref, up_ref, down_ref, route_ref,
    token_out, found_out, gate_out, up_out, down_out, found_buf, sems,
):
    copies = [
        pltpu.make_async_copy(src, dst, sems.at[n])
        for n, (src, dst) in enumerate((
            (gate_ref, gate_out), (up_ref, up_out), (down_ref, down_out), (token_ref, token_out),
        ))
    ]
    for copy in copies:
        copy.start()
    for k in range(route_ref.shape[0]):
        row = jnp.zeros((1, route_ref.shape[1]), jnp.float32)
        for expert in range(found_ref.shape[0]):
            hit = route_ref[pl.ds(k, 1), :] == expert
            row = row + jnp.where(hit, found_ref[expert], 0.0)
        found_buf[pl.ds(k, 1), :] = row
    last = pltpu.make_async_copy(found_buf, found_out, sems.at[4])
    last.start()
    for copy in copies:
        copy.wait()
    last.wait()


def store(token_grad, found, gate_grads, up_grads, down_grads, routes):
    arrays = (token_grad, found, gate_grads, up_grads, down_grads)
    outs = [jax.ShapeDtypeStruct(a.shape, a.dtype) for a in arrays]
    outs[1] = jax.ShapeDtypeStruct(routes.shape, jnp.float32)
    return pl.pallas_call(
        store_kernel,
        out_shape=tuple(outs),
        in_specs=[pl.BlockSpec(memory_space=pltpu.VMEM)] * 6,
        out_specs=(pl.BlockSpec(memory_space=pltpu.HBM),) * 5,
        scratch_shapes=[pltpu.VMEM(routes.shape, jnp.float32), pltpu.SemaphoreType.DMA((5,))],
        compiler_params=pltpu.CompilerParams(vmem_limit_bytes=8 * 1024 * 1024),
    )(*arrays, routes)


def gathered(tokens, routes, gate_weights, out_grad, w_gate, w_up, w_down):
    ep_count = lax.axis_size("ep")
    token_count, model_width = tokens.shape
    capacity = token_count * routes.shape[1] * 5 // (4 * ep_count)
    width = model_width // lax.axis_size("tp")
    arrays = (tokens, out_grad, routes.T, gate_weights.T, w_gate[0], w_up[0], w_down[0])
    arrays = [pltpu.with_memory_space_constraint(array, pltpu.HBM) for array in arrays]
    parts = fused(*arrays, capacity, width)
    token_grad, gate_grad, gate_grads, up_grads, down_grads = store(*parts, routes.T)
    return (token_grad, gate_grad.T, gate_grads[None], up_grads[None], down_grads[None])


def chosen(*args):
    tokens, w_gate = args[0], args[4]
    ep_count = lax.axis_size("ep")
    block_bytes = ep_count * tokens.size * 2
    if block_bytes <= 16 * 1024 * 1024 and w_gate.shape[0] == 1 and ep_count == 8:
        return gathered(*args)
    return local(*args)


def solution(mesh):
    return jax.shard_map(
        chosen,
        mesh=mesh,
        in_specs=(
            P("ep", None),
            P("ep", None),
            P("ep", None),
            P("ep", None),
            P("ep", None, "tp"),
            P("ep", None, "tp"),
            P("ep", "tp", None),
        ),
        out_specs=(
            P("ep", "tp"),
            P("ep", None),
            P("ep", None, "tp"),
            P("ep", None, "tp"),
            P("ep", "tp", None),
        ),
        check_vma=False,
    )
```
